32 devices in a mesh: sp: 8 (over z, x), tp: 4 (over y, core).
Axes of the slice: x: 2, y: 2, z: 4, core: 2. Of those that a mesh axis runs over, the one named last changes fastest.
Arguments:
- out_cotangent: bfloat16 [2048, 2048], P('sp'), may hold values from -6 to 6
- stream: bfloat16 [2048, 2048], P('sp'), may hold values from -6 to 6
- route_ids: int32 [2048, 2], P('sp'), may hold values from 0 to 7, all different within a row; in each aligned block of 256 rows (0 to 255, 256 to 511, ...) at most 128 rows name the same one
- route_weights: float32 [2048, 2], P('sp'), may hold values from 0.3 to 2
- gate_proj: bfloat16 [8, 2048, 1024], P('sp', None, 'tp'), may hold values from -0.125 to 0.125
- up_proj: bfloat16 [8, 2048, 1024], P('sp', None, 'tp'), may hold values from -0.125 to 0.125
- down_proj: bfloat16 [8, 1024, 2048], P('sp', 'tp'), may hold values from -0.1875 to 0.1875
- outer_gate: bfloat16 [2048, 512], P('sp', 'tp'), may hold values from -6 to 6
- inner_gate: bfloat16 [2048, 512], P('sp', 'tp'), may hold values from -6 to 6
- conv_input: bfloat16 [2048, 512], P('sp', 'tp'), may hold values from -6 to 6
- conv_taps: float32 [3, 512], P(None, 'tp'), may hold values from -4 to 4
- out_proj: bfloat16 [2048, 512], P(None, 'tp'), may hold values from -0.25 to 0.25
Outputs:
- grad_gate_proj: bfloat16 [8, 2048, 1024], P('sp', None, 'tp')
- grad_up_proj: bfloat16 [8, 2048, 1024], P('sp', None, 'tp')
- grad_down_proj: bfloat16 [8, 1024, 2048], P('sp', 'tp')
- grad_out_proj: float32 [2048, 512], P('sp', 'tp')
- grad_outer_gate: float32 [2048, 512], P('sp', 'tp')
- grad_inner_gate: float32 [2048, 512], P('sp', 'tp')
- grad_conv_input: float32 [2048, 512], P('sp', 'tp')
The draws below stay inside these ranges and needn't reach their ends.
Inputs may be any that keep to these rules, and one draw needn't show every extreme that they name: `route_ids`: the 2 experts of a token differ. Among the tokens of one index of sp, no expert is chosen more than 128 times, and in every draw some expert is chosen exactly 128 times by them.
All inputs are finite; a program needn't handle non-finite values.
Results may differ from the reference program's by a relative error of at most 0.018.
Values may be sent and summed in bfloat16 or wider, within the bound.
A program may use at most 64 MiB of HBM per device.

```python
import math
import jax
import jax.numpy as jnp
import numpy as np
from jax import lax

D = 2048
FF = 1024
CONV = 512
TAPS = 3
TOPK = 2
TOK_DEV = 256
EXPERTS = 8
CAP = 128
SLOTS = 1024
TOKENS = 2048
N_TP = 4


def with_spikes(entries, rng, source, target, shards_of, factor):
    owner, partner = [(jnp.arange(entries.shape[dim]) // (entries.shape[dim] // shards_of)).reshape([-1 if axis == dim else 1 for axis in range(entries.ndim)]) for dim in (source, target)]
    chosen = jax.random.permutation(rng, shards_of)[partner]
    strong = (owner == chosen) | (owner == (partner + shards_of // 2) % shards_of)
    return jnp.where(strong, factor * entries, entries)


def block_levels(stream_key, dims, cuts, low, largest):
    def one(dim, parts):
        heights = jax.random.uniform(jax.random.fold_in(jax.random.fold_in(stream_key, 6), dim), (parts,), jnp.float32, low / len(cuts), largest / len(cuts))
        return jnp.repeat(jnp.exp(heights), dims[dim] // parts).reshape((-1,) + (1,) * (len(dims) - dim - 1))

    gain = one(*cuts[0])
    for cut in cuts[1:]:
        gain = gain * one(*cut)
    return gain


def deal_out(own_key, own, number, rows, count, top, reach, lean):
    sequence = jax.random.permutation(own_key, count)
    heavy_load, ordinary = shares(count, rows * top, reach, lean, True), shares(count, rows * top, reach, lean, False)
    places = jnp.arange(count)

    def named(tallies, turn):
        used = int((tallies > 0).sum())
        fixed = max(1, used // 4)
        moved = fixed + (places - fixed + turn * (used - fixed)) % max(1, count - fixed)
        return jnp.zeros((count,), jnp.int32).at[sequence[jnp.where(places < fixed, places, moved)]].set(jnp.asarray(tallies, jnp.int32))

    tallies = jnp.where(number % 4 == 0, named(heavy_load, number // 4), named(ordinary, number - number // 4 - 1))
    mixed = jax.random.permutation(jax.random.fold_in(own, 3), count)
    donor, sink = mixed[0:count // 2 * 2:2], mixed[1:count // 2 * 2:2]
    room = jnp.minimum(tallies[donor] - 1, reach - tallies[sink]) // 2
    room = jnp.where((donor == sequence[0]) | (sink == sequence[0]) | (tallies[sink] == 0), 0, jnp.maximum(room, 0))
    moved = jax.random.randint(jax.random.fold_in(own, 4), (count // 2,), 0, 1 << 20) % (room + 1)
    tallies = tallies.at[donor].add(-moved).at[sink].add(moved)
    labels = jnp.searchsorted(jnp.cumsum(tallies), jnp.arange(rows * top), side="right").astype(jnp.int32)
    table = labels.reshape(top, rows).T
    table = table[jax.random.permutation(jax.random.fold_in(own, 1), rows)]
    turn = jax.random.randint(jax.random.fold_in(own, 2), (rows, 1), 0, top)
    return jnp.take_along_axis(table, (jnp.arange(top)[None, :] + turn) % top, axis=1)


def shares(number_of, total, reach, skew, full):
    portions = [(1 << 20) // math.isqrt(grade ** skew) + 1 for grade in range(1, number_of + 1)]
    largest = reach if full else min(reach, max(-(-total // number_of), total * portions[0] // sum(portions)))
    least = 1 if total - largest >= number_of - 1 else 0
    counts, rest = [largest] + [least] * (number_of - 1), total - largest - least * (number_of - 1)
    while rest > 0:
        movable = [i for i in range(1, number_of) if counts[i] < largest] or [i for i in range(1, number_of) if counts[i] < reach]
        whole, left = sum([portions[i] for i in movable]), rest
        for i in movable:
            more = min(reach - counts[i], max(1, left * portions[i] // whole), rest)
            counts[i] = counts[i] + more
            rest = rest - more
    return np.array(counts)


def bell_draw(own_key, dims, deviation, bound, cuts=(), kind=jnp.bfloat16):
    loudness = block_levels(own_key, dims, cuts, -0.22, 0.18) if cuts else 1.0
    entries = jax.random.normal(own_key, dims, jnp.float32) * deviation * loudness
    return jnp.minimum(jnp.maximum(entries, -bound), bound).astype(kind)


def bell_draw_with(stream_key, extent, width, most, cuts, heavy, kind=jnp.bfloat16):
    values = width * jax.random.normal(stream_key, extent, jnp.float32)
    if cuts:
        values = values * block_levels(stream_key, extent, cuts, -0.22, 0.18)
    return jnp.clip(with_spikes(values, jax.random.fold_in(stream_key, 3), *heavy), -most, most).astype(kind)


def setup_inputs(seed: int = 0) -> dict:
    seeds = jax.random.split(jax.random.key(seed), 13)
    out_cotangent = bell_draw_with(seeds[0], (TOKENS, D), 1.0, 6.0, ((0, 8),), (0, 1, 8, 2.0))
    stream = bell_draw(seeds[1], (TOKENS, D), 1.0, 6.0, ((0, 8),))
    route_ids_keys = jax.random.split(jax.random.fold_in(seeds[2], 1), TOKENS // TOK_DEV)
    route_ids_turns = jax.random.permutation(jax.random.fold_in(seeds[2], 3), TOKENS // TOK_DEV)
    route_ids = jax.vmap(lambda own, number: deal_out(jax.random.fold_in(seeds[2], 2), own, number, TOK_DEV, EXPERTS, TOPK, CAP, 1))(route_ids_keys, route_ids_turns).reshape((TOKENS, TOPK))
    route_weights = jnp.clip(0.3 + 1.7 * jax.random.uniform(seeds[3], (TOKENS, TOPK), jnp.float32) ** block_levels(seeds[3], (TOKENS, TOPK), ((0, 8),), -0.2, 0.2), 0.3, 2.0)
    gate_proj = bell_draw(seeds[4], (EXPERTS, D, FF), D ** -0.5, 0.125, ((0, 8), (2, 4)))
    up_proj = bell_draw(seeds[5], (EXPERTS, D, FF), D ** -0.5, 0.125, ((0, 8), (2, 4)))
    down_proj = bell_draw(seeds[6], (EXPERTS, FF, D), FF ** -0.5, 0.1875, ((0, 8), (1, 4)))
    outer_gate = bell_draw(seeds[7], (TOKENS, CONV), 1.0, 6.0, ((0, 8), (1, 4)))
    inner_gate = bell_draw(seeds[8], (TOKENS, CONV), 1.0, 6.0, ((0, 8), (1, 4)))
    conv_input = bell_draw(seeds[9], (TOKENS, CONV), 1.0, 6.0, ((0, 8), (1, 4)))
    conv_taps = bell_draw(seeds[10], (TAPS, CONV), 0.6, 4.0, ((1, 4),), jnp.float32)
    out_proj = bell_draw(seeds[11], (D, CONV), CONV ** -0.5, 0.25, ((1, 4),))
    return dict(out_cotangent=out_cotangent, stream=stream, route_ids=route_ids, route_weights=route_weights, gate_proj=gate_proj, up_proj=up_proj, down_proj=down_proj, outer_gate=outer_gate, inner_gate=inner_gate, conv_input=conv_input, conv_taps=conv_taps, out_proj=out_proj)


def expert_backward(out_cotangent, stream, route_ids, route_weights, w_gate, w_up, w_down, expert):
    chosen = route_ids == expert
    weight = jnp.sum(jnp.where(chosen, route_weights, 0.0), axis=1)
    hit = jnp.any(chosen, axis=1)
    index = jnp.nonzero(hit, size=SLOTS, fill_value=0)[0].astype(jnp.int32)
    count = jnp.sum(hit.astype(jnp.int32))
    valid = jnp.arange(SLOTS, dtype=jnp.int32) < count
    rows_input = jnp.where(valid[:, None], stream[index], jnp.zeros((), jnp.bfloat16))
    rows_grad = (weight[index][:, None] * out_cotangent[index].astype(jnp.float32))
    rows_grad = jnp.where(valid[:, None], rows_grad, 0.0).astype(jnp.bfloat16)
    gate = jnp.dot(rows_input, w_gate, preferred_element_type=jnp.float32)
    up = jnp.dot(rows_input, w_up, preferred_element_type=jnp.float32)
    sig = jax.nn.sigmoid(gate)
    silu_gate = gate * sig
    hidden = (silu_gate * up).astype(jnp.bfloat16)
    d_hidden = lax.dot_general(rows_grad, w_down, (((1,), (1,)), ((), ())), preferred_element_type=jnp.float32)
    d_gate = (d_hidden * up * sig * (1.0 + gate * (1.0 - sig))).astype(jnp.bfloat16)
    d_up = (d_hidden * silu_gate).astype(jnp.bfloat16)
    over_rows = (((0,), (0,)), ((), ()))
    grad_down = lax.dot_general(hidden, rows_grad, over_rows, preferred_element_type=jnp.float32).astype(jnp.bfloat16)
    grad_gate = lax.dot_general(rows_input, d_gate, over_rows, preferred_element_type=jnp.float32).astype(jnp.bfloat16)
    grad_up = lax.dot_general(rows_input, d_up, over_rows, preferred_element_type=jnp.float32).astype(jnp.bfloat16)
    block = FF // N_TP
    gate_blocks = d_gate.astype(jnp.float32).reshape(SLOTS, N_TP, block)
    up_blocks = d_up.astype(jnp.float32).reshape(SLOTS, N_TP, block)
    wg_blocks = w_gate.astype(jnp.float32).reshape(D, N_TP, block)
    wu_blocks = w_up.astype(jnp.float32).reshape(D, N_TP, block)
    partials = jnp.einsum('snf,dnf->nsd', gate_blocks, wg_blocks) + jnp.einsum('snf,dnf->nsd', up_blocks, wu_blocks)
    partials = partials.astype(jnp.bfloat16).astype(jnp.float32)
    row_grad = jnp.sum(partials, axis=0).astype(jnp.bfloat16)
    row_grad = jnp.where(valid[:, None], row_grad.astype(jnp.float32), 0.0)
    return index, row_grad, grad_gate, grad_up, grad_down


def reference(out_cotangent, stream, route_ids, route_weights, gate_proj, up_proj, down_proj,
              outer_gate, inner_gate, conv_input, conv_taps, out_proj):
    def step(carry, inputs):
        w_gate, w_up, w_down, expert = inputs
        index, row_grad, grad_gate, grad_up, grad_down = expert_backward(
            out_cotangent, stream, route_ids, route_weights, w_gate, w_up, w_down, expert)
        carry = carry.at[index].add(row_grad)
        return carry, (grad_gate, grad_up, grad_down)

    moe_grad, grads = lax.scan(step, jnp.zeros((TOKENS, D), jnp.float32),
                               (gate_proj, up_proj, down_proj, jnp.arange(EXPERTS, dtype=jnp.int32)))
    grad_gate_proj, grad_up_proj, grad_down_proj = grads
    stream_grad = (out_cotangent.astype(jnp.float32) + moe_grad).astype(jnp.bfloat16)
    mixed = inner_gate.astype(jnp.float32) * conv_input.astype(jnp.float32)
    padded = jnp.concatenate([jnp.zeros((2, CONV), jnp.float32), mixed], axis=0)
    conv_out = conv_taps[0] * padded[:TOKENS] + conv_taps[1] * padded[1:TOKENS + 1] + conv_taps[2] * padded[2:]
    mixer_out = (outer_gate.astype(jnp.float32) * conv_out).astype(jnp.bfloat16)
    d_mixer = jnp.dot(stream_grad, out_proj, preferred_element_type=jnp.float32)
    grad_outer_gate = d_mixer * conv_out
    d_conv = d_mixer * outer_gate.astype(jnp.float32)
    trailing = jnp.concatenate([d_conv, jnp.zeros((2, CONV), jnp.float32)], axis=0)
    d_mixed = conv_taps[2] * trailing[:TOKENS] + conv_taps[1] * trailing[1:TOKENS + 1] + conv_taps[0] * trailing[2:]
    grad_inner_gate = d_mixed * conv_input.astype(jnp.float32)
    grad_conv_input = d_mixed * inner_gate.astype(jnp.float32)
    grad_out_proj = lax.dot_general(stream_grad, mixer_out, (((0,), (0,)), ((), ())), preferred_element_type=jnp.float32)
    return (grad_gate_proj, grad_up_proj, grad_down_proj, grad_out_proj,
            grad_outer_gate, grad_inner_gate, grad_conv_input)
```

```python
import functools

import jax
import jax.numpy as jnp
from jax import lax
from jax.experimental import pallas as pl
from jax.experimental.pallas import tpu as pltpu
from jax.sharding import PartitionSpec as P


def passed_along(x, axis, by):
    devices = lax.axis_size(axis)
    pairs = [(i, i + by) for i in range(devices) if 0 <= i + by < devices]
    return lax.ppermute(x, axis, pairs)


def to_owners(x, devices):
    blocks = x.reshape(devices, -1, x.shape[1])
    return lax.all_to_all(blocks, "sp", split_axis=0, concat_axis=0, tiled=True).reshape(x.shape)


def partial_rows(d_gate, d_up, w_gate, w_up):
    across = (((1,), (1,)), ((), ()))
    total = lax.dot_general(
        d_gate, w_gate, across, preferred_element_type=jnp.float32
    ) + lax.dot_general(d_up, w_up, across, preferred_element_type=jnp.float32)
    return total.astype(jnp.bfloat16)


def reduced_quarter(d_gate, d_up, w_gate, w_up):
    devices = lax.axis_size("tp")
    if devices != 4:
        return lax.psum_scatter(
            partial_rows(d_gate, d_up, w_gate, w_up), "tp", scatter_dimension=1, tiled=True
        )
    quarter = w_gate.shape[0] // devices
    me = lax.axis_index("tp")

    def rows_of(w, *flips):
        return jnp.concatenate(
            [lax.dynamic_slice_in_dim(w, (me ^ flip) * quarter, quarter, 0) for flip in flips]
        )

    def swapped(x, flip):
        return lax.ppermute(x, "tp", [(i, i ^ flip) for i in range(devices)])

    sent = partial_rows(d_gate, d_up, rows_of(w_gate, 1, 3), rows_of(w_up, 1, 3))
    got = swapped(sent, 1)
    kept = partial_rows(d_gate, d_up, rows_of(w_gate, 0, 2), rows_of(w_up, 0, 2))
    far = kept[:, quarter:].astype(jnp.float32) + got[:, quarter:].astype(jnp.float32)
    near = kept[:, :quarter].astype(jnp.float32) + got[:, :quarter].astype(jnp.float32)
    other = swapped(far.astype(jnp.bfloat16), 2)
    return (near + other.astype(jnp.float32)).astype(jnp.bfloat16)


def shards(
    out_cotangent,
    stream,
    route_ids,
    route_weights,
    gate_proj,
    up_proj,
    down_proj,
    outer_gate,
    inner_gate,
    conv_input,
    conv_taps,
    out_proj,
):
    sp_devices = lax.axis_size("sp")
    tokens_here, width = stream.shape
    experts = sp_devices * gate_proj.shape[0]
    capacity = 4 * tokens_here // experts
    quarter = width // lax.axis_size("tp")
    first_column = lax.axis_index("tp") * quarter
    own_cotangent = lax.dynamic_slice_in_dim(out_cotangent, first_column, quarter, 1)
    own_stream = lax.dynamic_slice_in_dim(stream, first_column, quarter, 1)
    over_rows = (((0,), (0,)), ((), ()))
    expert_ids = jnp.arange(experts, dtype=jnp.int32)
    chosen = route_ids[:, :, None] == expert_ids
    hit = jnp.any(chosen, axis=1)
    token_weight = jnp.sum(jnp.where(chosen, route_weights[:, :, None], 0.0), axis=1)
    token_ids = jnp.arange(tokens_here, dtype=jnp.int32)
    below = (token_ids[:, None] < token_ids[None, :]).astype(jnp.bfloat16)
    rank = lax.dot_general(
        hit.astype(jnp.bfloat16), below, over_rows, preferred_element_type=jnp.float32
    )
    rank = jnp.where(hit.T, rank, -1.0)
    in_slot = rank[:, None, :] == jnp.arange(capacity, dtype=jnp.float32)[None, :, None]
    slot_weight = jnp.sum(jnp.where(in_slot, token_weight.T[:, None, :], 0.0), axis=2)
    pick = in_slot.astype(jnp.bfloat16).reshape(experts * capacity, tokens_here)
    send_input = jnp.dot(pick, own_stream, preferred_element_type=jnp.float32).astype(jnp.bfloat16)
    send_grad = (
        slot_weight.reshape(-1, 1)
        * jnp.dot(pick, own_cotangent, preferred_element_type=jnp.float32)
    ).astype(jnp.bfloat16)
    got_input = to_owners(send_input, sp_devices)
    rows_input = lax.all_gather(got_input, "tp", axis=1, tiled=True)
    send_grad, got_input = lax.optimization_barrier((send_grad, got_input))
    got_grad = to_owners(send_grad, sp_devices)
    rows_grad = lax.all_gather(got_grad, "tp", axis=1, tiled=True)
    mixed = inner_gate.astype(jnp.float32) * conv_input.astype(jnp.float32)
    previous = passed_along(mixed[tokens_here - 2 :], "sp", 1)
    extended = jnp.concatenate([previous, mixed], axis=0)
    conv_out = (
        conv_taps[0] * extended[:tokens_here]
        + conv_taps[1] * extended[1 : tokens_here + 1]
        + conv_taps[2] * extended[2:]
    )
    mixer_out = (outer_gate.astype(jnp.float32) * conv_out).astype(jnp.bfloat16)
    conv_out, mixer_out, rows_grad = lax.optimization_barrier((conv_out, mixer_out, rows_grad))
    w_gate = gate_proj[0]
    w_up = up_proj[0]
    w_down = down_proj[0]
    gate = jnp.dot(rows_input, w_gate, preferred_element_type=jnp.float32)
    up = jnp.dot(rows_input, w_up, preferred_element_type=jnp.float32)
    sig = jax.nn.sigmoid(gate)
    silu_gate = gate * sig
    hidden = (silu_gate * up).astype(jnp.bfloat16)
    across = (((1,), (1,)), ((), ()))
    d_hidden = lax.dot_general(rows_grad, w_down, across, preferred_element_type=jnp.float32)
    d_gate = (d_hidden * up * sig * (1.0 + gate * (1.0 - sig))).astype(jnp.bfloat16)
    d_up = (d_hidden * silu_gate).astype(jnp.bfloat16)
    grad_down = lax.dot_general(
        hidden, rows_grad, over_rows, preferred_element_type=jnp.float32
    ).astype(jnp.bfloat16)
    grad_gate = lax.dot_general(
        rows_input, d_gate, over_rows, preferred_element_type=jnp.float32
    ).astype(jnp.bfloat16)
    grad_up = lax.dot_general(
        rows_input, d_up, over_rows, preferred_element_type=jnp.float32
    ).astype(jnp.bfloat16)
    chunks = 2
    piece = capacity // chunks
    shape = (sp_devices, chunks, piece, d_gate.shape[1])
    gate_pieces = d_gate.reshape(shape)
    up_pieces = d_up.reshape(shape)
    shares = []
    for c in range(chunks):
        shares.append(
            reduced_quarter(
                gate_pieces[:, c].reshape(-1, shape[3]),
                up_pieces[:, c].reshape(-1, shape[3]),
                w_gate,
                w_up,
            )
        )
    shares[0], grad_down, grad_gate, grad_up = lax.optimization_barrier(
        (shares[0], grad_down, grad_gate, grad_up)
    )
    moe_grad = own_cotangent.astype(jnp.float32)
    pick_pieces = pick.reshape(experts, chunks, piece, tokens_here)
    for c in range(chunks):
        returned = to_owners(shares[c], sp_devices)
        moe_grad = moe_grad + lax.dot_general(
            pick_pieces[:, c].reshape(-1, tokens_here), returned, over_rows,
            preferred_element_type=jnp.float32,
        )
    stream_part = moe_grad.astype(jnp.bfloat16)
    stream_grad = lax.all_gather(stream_part, "tp", axis=1, tiled=True)
    own_projection = lax.dot_general(
        stream_grad, mixer_out, over_rows, preferred_element_type=jnp.float32
    ).astype(jnp.bfloat16)
    projections = to_owners(own_projection, sp_devices)
    grad_projection = jnp.sum(
        projections.astype(jnp.float32).reshape(sp_devices, -1, projections.shape[1]), axis=0
    )
    d_mixer = jnp.dot(stream_grad, out_proj, preferred_element_type=jnp.float32)
    grad_outer = d_mixer * conv_out
    d_conv = d_mixer * outer_gate.astype(jnp.float32)
    following = passed_along(d_conv[:2], "sp", -1)
    trailing = jnp.concatenate([d_conv, following], axis=0)
    d_mixed = (
        conv_taps[2] * trailing[:tokens_here]
        + conv_taps[1] * trailing[1 : tokens_here + 1]
        + conv_taps[0] * trailing[2:]
    )
    grad_inner = d_mixed * conv_input.astype(jnp.float32)
    grad_input = d_mixed * inner_gate.astype(jnp.float32)
    return (
        grad_gate[None],
        grad_up[None],
        grad_down[None],
        grad_projection,
        grad_outer,
        grad_inner,
        grad_input,
    )


MESH = pl.DeviceIdType.MESH


def flipped(index, flips):
    place = 1
    while place <= flips:
        if (flips // place) % 2:
            index = index + place * (1 - 2 * ((index // place) % 2))
        place *= 2
    return index


def fused(
    sp_devices,
    groups,
    cot_ref,
    stream_ref,
    pick_ref,
    slot_weight_ref,
    outer_ref,
    inner_ref,
    input_ref,
    taps_ref,
    out_proj_ref,
    w_gate_ref,
    w_up_ref,
    w_down_ref,
    grad_gate_ref,
    grad_up_ref,
    grad_down_ref,
    grad_proj_ref,
    grad_outer_ref,
    grad_inner_ref,
    grad_input_ref,
    rows,
    a_send,
    w_pair,
    w_down,
    hidden,
    d_pair,
    kept,
    near_got,
    core_send,
    core_got,
    y_send,
    y_got,
    back_send,
    back_got,
    stream_grad,
    proj_send,
    proj_got,
    before,
    after,
    conv_out,
    mixer_out,
    load_sem,
    a_sem,
    b_sem,
    c_sem,
    core_sem,
    y_sem,
    back_sem,
    gather_sem,
    proj_sem,
    conv_sem,
):
    f32, bf16 = jnp.float32, jnp.bfloat16
    me = lax.axis_index("sp")
    t = lax.axis_index("tp")
    t_core, t_y, t_far = flipped(t, 1), flipped(t, 2), flipped(t, 3)
    tokens, width = stream_ref.shape
    capacity = pick_ref.shape[0] // sp_devices
    units = hidden.shape[1]
    quarter = width // lax.axis_size("tp")
    per = width // sp_devices
    over_rows = (((0,), (0,)), ((), ()))
    across = (((1,), (1,)), ((), ()))

    def columns(q):
        return pl.ds(pl.multiple_of(q * quarter, quarter), quarter)

    def block(k):
        return pl.ds(k * capacity, capacity)

    def remote(src, dst, sems, sp, tp):
        return pltpu.make_async_remote_copy(
            src_ref=src,
            dst_ref=dst,
            send_sem=sems[0],
            recv_sem=sems[1],
            device_id=(sp, tp),
            device_id_type=MESH,
        )

    peers = [(flipped(me, k), t) for k in range(1, sp_devices)] + [(me, t_core), (me, t_y)]
    barrier = pltpu.get_barrier_semaphore()
    for peer in peers:
        pl.semaphore_signal(barrier, inc=1, device_id=peer, device_id_type=MESH)

    loads = [
        pltpu.make_async_copy(w_gate_ref, w_pair.at[:, pl.ds(0, units)], load_sem.at[0]),
        pltpu.make_async_copy(w_up_ref, w_pair.at[:, pl.ds(units, units)], load_sem.at[1]),
        pltpu.make_async_copy(w_down_ref, w_down, load_sem.at[2]),
    ]
    for load in loads:
        load.start()
    mixed = inner_ref[...].astype(f32) * input_ref[...].astype(f32)
    before[pl.ds(8, tokens), :] = mixed

    pl.semaphore_wait(barrier, len(peers))

    others = range(1, sp_devices)
    a, b, c_near, c_far, back = {}, {}, {}, {}, {}
    for k in others:
        mine, theirs = rows.at[:, block(k), columns(t)], rows.at[:, block(k), columns(t_y)]
        peer = flipped(me, k)
        a[k] = remote(a_send.at[k - 1], mine, (a_sem.at[0, k], a_sem.at[1, k]), peer, t)
        b[k] = remote(mine, mine, (b_sem.at[0, k], b_sem.at[1, k]), me, t_y)
        c_near[k] = remote(mine, mine, (c_sem.at[0, k], c_sem.at[1, k]), me, t_core)
        c_far[k] = remote(theirs, theirs, (c_sem.at[2, k], c_sem.at[3, k]), me, t_core)
        back[k] = remote(
            back_send.at[block(k)],
            back_got.at[pl.ds(pl.multiple_of(me * capacity, capacity), capacity)],
            (back_sem.at[0, k], back_sem.at[1, k]),
            peer,
            t,
        )

    def slots_of(k):
        return pl.ds(pl.multiple_of(flipped(me, k) * capacity, capacity), capacity)

    for k in others:
        pick = pick_ref[slots_of(k), :]
        a_send[k - 1, 0] = jnp.dot(
            pick, stream_ref[:, columns(t)], preferred_element_type=f32
        ).astype(bf16)
        a_send[k - 1, 1] = (
            slot_weight_ref[slots_of(k), :]
            * jnp.dot(pick, cot_ref[:, columns(t)], preferred_element_type=f32)
        ).astype(bf16)
        a[k].start()

    to_next = remote(
        before.at[pl.ds(tokens, 8)],
        before.at[pl.ds(0, 8)],
        (conv_sem.at[0], conv_sem.at[1]),
        me + 1,
        t,
    )
    to_previous = remote(
        after.at[pl.ds(0, 8)],
        after.at[pl.ds(tokens, 8)],
        (conv_sem.at[2], conv_sem.at[3]),
        me - 1,
        t,
    )

    @pl.when(me < sp_devices - 1)
    def _():
        to_next.start()

    pick = pick_ref[slots_of(0), :]
    rows[0, block(0), :] = jnp.dot(pick, stream_ref[...], preferred_element_type=f32).astype(bf16)
    rows[1, block(0), :] = (
        slot_weight_ref[slots_of(0), :]
        * jnp.dot(pick, cot_ref[...], preferred_element_type=f32)
    ).astype(bf16)

    @pl.when(me == 0)
    def _():
        before[pl.ds(0, 8), :] = jnp.zeros((8, before.shape[1]), f32)

    @pl.when(me > 0)
    def _():
        to_next.wait_recv()

    conv = (
        taps_ref[0:1, :] * before[pl.ds(6, tokens), :]
        + taps_ref[1:2, :] * before[pl.ds(7, tokens), :]
        + taps_ref[2:3, :] * before[pl.ds(8, tokens), :]
    )
    conv_out[...] = conv
    mixer_out[...] = (outer_ref[...].astype(f32) * conv).astype(bf16)
    for load in loads:
        load.wait()

    core, y_hop = {}, {}
    for g, ks in enumerate(groups):
        span = pl.ds(ks[0] * capacity, len(ks) * capacity)
        core[g] = [
            remote(
                core_send.at[i, span], core_got.at[i, span],
                (core_sem.at[0, i, g], core_sem.at[1, i, g]), me, t_core,
            )
            for i in range(2)
        ]
        y_hop[g] = remote(y_send.at[span], y_got.at[span], (y_sem.at[0, g], y_sem.at[1, g]), me, t_y)

    def stage_a(ks):
        for k in ks:
            if k:
                a[k].wait_recv()
                b[k].start()
                c_near[k].start()

    def stage_b(ks):
        for k in ks:
            if k:
                b[k].wait_recv()
                c_far[k].start()

    def stage_c(ks):
        for k in ks:
            if k:
                c_near[k].wait_recv()
                c_far[k].wait_recv()

    def expert(g, ks):
        span = pl.ds(ks[0] * capacity, len(ks) * capacity)
        both = jnp.dot(rows[0, span, :], w_pair[...], preferred_element_type=f32)
        gate, up = both[:, :units], both[:, units:]
        d_hidden = lax.dot_general(
            rows[1, span, :], w_down[...], across, preferred_element_type=f32
        )
        sig = jax.nn.sigmoid(gate)
        silu_gate = gate * sig
        hidden[span, :] = (silu_gate * up).astype(bf16)
        d_gate = (d_hidden * up * sig * (1.0 + gate * (1.0 - sig))).astype(bf16)
        d_up = (d_hidden * silu_gate).astype(bf16)
        d_pair[span, pl.ds(0, units)] = d_gate
        d_pair[span, pl.ds(units, units)] = d_up

        def partial(q):
            return lax.dot_general(
                d_pair[span, :], w_pair[columns(q), :], across, preferred_element_type=f32
            ).astype(bf16)

        core_send[1, span, :] = partial(t_far)
        core_send[0, span, :] = partial(t_core)
        core[g][1].start()
        kept[1, span, :] = partial(t_y)
        core[g][0].start()
        kept[0, span, :] = partial(t)

    def reduce_core(g, ks):
        span = pl.ds(ks[0] * capacity, len(ks) * capacity)
        core[g][1].wait_recv()
        y_send[span, :] = (
            kept[1, span, :].astype(f32) + core_got[1, span, :].astype(f32)
        ).astype(bf16)
        core[g][0].wait_recv()
        near_got[span, :] = kept[0, span, :].astype(f32) + core_got[0, span, :].astype(f32)
        y_hop[g].start()

    def reduce_y(g, ks):
        span = pl.ds(ks[0] * capacity, len(ks) * capacity)
        y_hop[g].wait_recv()
        back_send[span, :] = (near_got[span, :] + y_got[span, :].astype(f32)).astype(bf16)
        for k in ks:
            if k:
                back[k].start()
            else:
                own = pl.ds(pl.multiple_of(me * capacity, capacity), capacity)
                back_got[own, :] = back_send[block(0), :]

    stage_a(groups[0])
    last = len(groups) - 1
    for g, ks in enumerate(groups):
        if g < last:
            stage_a(groups[g + 1])
        stage_b(ks)
        if g:
            reduce_y(g - 1, groups[g - 1])
        stage_c(ks)
        expert(g, ks)
        if g < last:
            reduce_core(g, ks)

    step = 2 * units

    def down(j, carry):
        at = pl.ds(pl.multiple_of(j * step, step), step)
        grad_down_ref[:, at] = lax.dot_general(
            hidden[...], rows[1, :, at], over_rows, preferred_element_type=f32
        ).astype(bf16)
        return carry

    def gate_up(j, carry):
        at = pl.ds(pl.multiple_of(j * units, units), units)
        both = lax.dot_general(
            rows[0, :, at], d_pair[...], over_rows, preferred_element_type=f32
        ).astype(bf16)
        grad_gate_ref[at, :] = both[:, :units]
        grad_up_ref[at, :] = both[:, units:]
        return carry

    lax.fori_loop(0, width // step, down, 0)
    reduce_core(last, groups[last])
    lax.fori_loop(0, width // units // 2, gate_up, 0)
    reduce_y(last, groups[last])
    lax.fori_loop(width // units // 2, width // units, gate_up, 0)

    for k in others:
        back[k].wait_recv()
    moe_grad = lax.dot_general(pick_ref[...], back_got[...], over_rows, preferred_element_type=f32)
    stream_grad[:, columns(t)] = (cot_ref[:, columns(t)].astype(f32) + moe_grad).astype(bf16)
    part, part_y = stream_grad.at[:, columns(t)], stream_grad.at[:, columns(t_y)]
    gathers = [
        remote(part, part, (gather_sem.at[0, 0], gather_sem.at[1, 0]), me, t_y),
        remote(part, part, (gather_sem.at[0, 1], gather_sem.at[1, 1]), me, t_core),
        remote(part_y, part_y, (gather_sem.at[0, 2], gather_sem.at[1, 2]), me, t_core),
    ]
    gathers[0].start()
    gathers[1].start()
    share = quarter // per
    sends = []

    def project(j, q):
        piece = stream_grad[:, columns(q)]
        proj_send[j] = lax.dot_general(
            piece, mixer_out[...], over_rows, preferred_element_type=f32
        ).astype(bf16)
        for i in range(share):
            owner = q * share + i
            send = remote(
                proj_send.at[j, pl.ds(i * per, per)],
                proj_got.at[me],
                (proj_sem.at[0, j * share + i], proj_sem.at[1, me]),
                owner,
                t,
            )

            @pl.when(owner != me)
            def _():
                send.start()

            @pl.when(owner == me)
            def _():
                proj_got[me] = proj_send[j, pl.ds(i * per, per), :]

            sends.append((owner, send))
        return jnp.dot(piece, out_proj_ref[columns(q), :], preferred_element_type=f32)

    d_mixer = project(0, t)
    gathers[1].wait_recv()
    d_mixer = d_mixer + project(1, t_core)
    gathers[0].wait_recv()
    gathers[2].start()
    d_mixer = d_mixer + project(2, t_y)
    gathers[2].wait_recv()
    d_mixer = d_mixer + project(3, t_far)

    d_conv = d_mixer * outer_ref[...].astype(f32)
    after[pl.ds(0, tokens), :] = d_conv
    grad_outer_ref[...] = d_mixer * conv_out[...]

    @pl.when(me > 0)
    def _():
        to_previous.start()

    @pl.when(me == sp_devices - 1)
    def _():
        after[pl.ds(tokens, 8), :] = jnp.zeros((8, after.shape[1]), f32)

    @pl.when(me < sp_devices - 1)
    def _():
        to_previous.wait_recv()

    d_mixed = (
        taps_ref[2:3, :] * after[pl.ds(0, tokens), :]
        + taps_ref[1:2, :] * after[pl.ds(1, tokens), :]
        + taps_ref[0:1, :] * after[pl.ds(2, tokens), :]
    )
    grad_inner_ref[...] = d_mixed * input_ref[...].astype(f32)
    grad_input_ref[...] = d_mixed * inner_ref[...].astype(f32)

    for k in others:
        source = flipped(me, k)
        remote(
            proj_send.at[0, pl.ds(0, per)],
            proj_got.at[source],
            (proj_sem.at[0, 0], proj_sem.at[1, source]),
            source,
            t,
        ).wait_recv()
    total = proj_got[0].astype(f32)
    for s in range(1, sp_devices):
        total = total + proj_got[s].astype(f32)
    grad_proj_ref[...] = total

    for k in others:
        for copy in (a[k], b[k], c_near[k], c_far[k], back[k]):
            copy.wait_send()
    for g in range(len(groups)):
        core[g][0].wait_send()
        core[g][1].wait_send()
        y_hop[g].wait_send()
    for gather in gathers:
        gather.wait_send()
    for owner, send in sends:

        @pl.when(owner != me)
        def _():
            send.wait_send()

    @pl.when(me < sp_devices - 1)
    def _():
        to_next.wait_send()

    @pl.when(me > 0)
    def _():
        to_previous.wait_send()


def routing(route_ids, route_weights, experts, capacity):
    expert_ids = jnp.arange(experts, dtype=jnp.int32)
    chosen = route_ids[:, :, None] == expert_ids
    hit = jnp.any(chosen, axis=1)
    token_weight = jnp.sum(jnp.where(chosen, route_weights[:, :, None], 0.0), axis=1)
    tokens_here = route_ids.shape[0]
    token_ids = jnp.arange(tokens_here, dtype=jnp.int32)
    below = (token_ids[:, None] < token_ids[None, :]).astype(jnp.bfloat16)
    rank = lax.dot_general(
        hit.astype(jnp.bfloat16), below, (((0,), (0,)), ((), ())),
        preferred_element_type=jnp.float32,
    )
    rank = jnp.where(hit.T, rank, -1.0)
    in_slot = rank[:, None, :] == jnp.arange(capacity, dtype=jnp.float32)[None, :, None]
    slot_weight = jnp.sum(jnp.where(in_slot, token_weight.T[:, None, :], 0.0), axis=2)
    pick = in_slot.astype(jnp.bfloat16).reshape(experts * capacity, tokens_here)
    return pick, slot_weight.reshape(-1, 1)


def fused_shards(
    out_cotangent,
    stream,
    route_ids,
    route_weights,
    gate_proj,
    up_proj,
    down_proj,
    outer_gate,
    inner_gate,
    conv_input,
    conv_taps,
    out_proj,
):
    f32, bf16 = jnp.float32, jnp.bfloat16
    n = lax.axis_size("sp")
    tokens, width = stream.shape
    units = gate_proj.shape[2]
    channels = out_proj.shape[1]
    capacity = 4 * tokens // n
    slots = n * capacity
    quarter = width // lax.axis_size("tp")
    per = width // n
    pick, slot_weight = routing(route_ids, route_weights, n, capacity)
    groups = [list(range(i, i + 2)) for i in range(0, n, 2)]
    vmem = pl.BlockSpec(memory_space=pltpu.VMEM)
    hbm = pl.BlockSpec(memory_space=pl.ANY)
    dma = pltpu.SemaphoreType.DMA
    grads = pl.pallas_call(
        functools.partial(fused, n, groups),
        out_shape=[
            jax.ShapeDtypeStruct((width, units), bf16),
            jax.ShapeDtypeStruct((width, units), bf16),
            jax.ShapeDtypeStruct((units, width), bf16),
            jax.ShapeDtypeStruct((per, channels), f32),
            jax.ShapeDtypeStruct((tokens, channels), f32),
            jax.ShapeDtypeStruct((tokens, channels), f32),
            jax.ShapeDtypeStruct((tokens, channels), f32),
        ],
        in_specs=[vmem] * 9 + [hbm] * 3,
        out_specs=[vmem] * 7,
        scratch_shapes=[
            pltpu.VMEM((2, slots, width), bf16),
            pltpu.VMEM((n - 1, 2, capacity, quarter), bf16),
            pltpu.VMEM((width, 2 * units), bf16),
            pltpu.VMEM((units, width), bf16),
            pltpu.VMEM((slots, units), bf16),
            pltpu.VMEM((slots, 2 * units), bf16),
            pltpu.VMEM((2, slots, quarter), bf16),
            pltpu.VMEM((slots, quarter), f32),
            pltpu.VMEM((2, slots, quarter), bf16),
            pltpu.VMEM((2, slots, quarter), bf16),
            pltpu.VMEM((slots, quarter), bf16),
            pltpu.VMEM((slots, quarter), bf16),
            pltpu.VMEM((slots, quarter), bf16),
            pltpu.VMEM((slots, quarter), bf16),
            pltpu.VMEM((tokens, width), bf16),
            pltpu.VMEM((width // quarter, quarter, channels), bf16),
            pltpu.VMEM((n, per, channels), bf16),
            pltpu.VMEM((tokens + 8, channels), f32),
            pltpu.VMEM((tokens + 8, channels), f32),
            pltpu.VMEM((tokens, channels), f32),
            pltpu.VMEM((tokens, channels), bf16),
            dma((3,)),
            dma((2, n)),
            dma((2, n)),
            dma((4, n)),
            dma((2, 2, len(groups))),
            dma((2, len(groups))),
            dma((2, n)),
            dma((2, 3)),
            dma((2, n)),
            dma((4,)),
        ],
        compiler_params=pltpu.CompilerParams(
            collective_id=0, has_side_effects=True, vmem_limit_bytes=60 * 1024 * 1024
        ),
    )(
        out_cotangent,
        stream,
        pick,
        slot_weight,
        outer_gate,
        inner_gate,
        conv_input,
        conv_taps,
        out_proj,
        gate_proj[0],
        up_proj[0],
        down_proj[0],
    )
    return (grads[0][None], grads[1][None], grads[2][None], *grads[3:])


def fits_kernel(mesh):
    n = mesh.shape["sp"]
    return mesh.shape["tp"] == 4 and n & (n - 1) == 0 and n <= 8


def solution(mesh):
    placed = (
        P("sp", None),
        P("sp", None),
        P("sp", None),
        P("sp", None),
        P("sp", None, "tp"),
        P("sp", None, "tp"),
        P("sp", "tp", None),
        P("sp", "tp"),
        P("sp", "tp"),
        P("sp", "tp"),
        P(None, "tp"),
        P(None, "tp"),
    )
    return jax.shard_map(
        fused_shards if fits_kernel(mesh) else shards,
        mesh=mesh,
        in_specs=placed,
        out_specs=(
            P("sp", None, "tp"),
            P("sp", None, "tp"),
            P("sp", "tp", None),
            P("sp", "tp"),
            P("sp", "tp"),
            P("sp", "tp"),
            P("sp", "tp"),
        ),
        check_vma=False,
    )
```

```python
import functools

import jax
import jax.numpy as jnp
from jax import lax
from jax.experimental import pallas as pl
from jax.experimental.pallas import tpu as pltpu
from jax.sharding import PartitionSpec as P


def passed_along(x, axis, by):
    devices = lax.axis_size(axis)
    pairs = [(i, i + by) for i in range(devices) if 0 <= i + by < devices]
    return lax.ppermute(x, axis, pairs)


def to_owners(x, devices):
    blocks = x.reshape(devices, -1, x.shape[1])
    return lax.all_to_all(blocks, "sp", split_axis=0, concat_axis=0, tiled=True).reshape(x.shape)


def partial_rows(d_gate, d_up, w_gate, w_up):
    across = (((1,), (1,)), ((), ()))
    total = lax.dot_general(
        d_gate, w_gate, across, preferred_element_type=jnp.float32
    ) + lax.dot_general(d_up, w_up, across, preferred_element_type=jnp.float32)
    return total.astype(jnp.bfloat16)


def reduced_quarter(d_gate, d_up, w_gate, w_up):
    devices = lax.axis_size("tp")
    if devices != 4:
        return lax.psum_scatter(
            partial_rows(d_gate, d_up, w_gate, w_up), "tp", scatter_dimension=1, tiled=True
        )
    quarter = w_gate.shape[0] // devices
    me = lax.axis_index("tp")

    def rows_of(w, *flips):
        return jnp.concatenate(
            [lax.dynamic_slice_in_dim(w, (me ^ flip) * quarter, quarter, 0) for flip in flips]
        )

    def swapped(x, flip):
        return lax.ppermute(x, "tp", [(i, i ^ flip) for i in range(devices)])

    sent = partial_rows(d_gate, d_up, rows_of(w_gate, 1, 3), rows_of(w_up, 1, 3))
    got = swapped(sent, 1)
    kept = partial_rows(d_gate, d_up, rows_of(w_gate, 0, 2), rows_of(w_up, 0, 2))
    far = kept[:, quarter:].astype(jnp.float32) + got[:, quarter:].astype(jnp.float32)
    near = kept[:, :quarter].astype(jnp.float32) + got[:, :quarter].astype(jnp.float32)
    other = swapped(far.astype(jnp.bfloat16), 2)
    return (near + other.astype(jnp.float32)).astype(jnp.bfloat16)


def shards(
    out_cotangent,
    stream,
    route_ids,
    route_weights,
    gate_proj,
    up_proj,
    down_proj,
    outer_gate,
    inner_gate,
    conv_input,
    conv_taps,
    out_proj,
):
    sp_devices = lax.axis_size("sp")
    tokens_here, width = stream.shape
    experts = sp_devices * gate_proj.shape[0]
    capacity = 4 * tokens_here // experts
    quarter = width // lax.axis_size("tp")
    first_column = lax.axis_index("tp") * quarter
    own_cotangent = lax.dynamic_slice_in_dim(out_cotangent, first_column, quarter, 1)
    own_stream = lax.dynamic_slice_in_dim(stream, first_column, quarter, 1)
    over_rows = (((0,), (0,)), ((), ()))
    expert_ids = jnp.arange(experts, dtype=jnp.int32)
    chosen = route_ids[:, :, None] == expert_ids
    hit = jnp.any(chosen, axis=1)
    token_weight = jnp.sum(jnp.where(chosen, route_weights[:, :, None], 0.0), axis=1)
    token_ids = jnp.arange(tokens_here, dtype=jnp.int32)
    below = (token_ids[:, None] < token_ids[None, :]).astype(jnp.bfloat16)
    rank = lax.dot_general(
        hit.astype(jnp.bfloat16), below, over_rows, preferred_element_type=jnp.float32
    )
    rank = jnp.where(hit.T, rank, -1.0)
    in_slot = rank[:, None, :] == jnp.arange(capacity, dtype=jnp.float32)[None, :, None]
    slot_weight = jnp.sum(jnp.where(in_slot, token_weight.T[:, None, :], 0.0), axis=2)
    pick = in_slot.astype(jnp.bfloat16).reshape(experts * capacity, tokens_here)
    send_input = jnp.dot(pick, own_stream, preferred_element_type=jnp.float32).astype(jnp.bfloat16)
    send_grad = (
        slot_weight.reshape(-1, 1)
        * jnp.dot(pick, own_cotangent, preferred_element_type=jnp.float32)
    ).astype(jnp.bfloat16)
    got_input = to_owners(send_input, sp_devices)
    rows_input = lax.all_gather(got_input, "tp", axis=1, tiled=True)
    send_grad, got_input = lax.optimization_barrier((send_grad, got_input))
    got_grad = to_owners(send_grad, sp_devices)
    rows_grad = lax.all_gather(got_grad, "tp", axis=1, tiled=True)
    mixed = inner_gate.astype(jnp.float32) * conv_input.astype(jnp.float32)
    previous = passed_along(mixed[tokens_here - 2 :], "sp", 1)
    extended = jnp.concatenate([previous, mixed], axis=0)
    conv_out = (
        conv_taps[0] * extended[:tokens_here]
        + conv_taps[1] * extended[1 : tokens_here + 1]
        + conv_taps[2] * extended[2:]
    )
    mixer_out = (outer_gate.astype(jnp.float32) * conv_out).astype(jnp.bfloat16)
    conv_out, mixer_out, rows_grad = lax.optimization_barrier((conv_out, mixer_out, rows_grad))
    w_gate = gate_proj[0]
    w_up = up_proj[0]
    w_down = down_proj[0]
    gate = jnp.dot(rows_input, w_gate, preferred_element_type=jnp.float32)
    up = jnp.dot(rows_input, w_up, preferred_element_type=jnp.float32)
    sig = jax.nn.sigmoid(gate)
    silu_gate = gate * sig
    hidden = (silu_gate * up).astype(jnp.bfloat16)
    across = (((1,), (1,)), ((), ()))
    d_hidden = lax.dot_general(rows_grad, w_down, across, preferred_element_type=jnp.float32)
    d_gate = (d_hidden * up * sig * (1.0 + gate * (1.0 - sig))).astype(jnp.bfloat16)
    d_up = (d_hidden * silu_gate).astype(jnp.bfloat16)
    grad_down = lax.dot_general(
        hidden, rows_grad, over_rows, preferred_element_type=jnp.float32
    ).astype(jnp.bfloat16)
    grad_gate = lax.dot_general(
        rows_input, d_gate, over_rows, preferred_element_type=jnp.float32
    ).astype(jnp.bfloat16)
    grad_up = lax.dot_general(
        rows_input, d_up, over_rows, preferred_element_type=jnp.float32
    ).astype(jnp.bfloat16)
    chunks = 2
    piece = capacity // chunks
    shape = (sp_devices, chunks, piece, d_gate.shape[1])
    gate_pieces = d_gate.reshape(shape)
    up_pieces = d_up.reshape(shape)
    shares = []
    for c in range(chunks):
        shares.append(
            reduced_quarter(
                gate_pieces[:, c].reshape(-1, shape[3]),
                up_pieces[:, c].reshape(-1, shape[3]),
                w_gate,
                w_up,
            )
        )
    shares[0], grad_down, grad_gate, grad_up = lax.optimization_barrier(
        (shares[0], grad_down, grad_gate, grad_up)
    )
    moe_grad = own_cotangent.astype(jnp.float32)
    pick_pieces = pick.reshape(experts, chunks, piece, tokens_here)
    for c in range(chunks):
        returned = to_owners(shares[c], sp_devices)
        moe_grad = moe_grad + lax.dot_general(
            pick_pieces[:, c].reshape(-1, tokens_here), returned, over_rows,
            preferred_element_type=jnp.float32,
        )
    stream_part = moe_grad.astype(jnp.bfloat16)
    stream_grad = lax.all_gather(stream_part, "tp", axis=1, tiled=True)
    own_projection = lax.dot_general(
        stream_grad, mixer_out, over_rows, preferred_element_type=jnp.float32
    ).astype(jnp.bfloat16)
    projections = to_owners(own_projection, sp_devices)
    grad_projection = jnp.sum(
        projections.astype(jnp.float32).reshape(sp_devices, -1, projections.shape[1]), axis=0
    )
    d_mixer = jnp.dot(stream_grad, out_proj, preferred_element_type=jnp.float32)
    grad_outer = d_mixer * conv_out
    d_conv = d_mixer * outer_gate.astype(jnp.float32)
    following = passed_along(d_conv[:2], "sp", -1)
    trailing = jnp.concatenate([d_conv, following], axis=0)
    d_mixed = (
        conv_taps[2] * trailing[:tokens_here]
        + conv_taps[1] * trailing[1 : tokens_here + 1]
        + conv_taps[0] * trailing[2:]
    )
    grad_inner = d_mixed * conv_input.astype(jnp.float32)
    grad_input = d_mixed * inner_gate.astype(jnp.float32)
    return (
        grad_gate[None],
        grad_up[None],
        grad_down[None],
        grad_projection,
        grad_outer,
        grad_inner,
        grad_input,
    )


MESH = pl.DeviceIdType.MESH


def flipped(index, flips):
    place = 1
    while place <= flips:
        if (flips // place) % 2:
            index = index + place * (1 - 2 * ((index // place) % 2))
        place *= 2
    return index


def fused(
    sp_devices,
    labels,
    sending,
    groups,
    cot_hbm,
    stream_hbm,
    ids_hbm,
    weights_hbm,
    outer_hbm,
    inner_hbm,
    input_hbm,
    taps_hbm,
    out_proj_hbm,
    w_gate_hbm,
    w_up_hbm,
    w_down_hbm,
    grad_gate_ref,
    grad_up_ref,
    grad_down_ref,
    grad_proj_ref,
    grad_outer_ref,
    grad_inner_ref,
    grad_input_ref,
    cot_ref,
    stream_ref,
    ids_ref,
    weights_ref,
    outer_ref,
    inner_ref,
    input_ref,
    taps_ref,
    out_proj_ref,
    rank_ref,
    weight_ref,
    pick_ref,
    rows,
    a_send,
    w_pair,
    w_down,
    hidden,
    d_pair,
    kept,
    near_got,
    core_send,
    core_got,
    y_send,
    y_got,
    back_send,
    back_got,
    stream_grad,
    proj_send,
    proj_got,
    before,
    after,
    conv_out,
    mixer_out,
    load_sem,
    a_sem,
    b_sem,
    c_sem,
    core_sem,
    y_sem,
    back_sem,
    gather_sem,
    proj_sem,
    conv_sem,
):
    f32, bf16 = jnp.float32, jnp.bfloat16
    scope = jax.named_scope
    me = lax.axis_index("sp")
    t = lax.axis_index("tp")
    t_core, t_y = flipped(t, 1), flipped(t, 2)
    half = lax.axis_size("tp") // 2
    tokens, width = stream_ref.shape
    capacity = pick_ref.shape[0] // sp_devices
    units = hidden.shape[1]
    quarter = width // lax.axis_size("tp")
    per = width // sp_devices
    over_rows = (((0,), (0,)), ((), ()))
    across = (((1,), (1,)), ((), ()))
    others = range(1, sp_devices)

    def owned(member):
        return (member % 2) * half + member // 2

    q, q_core, q_y, q_far = owned(t), owned(t_core), owned(t_y), owned(flipped(t, 3))

    def columns(index):
        return pl.ds(pl.multiple_of(index * quarter, quarter), quarter)

    def block(p):
        return pl.ds(p * capacity, capacity)

    def dynamic_block(p):
        return pl.ds(pl.multiple_of(p * capacity, capacity), capacity)

    def remote(src, dst, sems, sp, tp):
        return pltpu.make_async_remote_copy(
            src_ref=src,
            dst_ref=dst,
            send_sem=sems[0],
            recv_sem=sems[1],
            device_id=(sp, tp),
            device_id_type=MESH,
        )

    peers = [(flipped(me, k), t) for k in others] + [(me, t_core), (me, t_y)]
    barrier = pltpu.get_barrier_semaphore()
    for peer in peers:
        pl.semaphore_signal(barrier, inc=1, device_id=peer, device_id_type=MESH)

    moved = [
        (ids_hbm, ids_ref),
        (weights_hbm, weights_ref),
        (inner_hbm, inner_ref),
        (input_hbm, input_ref),
        (stream_hbm, stream_ref),
        (cot_hbm, cot_ref),
        (w_gate_hbm, w_pair.at[:, pl.ds(0, units)]),
        (w_up_hbm, w_pair.at[:, pl.ds(units, units)]),
        (w_down_hbm, w_down),
        (outer_hbm, outer_ref),
        (taps_hbm, taps_ref),
        (out_proj_hbm, out_proj_ref),
    ]
    loads = [
        pltpu.make_async_copy(src, dst, load_sem.at[i]) for i, (src, dst) in enumerate(moved)
    ]
    for load in loads:
        load.start()

    with scope("prep"):
        for load in loads[:4]:
            load.wait()
        before[pl.ds(8, tokens), :] = inner_ref[...].astype(f32) * input_ref[...].astype(f32)
        expert_ids = lax.broadcasted_iota(jnp.int32, (sp_devices, tokens), 0)
        chosen = [ids_ref[j : j + 1, :] == expert_ids for j in range(ids_ref.shape[0])]
        hit = jnp.zeros((sp_devices, tokens), f32)
        weight = jnp.zeros((sp_devices, tokens), f32)
        for j, choice in enumerate(chosen):
            hit = jnp.where(choice, 1.0, hit)
            weight = jnp.where(choice, weights_ref[j : j + 1, :], weight)
        earlier = lax.broadcasted_iota(jnp.int32, (tokens, tokens), 0)
        later = lax.broadcasted_iota(jnp.int32, (tokens, tokens), 1)
        below = jnp.where(earlier < later, 1.0, 0.0).astype(bf16)
        rank = jnp.dot(hit.astype(bf16), below, preferred_element_type=f32)
        rank_ref[...] = jnp.where(hit > 0.0, rank, -1.0)
        weight_ref[...] = weight
        slot = lax.broadcasted_iota(jnp.int32, (capacity, tokens), 0).astype(f32)

    def picked(expert):
        chosen_slot = rank_ref[pl.ds(expert, 1), :] == slot
        pick = jnp.where(chosen_slot, 1.0, 0.0).astype(bf16)
        pick_ref[dynamic_block(expert), :] = pick
        scale = jnp.sum(
            jnp.where(chosen_slot, weight_ref[pl.ds(expert, 1), :], 0.0), axis=1, keepdims=True
        )
        return pick, scale

    def compacted(choice, at):
        pick, scale = choice
        return (
            jnp.dot(pick, stream_ref[:, at], preferred_element_type=f32).astype(bf16),
            (scale * jnp.dot(pick, cot_ref[:, at], preferred_element_type=f32)).astype(bf16),
        )

    place = {label: p for p, label in enumerate(labels)}
    a, a_extra, b, c_near, c_far, back_out, back_in = {}, {}, {}, {}, {}, {}, {}
    partners = {}
    for label in others:
        p = place[label]
        partner = partners[label] = flipped(me, label)
        mine, theirs = rows.at[:, block(p), columns(q)], rows.at[:, block(p), columns(q_y)]
        a[p] = remote(a_send.at[label], mine, (a_sem.at[0, label], a_sem.at[1, p]), partner, t)
        if label == 1:
            a_extra[p] = remote(
                a_send.at[0], theirs, (a_sem.at[0, 0], a_sem.at[1, 0]), partner, t
            )
        b[p] = remote(mine, mine, (b_sem.at[0, p], b_sem.at[1, p]), me, t_y)
        c_near[p] = remote(mine, mine, (c_sem.at[0, p], c_sem.at[1, p]), me, t_core)
        c_far[p] = remote(theirs, theirs, (c_sem.at[2, p], c_sem.at[3, p]), me, t_core)
        back_out[p] = remote(
            back_send.at[block(p)],
            back_got.at[dynamic_block(me)],
            (back_sem.at[0, p], back_sem.at[1, p]),
            partner,
            t,
        )
        back_in[p] = remote(
            back_send.at[block(p)],
            back_got.at[dynamic_block(partner)],
            (back_sem.at[0, p], back_sem.at[1, p]),
            partner,
            t,
        )
    to_next = remote(
        before.at[pl.ds(tokens, 8)],
        before.at[pl.ds(0, 8)],
        (conv_sem.at[0], conv_sem.at[1]),
        me + 1,
        t,
    )
    to_previous = remote(
        after.at[pl.ds(0, 8)],
        after.at[pl.ds(tokens, 8)],
        (conv_sem.at[2], conv_sem.at[3]),
        me - 1,
        t,
    )

    with scope("loads"):
        loads[4].wait()
        loads[5].wait()
    first = True
    for label in sending:
        p = place[label]
        choice = picked(partners[label])
        a_send[label, 0], a_send[label, 1] = compacted(choice, columns(q))
        if label == 1:
            a_send[0, 0], a_send[0, 1] = compacted(choice, columns(q_y))
        if first:
            first = False
            with scope("barrier"):
                pl.semaphore_wait(barrier, len(peers))

            @pl.when(me < sp_devices - 1)
            def _():
                to_next.start()

        a[p].start()
        if label == 1:
            a_extra[p].start()

    own = compacted(picked(me), pl.ds(0, width))
    rows[0, block(place[0]), :], rows[1, block(place[0]), :] = own
    for load in loads[6:]:
        load.wait()

    core, y_hop = {}, {}

    def span_of(ps):
        return pl.ds(ps[0] * capacity, len(ps) * capacity)

    for g, ps in enumerate(groups):
        span = span_of(ps)
        core[g] = [
            remote(
                core_send.at[i, span],
                core_got.at[i, span],
                (core_sem.at[0, i, g], core_sem.at[1, i, g]),
                me,
                t_core,
            )
            for i in range(2)
        ]
        y_hop[g] = remote(
            y_send.at[span], y_got.at[span], (y_sem.at[0, g], y_sem.at[1, g]), me, t_y
        )

    def stage_a(ps):
        for p in ps:
            if labels[p]:
                with scope(f"a{labels[p]}"):
                    a[p].wait_recv()
                if p not in a_extra:
                    b[p].start()
                c_near[p].start()

    def stage_b(ps):
        for p in ps:
            if labels[p]:
                with scope(f"b{labels[p]}"):
                    if p in a_extra:
                        a_extra[p].wait_recv()
                    else:
                        b[p].wait_recv()
                c_far[p].start()

    def stage_c(ps):
        for p in ps:
            if labels[p]:
                with scope(f"c{labels[p]}"):
                    c_near[p].wait_recv()
                    c_far[p].wait_recv()

    def expert(g, ps):
        span = span_of(ps)
        both = jnp.dot(rows[0, span, :], w_pair[...], preferred_element_type=f32)
        gate, up = both[:, :units], both[:, units:]
        d_hidden = lax.dot_general(
            rows[1, span, :], w_down[...], across, preferred_element_type=f32
        )
        sig = jax.nn.sigmoid(gate)
        silu_gate = gate * sig
        hidden[span, :] = (silu_gate * up).astype(bf16)
        d_gate = (d_hidden * up * sig * (1.0 + gate * (1.0 - sig))).astype(bf16)
        d_up = (d_hidden * silu_gate).astype(bf16)
        d_pair[span, pl.ds(0, units)] = d_gate
        d_pair[span, pl.ds(units, units)] = d_up

        def partial(index):
            return lax.dot_general(
                d_pair[span, :], w_pair[columns(index), :], across, preferred_element_type=f32
            ).astype(bf16)

        core_send[1, span, :] = partial(q_far)
        core_send[0, span, :] = partial(q_core)
        core[g][1].start()
        kept[1, span, :] = partial(q_y)
        core[g][0].start()
        kept[0, span, :] = partial(q)

    def reduce_core(g, ps):
        span = span_of(ps)
        with scope(f"rcw{g}"):
            core[g][1].wait_recv()
        y_send[span, :] = (
            kept[1, span, :].astype(f32) + core_got[1, span, :].astype(f32)
        ).astype(bf16)
        core[g][0].wait_recv()
        near_got[span, :] = kept[0, span, :].astype(f32) + core_got[0, span, :].astype(f32)
        y_hop[g].start()

    def reduce_y(g, ps):
        span = span_of(ps)
        with scope(f"ryw{g}"):
            y_hop[g].wait_recv()
        back_send[span, :] = (near_got[span, :] + y_got[span, :].astype(f32)).astype(bf16)
        for p in ps:
            if labels[p]:
                back_out[p].start()
            else:
                back_got[dynamic_block(me), :] = back_send[block(p), :]

    stage_a(groups[0])
    last = len(groups) - 1
    for g, ps in enumerate(groups):
        if g < last:
            stage_a(groups[g + 1])
        stage_b(ps)
        if g:
            reduce_y(g - 1, groups[g - 1])
        stage_c(ps)
        with scope(f"expert{g}"):
            expert(g, ps)
        if g < last:
            reduce_core(g, ps)

    step = 2 * units

    def down(j, carry):
        at = pl.ds(pl.multiple_of(j * step, step), step)
        grad_down_ref[:, at] = lax.dot_general(
            hidden[...], rows[1, :, at], over_rows, preferred_element_type=f32
        ).astype(bf16)
        return carry

    def gate_up(j, carry):
        at = pl.ds(pl.multiple_of(j * units, units), units)
        both = lax.dot_general(
            rows[0, :, at], d_pair[...], over_rows, preferred_element_type=f32
        ).astype(bf16)
        grad_gate_ref[at, :] = both[:, :units]
        grad_up_ref[at, :] = both[:, units:]
        return carry

    with scope("down"):
        lax.fori_loop(0, width // step, down, 0)
    reduce_core(last, groups[last])

    @pl.when(me == 0)
    def _():
        before[pl.ds(0, 8), :] = jnp.zeros((8, before.shape[1]), f32)

    @pl.when(me > 0)
    def _():
        to_next.wait_recv()

    conv = (
        taps_ref[0:1, :] * before[pl.ds(6, tokens), :]
        + taps_ref[1:2, :] * before[pl.ds(7, tokens), :]
        + taps_ref[2:3, :] * before[pl.ds(8, tokens), :]
    )
    conv_out[...] = conv
    mixer_out[...] = (outer_ref[...].astype(f32) * conv).astype(bf16)
    with scope("gu1"):
        lax.fori_loop(0, width // units // 2, gate_up, 0)
    reduce_y(last, groups[last])
    with scope("gu2"):
        lax.fori_loop(width // units // 2, width // units, gate_up, 0)

    for p, label in enumerate(labels):
        if label:
            with scope(f"back{label}"):
                back_in[p].wait_recv()
    moe_grad = lax.dot_general(pick_ref[...], back_got[...], over_rows, preferred_element_type=f32)
    stream_grad[:, columns(q)] = (cot_ref[:, columns(q)].astype(f32) + moe_grad).astype(bf16)
    part, part_y = stream_grad.at[:, columns(q)], stream_grad.at[:, columns(q_y)]
    gathers = [
        remote(part, part, (gather_sem.at[0, 0], gather_sem.at[1, 0]), me, t_y),
        remote(part, part, (gather_sem.at[0, 1], gather_sem.at[1, 1]), me, t_core),
        remote(part_y, part_y, (gather_sem.at[0, 2], gather_sem.at[1, 2]), me, t_core),
    ]
    gathers[0].start()
    gathers[1].start()
    share = quarter // per
    sends = []

    def project(j, index):
        piece = stream_grad[:, columns(index)]
        proj_send[j] = lax.dot_general(
            piece, mixer_out[...], over_rows, preferred_element_type=f32
        ).astype(bf16)
        for i in range(share):
            owner = index * share + i
            send = remote(
                proj_send.at[j, pl.ds(i * per, per)],
                proj_got.at[me],
                (proj_sem.at[0, j * share + i], proj_sem.at[1, me]),
                owner,
                t,
            )

            @pl.when(owner != me)
            def _():
                send.start()

            @pl.when(owner == me)
            def _():
                proj_got[me] = proj_send[j, pl.ds(i * per, per), :]

            sends.append((owner, send))
        return jnp.dot(piece, out_proj_ref[columns(index), :], preferred_element_type=f32)

    with scope("p0"):
        d_mixer = project(0, q)
    with scope("g1"):
        gathers[1].wait_recv()
    d_mixer = d_mixer + project(1, q_core)
    with scope("g0"):
        gathers[0].wait_recv()
    gathers[2].start()
    d_mixer = d_mixer + project(2, q_y)
    with scope("g2"):
        gathers[2].wait_recv()
    d_mixer = d_mixer + project(3, q_far)

    d_conv = d_mixer * outer_ref[...].astype(f32)
    after[pl.ds(0, tokens), :] = d_conv
    grad_outer_ref[...] = d_mixer * conv_out[...]

    @pl.when(me > 0)
    def _():
        to_previous.start()

    @pl.when(me == sp_devices - 1)
    def _():
        after[pl.ds(tokens, 8), :] = jnp.zeros((8, after.shape[1]), f32)

    with scope("prevw"):

        @pl.when(me < sp_devices - 1)
        def _():
            to_previous.wait_recv()

    d_mixed = (
        taps_ref[2:3, :] * after[pl.ds(0, tokens), :]
        + taps_ref[1:2, :] * after[pl.ds(1, tokens), :]
        + taps_ref[0:1, :] * after[pl.ds(2, tokens), :]
    )
    grad_inner_ref[...] = d_mixed * input_ref[...].astype(f32)
    grad_input_ref[...] = d_mixed * inner_ref[...].astype(f32)

    for k in others:
        source = flipped(me, k)
        with scope(f"pw{k}"):
            remote(
                proj_send.at[0, pl.ds(0, per)],
                proj_got.at[source],
                (proj_sem.at[0, 0], proj_sem.at[1, source]),
                source,
                t,
            ).wait_recv()
    total = proj_got[0].astype(f32)
    for s in range(1, sp_devices):
        total = total + proj_got[s].astype(f32)
    grad_proj_ref[...] = total

    for label in others:
        p = place[label]
        for copy in (a[p], a_extra.get(p), c_near[p], c_far[p], back_out[p]):
            if copy is not None:
                copy.wait_send()
        if p not in a_extra:
            b[p].wait_send()
    for g in range(len(groups)):
        core[g][0].wait_send()
        core[g][1].wait_send()
        y_hop[g].wait_send()
    for gather in gathers:
        gather.wait_send()
    for owner, send in sends:

        @pl.when(owner != me)
        def _():
            send.wait_send()

    @pl.when(me < sp_devices - 1)
    def _():
        to_next.wait_send()

    @pl.when(me > 0)
    def _():
        to_previous.wait_send()


def written(*refs):
    count = (len(refs) - 1) // 2
    sem = refs[-1]
    outs = [
        pltpu.make_async_copy(refs[i], refs[count + i], sem.at[i]) for i in range(count)
    ]
    for out in outs:
        out.start()
    for out in outs:
        out.wait()


def fused_shards(
    out_cotangent,
    stream,
    route_ids,
    route_weights,
    gate_proj,
    up_proj,
    down_proj,
    outer_gate,
    inner_gate,
    conv_input,
    conv_taps,
    out_proj,
):
    f32, bf16 = jnp.float32, jnp.bfloat16
    n = lax.axis_size("sp")
    tokens, width = stream.shape
    units = gate_proj.shape[2]
    channels = out_proj.shape[1]
    capacity = 4 * tokens // n
    slots = n * capacity
    quarter = width // lax.axis_size("tp")
    per = width // n
    if n == 8:
        labels = [0, 2, 3, 6, 7, 1, 4, 5]
        sending = [2, 3, 6, 7, 4, 5, 1]
        groups = [[0, 1], [2, 3], [4, 5], [6], [7]]
    else:
        labels = list(range(n))
        sending = labels[1:]
        groups = [[i] for i in labels]
    vmem = pl.BlockSpec(memory_space=pltpu.VMEM)
    hbm = pl.BlockSpec(memory_space=pltpu.HBM)
    anywhere = pl.BlockSpec(memory_space=pl.ANY)
    dma = pltpu.SemaphoreType.DMA
    shapes = [
        ((width, units), bf16),
        ((width, units), bf16),
        ((units, width), bf16),
        ((per, channels), f32),
        ((tokens, channels), f32),
        ((tokens, channels), f32),
        ((tokens, channels), f32),
    ]
    args = (
        out_cotangent,
        stream,
        route_ids.T,
        route_weights.T,
        outer_gate,
        inner_gate,
        conv_input,
        conv_taps,
        out_proj,
        gate_proj[0],
        up_proj[0],
        down_proj[0],
    )
    grads = pl.pallas_call(
        functools.partial(fused, n, labels, sending, groups),
        out_shape=[pltpu.VMEM(*shape) for shape in shapes],
        in_specs=[hbm] * 12,
        out_specs=[vmem] * 7,
        scratch_shapes=[
            pltpu.VMEM((tokens, width), bf16),
            pltpu.VMEM((tokens, width), bf16),
            pltpu.VMEM(route_ids.shape[::-1], jnp.int32),
            pltpu.VMEM(route_ids.shape[::-1], f32),
            pltpu.VMEM((tokens, channels), bf16),
            pltpu.VMEM((tokens, channels), bf16),
            pltpu.VMEM((tokens, channels), bf16),
            pltpu.VMEM(conv_taps.shape, f32),
            pltpu.VMEM((width, channels), bf16),
            pltpu.VMEM((n, tokens), f32),
            pltpu.VMEM((n, tokens), f32),
            pltpu.VMEM((slots, tokens), bf16),
            pltpu.VMEM((2, slots, width), bf16),
            pltpu.VMEM((n, 2, capacity, quarter), bf16),
            pltpu.VMEM((width, 2 * units), bf16),
            pltpu.VMEM((units, width), bf16),
            pltpu.VMEM((slots, units), bf16),
            pltpu.VMEM((slots, 2 * units), bf16),
            pltpu.VMEM((2, slots, quarter), bf16),
            pltpu.VMEM((slots, quarter), f32),
            pltpu.VMEM((2, slots, quarter), bf16),
            pltpu.VMEM((2, slots, quarter), bf16),
            pltpu.VMEM((slots, quarter), bf16),
            pltpu.VMEM((slots, quarter), bf16),
            pltpu.VMEM((slots, quarter), bf16),
            pltpu.VMEM((slots, quarter), bf16),
            pltpu.VMEM((tokens, width), bf16),
            pltpu.VMEM((width // quarter, quarter, channels), bf16),
            pltpu.VMEM((n, per, channels), bf16),
            pltpu.VMEM((tokens + 8, channels), f32),
            pltpu.VMEM((tokens + 8, channels), f32),
            pltpu.VMEM((tokens, channels), f32),
            pltpu.VMEM((tokens, channels), bf16),
            dma((12,)),
            dma((2, n)),
            dma((2, n)),
            dma((4, n)),
            dma((2, 2, len(groups))),
            dma((2, len(groups))),
            dma((2, n)),
            dma((2, 3)),
            dma((2, n)),
            dma((4,)),
        ],
        compiler_params=pltpu.CompilerParams(
            collective_id=0, has_side_effects=True, vmem_limit_bytes=48 * 1024 * 1024
        ),
    )(*(pltpu.with_memory_space_constraint(arg, pltpu.HBM) for arg in args))
    outs = pl.pallas_call(
        written,
        out_shape=[jax.ShapeDtypeStruct(*shape) for shape in shapes],
        in_specs=[anywhere] * 7,
        out_specs=[hbm] * 7,
        scratch_shapes=[dma((7,))],
        compiler_params=pltpu.CompilerParams(vmem_limit_bytes=1024 * 1024),
    )(*(pltpu.with_memory_space_constraint(grad, pltpu.VMEM) for grad in grads))
    return (outs[0][None], outs[1][None], outs[2][None], *outs[3:])


def fits_kernel(mesh):
    n = mesh.shape["sp"]
    return mesh.shape["tp"] == 4 and n & (n - 1) == 0 and n <= 8


def solution(mesh):
    placed = (
        P("sp", None),
        P("sp", None),
        P("sp", None),
        P("sp", None),
        P("sp", None, "tp"),
        P("sp", None, "tp"),
        P("sp", "tp", None),
        P("sp", "tp"),
        P("sp", "tp"),
        P("sp", "tp"),
        P(None, "tp"),
        P(None, "tp"),
    )
    return jax.shard_map(
        fused_shards if fits_kernel(mesh) else shards,
        mesh=mesh,
        in_specs=placed,
        out_specs=(
            P("sp", None, "tp"),
            P("sp", None, "tp"),
            P("sp", "tp", None),
            P("sp", "tp"),
            P("sp", "tp"),
            P("sp", "tp"),
            P("sp", "tp"),
        ),
        check_vma=False,
    )
```

```python
import functools

import jax
import jax.numpy as jnp
from jax import lax
from jax.experimental import pallas as pl
from jax.experimental.pallas import tpu as pltpu
from jax.sharding import PartitionSpec as P


def passed_along(x, axis, by):
    devices = lax.axis_size(axis)
    pairs = [(i, i + by) for i in range(devices) if 0 <= i + by < devices]
    return lax.ppermute(x, axis, pairs)


def to_owners(x, devices):
    blocks = x.reshape(devices, -1, x.shape[1])
    return lax.all_to_all(blocks, "sp", split_axis=0, concat_axis=0, tiled=True).reshape(x.shape)


def partial_rows(d_gate, d_up, w_gate, w_up):
    across = (((1,), (1,)), ((), ()))
    total = lax.dot_general(
        d_gate, w_gate, across, preferred_element_type=jnp.float32
    ) + lax.dot_general(d_up, w_up, across, preferred_element_type=jnp.float32)
    return total.astype(jnp.bfloat16)


def reduced_quarter(d_gate, d_up, w_gate, w_up):
    devices = lax.axis_size("tp")
    if devices != 4:
        return lax.psum_scatter(
            partial_rows(d_gate, d_up, w_gate, w_up), "tp", scatter_dimension=1, tiled=True
        )
    quarter = w_gate.shape[0] // devices
    me = lax.axis_index("tp")

    def rows_of(w, *flips):
        return jnp.concatenate(
            [lax.dynamic_slice_in_dim(w, (me ^ flip) * quarter, quarter, 0) for flip in flips]
        )

    def swapped(x, flip):
        return lax.ppermute(x, "tp", [(i, i ^ flip) for i in range(devices)])

    sent = partial_rows(d_gate, d_up, rows_of(w_gate, 1, 3), rows_of(w_up, 1, 3))
    got = swapped(sent, 1)
    kept = partial_rows(d_gate, d_up, rows_of(w_gate, 0, 2), rows_of(w_up, 0, 2))
    far = kept[:, quarter:].astype(jnp.float32) + got[:, quarter:].astype(jnp.float32)
    near = kept[:, :quarter].astype(jnp.float32) + got[:, :quarter].astype(jnp.float32)
    other = swapped(far.astype(jnp.bfloat16), 2)
    return (near + other.astype(jnp.float32)).astype(jnp.bfloat16)


def shards(
    out_cotangent,
    stream,
    route_ids,
    route_weights,
    gate_proj,
    up_proj,
    down_proj,
    outer_gate,
    inner_gate,
    conv_input,
    conv_taps,
    out_proj,
):
    sp_devices = lax.axis_size("sp")
    tokens_here, width = stream.shape
    experts = sp_devices * gate_proj.shape[0]
    capacity = 4 * tokens_here // experts
    quarter = width // lax.axis_size("tp")
    first_column = lax.axis_index("tp") * quarter
    own_cotangent = lax.dynamic_slice_in_dim(out_cotangent, first_column, quarter, 1)
    own_stream = lax.dynamic_slice_in_dim(stream, first_column, quarter, 1)
    over_rows = (((0,), (0,)), ((), ()))
    expert_ids = jnp.arange(experts, dtype=jnp.int32)
    chosen = route_ids[:, :, None] == expert_ids
    hit = jnp.any(chosen, axis=1)
    token_weight = jnp.sum(jnp.where(chosen, route_weights[:, :, None], 0.0), axis=1)
    token_ids = jnp.arange(tokens_here, dtype=jnp.int32)
    below = (token_ids[:, None] < token_ids[None, :]).astype(jnp.bfloat16)
    rank = lax.dot_general(
        hit.astype(jnp.bfloat16), below, over_rows, preferred_element_type=jnp.float32
    )
    rank = jnp.where(hit.T, rank, -1.0)
    in_slot = rank[:, None, :] == jnp.arange(capacity, dtype=jnp.float32)[None, :, None]
    slot_weight = jnp.sum(jnp.where(in_slot, token_weight.T[:, None, :], 0.0), axis=2)
    pick = in_slot.astype(jnp.bfloat16).reshape(experts * capacity, tokens_here)
    send_input = jnp.dot(pick, own_stream, preferred_element_type=jnp.float32).astype(jnp.bfloat16)
    send_grad = (
        slot_weight.reshape(-1, 1)
        * jnp.dot(pick, own_cotangent, preferred_element_type=jnp.float32)
    ).astype(jnp.bfloat16)
    got_input = to_owners(send_input, sp_devices)
    rows_input = lax.all_gather(got_input, "tp", axis=1, tiled=True)
    send_grad, got_input = lax.optimization_barrier((send_grad, got_input))
    got_grad = to_owners(send_grad, sp_devices)
    rows_grad = lax.all_gather(got_grad, "tp", axis=1, tiled=True)
    mixed = inner_gate.astype(jnp.float32) * conv_input.astype(jnp.float32)
    previous = passed_along(mixed[tokens_here - 2 :], "sp", 1)
    extended = jnp.concatenate([previous, mixed], axis=0)
    conv_out = (
        conv_taps[0] * extended[:tokens_here]
        + conv_taps[1] * extended[1 : tokens_here + 1]
        + conv_taps[2] * extended[2:]
    )
    mixer_out = (outer_gate.astype(jnp.float32) * conv_out).astype(jnp.bfloat16)
    conv_out, mixer_out, rows_grad = lax.optimization_barrier((conv_out, mixer_out, rows_grad))
    w_gate = gate_proj[0]
    w_up = up_proj[0]
    w_down = down_proj[0]
    gate = jnp.dot(rows_input, w_gate, preferred_element_type=jnp.float32)
    up = jnp.dot(rows_input, w_up, preferred_element_type=jnp.float32)
    sig = jax.nn.sigmoid(gate)
    silu_gate = gate * sig
    hidden = (silu_gate * up).astype(jnp.bfloat16)
    across = (((1,), (1,)), ((), ()))
    d_hidden = lax.dot_general(rows_grad, w_down, across, preferred_element_type=jnp.float32)
    d_gate = (d_hidden * up * sig * (1.0 + gate * (1.0 - sig))).astype(jnp.bfloat16)
    d_up = (d_hidden * silu_gate).astype(jnp.bfloat16)
    grad_down = lax.dot_general(
        hidden, rows_grad, over_rows, preferred_element_type=jnp.float32
    ).astype(jnp.bfloat16)
    grad_gate = lax.dot_general(
        rows_input, d_gate, over_rows, preferred_element_type=jnp.float32
    ).astype(jnp.bfloat16)
    grad_up = lax.dot_general(
        rows_input, d_up, over_rows, preferred_element_type=jnp.float32
    ).astype(jnp.bfloat16)
    chunks = 2
    piece = capacity // chunks
    shape = (sp_devices, chunks, piece, d_gate.shape[1])
    gate_pieces = d_gate.reshape(shape)
    up_pieces = d_up.reshape(shape)
    shares = []
    for c in range(chunks):
        shares.append(
            reduced_quarter(
                gate_pieces[:, c].reshape(-1, shape[3]),
                up_pieces[:, c].reshape(-1, shape[3]),
                w_gate,
                w_up,
            )
        )
    shares[0], grad_down, grad_gate, grad_up = lax.optimization_barrier(
        (shares[0], grad_down, grad_gate, grad_up)
    )
    moe_grad = own_cotangent.astype(jnp.float32)
    pick_pieces = pick.reshape(experts, chunks, piece, tokens_here)
    for c in range(chunks):
        returned = to_owners(shares[c], sp_devices)
        moe_grad = moe_grad + lax.dot_general(
            pick_pieces[:, c].reshape(-1, tokens_here), returned, over_rows,
            preferred_element_type=jnp.float32,
        )
    stream_part = moe_grad.astype(jnp.bfloat16)
    stream_grad = lax.all_gather(stream_part, "tp", axis=1, tiled=True)
    own_projection = lax.dot_general(
        stream_grad, mixer_out, over_rows, preferred_element_type=jnp.float32
    ).astype(jnp.bfloat16)
    projections = to_owners(own_projection, sp_devices)
    grad_projection = jnp.sum(
        projections.astype(jnp.float32).reshape(sp_devices, -1, projections.shape[1]), axis=0
    )
    d_mixer = jnp.dot(stream_grad, out_proj, preferred_element_type=jnp.float32)
    grad_outer = d_mixer * conv_out
    d_conv = d_mixer * outer_gate.astype(jnp.float32)
    following = passed_along(d_conv[:2], "sp", -1)
    trailing = jnp.concatenate([d_conv, following], axis=0)
    d_mixed = (
        conv_taps[2] * trailing[:tokens_here]
        + conv_taps[1] * trailing[1 : tokens_here + 1]
        + conv_taps[0] * trailing[2:]
    )
    grad_inner = d_mixed * conv_input.astype(jnp.float32)
    grad_input = d_mixed * inner_gate.astype(jnp.float32)
    return (
        grad_gate[None],
        grad_up[None],
        grad_down[None],
        grad_projection,
        grad_outer,
        grad_inner,
        grad_input,
    )


MESH = pl.DeviceIdType.MESH


def flipped(index, flips):
    place = 1
    while place <= flips:
        if (flips // place) % 2:
            index = index + place * (1 - 2 * ((index // place) % 2))
        place *= 2
    return index


def fused(
    sp_devices,
    labels,
    outer_steps,
    inner_steps,
    cot_hbm,
    stream_hbm,
    ids_hbm,
    weights_hbm,
    outer_hbm,
    inner_hbm,
    input_hbm,
    taps_hbm,
    out_proj_hbm,
    w_gate_hbm,
    w_up_hbm,
    w_down_hbm,
    grad_gate_ref,
    grad_up_ref,
    grad_down_ref,
    grad_proj_ref,
    grad_outer_ref,
    grad_inner_ref,
    grad_input_ref,
    cot_ref,
    stream_ref,
    ids_ref,
    weights_ref,
    outer_ref,
    inner_ref,
    input_ref,
    taps_ref,
    out_proj_ref,
    route,
    far_route,
    far_pick,
    pick_ref,
    raw,
    rows,
    a_send,
    close_send,
    w_pair,
    w_down,
    hidden,
    d_pair,
    kept,
    near_got,
    core_send,
    core_got,
    y_send,
    y_got,
    back_send,
    back_got,
    stream_grad,
    proj_send,
    proj_got,
    before,
    after,
    conv_out,
    mixer_out,
    load_sem,
    route_sem,
    raw_sem,
    close_sem,
    a_sem,
    b_sem,
    c_sem,
    core_sem,
    y_sem,
    back_sem,
    gather_sem,
    proj_sem,
    conv_sem,
):
    f32, bf16 = jnp.float32, jnp.bfloat16
    scope = jax.named_scope
    me = lax.axis_index("sp")
    t = lax.axis_index("tp")
    t_core, t_y = flipped(t, 1), flipped(t, 2)
    half = lax.axis_size("tp") // 2
    tokens, width = stream_ref.shape
    capacity = pick_ref.shape[0] // sp_devices
    units = hidden.shape[1]
    quarter = width // lax.axis_size("tp")
    per = width // sp_devices
    over_rows = (((0,), (0,)), ((), ()))
    across = (((1,), (1,)), ((), ()))
    others = range(1, sp_devices)

    def owned(member):
        return (member % 2) * half + member // 2

    q, q_core, q_y, q_far = owned(t), owned(t_core), owned(t_y), owned(flipped(t, 3))

    def columns(index):
        return pl.ds(pl.multiple_of(index * quarter, quarter), quarter)

    def block(p):
        return pl.ds(p * capacity, capacity)

    def dynamic_block(p):
        return pl.ds(pl.multiple_of(p * capacity, capacity), capacity)

    def remote(src, dst, sems, sp, tp):
        return pltpu.make_async_remote_copy(
            src_ref=src,
            dst_ref=dst,
            send_sem=sems[0],
            recv_sem=sems[1],
            device_id=(sp, tp),
            device_id_type=MESH,
        )

    peers = [(flipped(me, k), t) for k in others] + [(me, t_core), (me, t_y)]
    barrier = pltpu.get_barrier_semaphore()
    for peer in peers:
        pl.semaphore_signal(barrier, inc=1, device_id=peer, device_id_type=MESH)

    moved = [
        (ids_hbm, ids_ref),
        (weights_hbm, weights_ref),
        (inner_hbm, inner_ref),
        (input_hbm, input_ref),
        (stream_hbm, stream_ref),
        (cot_hbm, cot_ref),
        (w_gate_hbm, w_pair.at[:, pl.ds(0, units)]),
        (w_up_hbm, w_pair.at[:, pl.ds(units, units)]),
        (w_down_hbm, w_down),
        (outer_hbm, outer_ref),
        (taps_hbm, taps_ref),
        (out_proj_hbm, out_proj_ref),
    ]
    loads = [
        pltpu.make_async_copy(src, dst, load_sem.at[i]) for i, (src, dst) in enumerate(moved)
    ]
    for load in loads:
        load.start()

    with scope("prep"):
        for load in loads[:4]:
            load.wait()
        before[pl.ds(8, tokens), :] = inner_ref[...].astype(f32) * input_ref[...].astype(f32)
        expert_ids = lax.broadcasted_iota(jnp.int32, (sp_devices, tokens), 0)
        chosen = [ids_ref[j : j + 1, :] == expert_ids for j in range(ids_ref.shape[0])]
        hit = jnp.zeros((sp_devices, tokens), f32)
        weight = jnp.zeros((sp_devices, tokens), f32)
        for j, choice in enumerate(chosen):
            hit = jnp.where(choice, 1.0, hit)
            weight = jnp.where(choice, weights_ref[j : j + 1, :], weight)
        earlier = lax.broadcasted_iota(jnp.int32, (tokens, tokens), 0)
        later = lax.broadcasted_iota(jnp.int32, (tokens, tokens), 1)
        below = jnp.where(earlier < later, 1.0, 0.0).astype(bf16)
        rank = jnp.dot(hit.astype(bf16), below, preferred_element_type=f32)
        route[0] = jnp.where(hit > 0.0, rank, -1.0)
        route[1] = weight
        slot = lax.broadcasted_iota(jnp.int32, (capacity, tokens), 0).astype(f32)

    def slots_of(ref, expert):
        return ref[0, pl.ds(expert, 1), :] == slot

    def one_hot(chosen_slot):
        return jnp.where(chosen_slot, 1.0, 0.0).astype(bf16)

    def scale_of(ref, expert, chosen_slot):
        return jnp.sum(
            jnp.where(chosen_slot, ref[1, pl.ds(expert, 1), :], 0.0), axis=1, keepdims=True
        )

    def compacted(expert, ranges):
        chosen_slot = slots_of(route, expert)
        pick = one_hot(chosen_slot)
        pick_ref[dynamic_block(expert), :] = pick
        scale = scale_of(route, expert, chosen_slot)
        return [
            (
                jnp.dot(pick, stream_ref[:, at], preferred_element_type=f32).astype(bf16),
                (scale * jnp.dot(pick, cot_ref[:, at], preferred_element_type=f32)).astype(bf16),
            )
            for at in ranges
        ]

    z, side = me // 2, me % 2
    upper = z // 2
    inside = (z + upper) % 2
    across_x, near, opposite = flipped(me, 1), flipped(me, 2), flipped(me, 6)
    lines = [z, z + 1 - 2 * (z % 2), 2 - upper, 3 - 3 * upper]
    place = {label: p for p, label in enumerate(labels)}
    a, a_extra, b, c_near, c_far, back_out, back_in, partners = {}, {}, {}, {}, {}, {}, {}, {}
    for label in range(sp_devices):
        p = place[label]
        across_side = 1 - side if label % 2 else side
        partner = partners[p] = 2 * lines[label // 2] + across_side
        a[p], a_extra[p], b[p], c_near[p], c_far[p] = [], [], [], [], []
        for i in range(2):
            mine, theirs = rows.at[i, block(p), columns(q)], rows.at[i, block(p), columns(q_y)]
            if label % 2:
                a[p].append(
                    remote(
                        a_send.at[label // 2, i],
                        mine,
                        (a_sem.at[0, i, p], a_sem.at[1, i, p]),
                        across_x,
                        t,
                    )
                )
            if label == 1:
                a_extra[p].append(
                    remote(
                        a_send.at[sp_devices // 2, i],
                        theirs,
                        (a_sem.at[0, i, 0], a_sem.at[1, i, 0]),
                        across_x,
                        t,
                    )
                )
            b[p].append(remote(mine, mine, (b_sem.at[0, i, p], b_sem.at[1, i, p]), me, t_y))
            c_near[p].append(
                remote(mine, mine, (c_sem.at[0, i, p], c_sem.at[1, i, p]), me, t_core)
            )
            c_far[p].append(
                remote(theirs, theirs, (c_sem.at[2, i, p], c_sem.at[3, i, p]), me, t_core)
            )
        back_out[p] = remote(
            back_send.at[block(p)],
            back_got.at[dynamic_block(me)],
            (back_sem.at[0, p], back_sem.at[1, me]),
            partner,
            t,
        )
        back_in[p] = remote(
            back_send.at[block(p)],
            back_got.at[dynamic_block(partner)],
            (back_sem.at[0, p], back_sem.at[1, partner]),
            partner,
            t,
        )
    close = [
        [
            remote(
                close_send.at[j, i],
                rows.at[i, block(place[2 + j]), columns(q)],
                (close_sem.at[j, i], a_sem.at[1, i, place[2 + j]]),
                flipped(me, 2 + j),
                t,
            )
            for i in range(2)
        ]
        for j in range(2)
    ]
    to_near, to_opposite, on_opposite, on_near = [], [], [], [[], []]
    for i, ref in enumerate((stream_ref, cot_ref)):
        own = ref.at[:, columns(q)]
        to_near.append(
            remote(own, raw.at[0, i], (raw_sem.at[0, i], raw_sem.at[5, i]), near, t)
        )
        to_opposite.append(
            remote(own, raw.at[1, i], (raw_sem.at[1, i], raw_sem.at[6, i]), opposite, t)
        )
        on_opposite.append(
            remote(raw.at[0, i], raw.at[2, i], (raw_sem.at[2, i], raw_sem.at[7, i]), opposite, t)
        )
        for j in range(2):
            on_near[j].append(
                remote(
                    raw.at[1 + j, i],
                    raw.at[1 + j, i],
                    (raw_sem.at[3 + j, i], raw_sem.at[6 + j, i]),
                    near,
                    t,
                )
            )
    as_far = 2 - inside
    route_out = [
        remote(route, far_route.at[0], (route_sem.at[0, 0], route_sem.at[1, 0]), near, t)
    ] + [
        remote(
            route,
            far_route.at[as_far],
            (route_sem.at[0, j], route_sem.at[1, as_far]),
            flipped(me, 2 + 2 * j),
            t,
        )
        for j in (1, 2)
    ]
    route_in = [
        remote(route, far_route.at[j], (route_sem.at[0, j], route_sem.at[1, j]), near, t)
        for j in range(3)
    ]
    to_next = remote(
        before.at[pl.ds(tokens, 8)],
        before.at[pl.ds(0, 8)],
        (conv_sem.at[0], conv_sem.at[1]),
        me + 1,
        t,
    )
    to_previous = remote(
        after.at[pl.ds(0, 8)],
        after.at[pl.ds(tokens, 8)],
        (conv_sem.at[2], conv_sem.at[3]),
        me - 1,
        t,
    )

    with scope("barrier"):
        pl.semaphore_wait(barrier, len(peers))
    for out in route_out:
        out.start()

    @pl.when(me < sp_devices - 1)
    def _():
        to_next.start()

    for i in range(2):
        loads[4 + i].wait()

        @pl.when(inside == 0)
        def _():
            to_near[i].start()

        @pl.when(inside == 1)
        def _():
            to_opposite[i].start()

    @pl.when(inside == 1)
    def _():
        for j in range(2):
            close_send[j, 0], close_send[j, 1] = compacted(flipped(me, 2 + j), [columns(q)])[0]
            for i in range(2):
                close[j][i].start()

    own = compacted(me, [pl.ds(0, width)])[0]
    rows[0, block(place[0]), :], rows[1, block(place[0]), :] = own
    for load in loads[6:]:
        load.wait()

    core, y_hop = {}, {}
    for p in range(len(labels)):
        core[p] = [
            remote(
                core_send.at[i, block(p)],
                core_got.at[i, block(p)],
                (core_sem.at[0, i, p], core_sem.at[1, i, p]),
                me,
                t_core,
            )
            for i in range(2)
        ]
        y_hop[p] = remote(
            y_send.at[block(p)], y_got.at[block(p)], (y_sem.at[0, p], y_sem.at[1, p]), me, t_y
        )

    def compact_far(line, i):
        far = far_route.at[line - 1]
        if i == 0:
            route_in[line - 1].wait_recv()
        for j, expert in enumerate((me, across_x)):
            chosen_slot = slots_of(far, expert)
            if i == 0:
                pick = one_hot(chosen_slot)
                far_pick[line - 1, j] = pick
            else:
                pick = far_pick[line - 1, j]
            part = jnp.dot(pick, raw[line - 1, i], preferred_element_type=f32)
            if i:
                part = scale_of(far, expert, chosen_slot) * part
            p = place[2 * line + j]
            if j:
                a_send[line, i] = part.astype(bf16)
                a[p][i].start()
            else:
                rows[i, block(p), columns(q)] = part.astype(bf16)
                b[p][i].start()
                c_near[p][i].start()

    def first_line(i):
        def go(_):
            to_near[i].wait_recv()
            on_opposite[i].start()
            to_opposite[i].wait_recv()
            on_near[0][i].start()
            compact_far(1, i)

        return go

    def relay(i):
        def go(_):
            on_opposite[i].wait_recv()
            on_near[1][i].start()

        return go

    def later_line(line, i, waits):
        def go(_):
            if waits:
                on_near[line - 2][i].wait_recv()
            compact_far(line, i)

        return go

    def to_side(_):
        p = place[1]
        both = compacted(across_x, [columns(q), columns(q_y)])
        a_send[0, 0], a_send[0, 1] = both[0]
        a_send[sp_devices // 2, 0], a_send[sp_devices // 2, 1] = both[1]
        for i in range(2):
            a[p][i].start()

    def to_side_more(_):
        for copy in a_extra[place[1]]:
            copy.start()

    def other_picks(_):
        for k in range(2, sp_devices):
            expert = flipped(me, k)
            pick_ref[dynamic_block(expert), :] = one_hot(slots_of(route, expert))

    def arrive(i):
        def go(p):
            (a[p] or close[0])[i].wait_recv()
            if labels[p] != 1:
                b[p][i].start()
            c_near[p][i].start()

        return go

    def cross(i):
        def go(p):
            if labels[p] == 1:
                a_extra[p][i].wait_recv()
            else:
                b[p][i].wait_recv()
            c_far[p][i].start()

        return go

    def gather(p):
        for i in range(2):
            c_near[p][i].wait_recv()
            c_far[p][i].wait_recv()

    def expert(p):
        span = block(p)
        both = jnp.dot(rows[0, span, :], w_pair[...], preferred_element_type=f32)
        gate, up = both[:, :units], both[:, units:]
        d_hidden = lax.dot_general(
            rows[1, span, :], w_down[...], across, preferred_element_type=f32
        )
        sig = jax.nn.sigmoid(gate)
        silu_gate = gate * sig
        hidden[span, :] = (silu_gate * up).astype(bf16)
        d_gate = (d_hidden * up * sig * (1.0 + gate * (1.0 - sig))).astype(bf16)
        d_up = (d_hidden * silu_gate).astype(bf16)
        d_pair[span, pl.ds(0, units)] = d_gate
        d_pair[span, pl.ds(units, units)] = d_up

        def partial(index):
            return lax.dot_general(
                d_pair[span, :], w_pair[columns(index), :], across, preferred_element_type=f32
            ).astype(bf16)

        core_send[1, span, :] = partial(q_far)
        core_send[0, span, :] = partial(q_core)
        core[p][1].start()
        kept[1, span, :] = partial(q_y)
        core[p][0].start()
        kept[0, span, :] = partial(q)

    def reduce_core(p):
        span = block(p)
        core[p][1].wait_recv()
        y_send[span, :] = (
            kept[1, span, :].astype(f32) + core_got[1, span, :].astype(f32)
        ).astype(bf16)
        y_hop[p].start()
        core[p][0].wait_recv()
        near_got[span, :] = kept[0, span, :].astype(f32) + core_got[0, span, :].astype(f32)

    def reduce_y(p):
        span = block(p)
        y_hop[p].wait_recv()
        back_send[span, :] = (near_got[span, :] + y_got[span, :].astype(f32)).astype(bf16)
        if labels[p]:
            back_out[p].start()
        else:
            back_got[dynamic_block(me), :] = back_send[span, :]

    def convolve(p):
        @pl.when(me == 0)
        def _():
            before[pl.ds(0, 8), :] = jnp.zeros((8, before.shape[1]), f32)

        @pl.when(me > 0)
        def _():
            to_next.wait_recv()

        conv = (
            taps_ref[0:1, :] * before[pl.ds(6, tokens), :]
            + taps_ref[1:2, :] * before[pl.ds(7, tokens), :]
            + taps_ref[2:3, :] * before[pl.ds(8, tokens), :]
        )
        conv_out[...] = conv
        mixer_out[...] = (outer_ref[...].astype(f32) * conv).astype(bf16)

    step = 2 * units

    def down(j, carry):
        at = pl.ds(pl.multiple_of(j * step, step), step)
        grad_down_ref[:, at] = lax.dot_general(
            hidden[...], rows[1, :, at], over_rows, preferred_element_type=f32
        ).astype(bf16)
        return carry

    def gate_up(j, carry):
        at = pl.ds(pl.multiple_of(j * units, units), units)
        both = lax.dot_general(
            rows[0, :, at], d_pair[...], over_rows, preferred_element_type=f32
        ).astype(bf16)
        grad_gate_ref[at, :] = both[:, :units]
        grad_up_ref[at, :] = both[:, units:]
        return carry

    def first_gate_up(p):
        lax.fori_loop(0, width // units // 2, gate_up, 0)

    def second_gate_up(p):
        lax.fori_loop(width // units // 2, width // units, gate_up, 0)

    def all_down(p):
        lax.fori_loop(0, width // step, down, 0)

    def follow(steps, waits):
        run = dict(
            a=arrive(0),
            A=arrive(1),
            b=cross(0),
            B=cross(1),
            C=gather,
            E=expert,
            R=reduce_core,
            Y=reduce_y,
            V=convolve,
            G=first_gate_up,
            H=second_gate_up,
            D=all_down,
            w=first_line(0),
            W=first_line(1),
            X=to_side,
            Z=to_side_more,
            P=other_picks,
            J=later_line(2, 0, waits),
            K=later_line(2, 1, waits),
            L=later_line(3, 0, waits),
            M=later_line(3, 1, waits),
            S=relay(0),
            T=relay(1),
        )
        for item in steps.split():
            with scope(item):
                run[item[0]](place.get(int(item[1:] or 0)))

    @pl.when(inside == 0)
    def _():
        follow(outer_steps, True)

    @pl.when(inside == 1)
    def _():
        follow(inner_steps, False)

    for p, label in enumerate(labels):
        if label:
            with scope(f"back{label}"):
                back_in[p].wait_recv()
    share = quarter // per

    def piece_of(index, i):
        return pl.ds(pl.multiple_of(index * quarter + i * per, per), per)

    gathers = []
    for i in range(share):
        part, part_y = stream_grad.at[:, piece_of(q, i)], stream_grad.at[:, piece_of(q_y, i)]
        gathers.append(
            [
                remote(part, part, (gather_sem.at[0, 0, i], gather_sem.at[1, 0, i]), me, t_y),
                remote(part, part, (gather_sem.at[0, 1, i], gather_sem.at[1, 1, i]), me, t_core),
                remote(part_y, part_y, (gather_sem.at[0, 2, i], gather_sem.at[1, 2, i]), me, t_core),
            ]
        )
    sends = []

    def project(j, index, i):
        piece = stream_grad[:, piece_of(index, i)]
        proj_send[j * share + i] = lax.dot_general(
            piece, mixer_out[...], over_rows, preferred_element_type=f32
        ).astype(bf16)
        owner = index * share + i
        send = remote(
            proj_send.at[j * share + i],
            proj_got.at[me],
            (proj_sem.at[0, j * share + i], proj_sem.at[1, me]),
            owner,
            t,
        )

        @pl.when(owner != me)
        def _():
            send.start()

        @pl.when(owner == me)
        def _():
            proj_got[me] = proj_send[j * share + i]

        sends.append((owner, send))
        return jnp.dot(piece, out_proj_ref[piece_of(index, i), :], preferred_element_type=f32)

    for i in range(share):
        at = piece_of(q, i)
        moe_grad = lax.dot_general(
            pick_ref[...],
            back_got[:, pl.ds(i * per, per)],
            over_rows,
            preferred_element_type=f32,
        )
        stream_grad[:, at] = (cot_ref[:, at].astype(f32) + moe_grad).astype(bf16)
        gathers[i][0].start()
        gathers[i][1].start()
    d_mixer = project(0, q, 0)
    for i in range(1, share):
        d_mixer = d_mixer + project(0, q, i)
    for i in range(share):
        with scope(f"g1{i}"):
            gathers[i][1].wait_recv()
        d_mixer = d_mixer + project(1, q_core, i)
    for i in range(share):
        with scope(f"g0{i}"):
            gathers[i][0].wait_recv()
        gathers[i][2].start()
        d_mixer = d_mixer + project(2, q_y, i)
        with scope(f"g2{i}"):
            gathers[i][2].wait_recv()
        d_mixer = d_mixer + project(3, q_far, i)

    d_conv = d_mixer * outer_ref[...].astype(f32)
    after[pl.ds(0, tokens), :] = d_conv
    grad_outer_ref[...] = d_mixer * conv_out[...]

    @pl.when(me > 0)
    def _():
        to_previous.start()

    @pl.when(me == sp_devices - 1)
    def _():
        after[pl.ds(tokens, 8), :] = jnp.zeros((8, after.shape[1]), f32)

    with scope("prevw"):

        @pl.when(me < sp_devices - 1)
        def _():
            to_previous.wait_recv()

    d_mixed = (
        taps_ref[2:3, :] * after[pl.ds(0, tokens), :]
        + taps_ref[1:2, :] * after[pl.ds(1, tokens), :]
        + taps_ref[0:1, :] * after[pl.ds(2, tokens), :]
    )
    grad_inner_ref[...] = d_mixed * input_ref[...].astype(f32)
    grad_input_ref[...] = d_mixed * inner_ref[...].astype(f32)

    for k in others:
        source = flipped(me, k)
        with scope(f"pw{k}"):
            remote(
                proj_send.at[0],
                proj_got.at[source],
                (proj_sem.at[0, 0], proj_sem.at[1, source]),
                source,
                t,
            ).wait_recv()
    total = proj_got[0].astype(f32)
    for s in range(1, sp_devices):
        total = total + proj_got[s].astype(f32)
    grad_proj_ref[...] = total

    for label in others:
        p = place[label]
        for copy in (a[p] if label != 3 else []) + a_extra[p] + c_near[p] + c_far[p]:
            copy.wait_send()
        for copy in b[p] if label > 1 else []:
            copy.wait_send()
        back_out[p].wait_send()
    for copy in route_out:
        copy.wait_send()

    @pl.when(inside == 0)
    def _():
        for copy in to_near:
            copy.wait_send()
        route_in[0].wait_recv()

    @pl.when(inside == 1)
    def _():
        for copy in a[place[3]] + to_opposite + on_opposite + on_near[0] + on_near[1]:
            copy.wait_send()
        for copy in close[0] + close[1]:
            copy.wait_send()

    for p in range(len(labels)):
        core[p][0].wait_send()
        core[p][1].wait_send()
        y_hop[p].wait_send()
    for copies in gathers:
        for copy in copies:
            copy.wait_send()
    for owner, send in sends:

        @pl.when(owner != me)
        def _():
            send.wait_send()

    @pl.when(me < sp_devices - 1)
    def _():
        to_next.wait_send()

    @pl.when(me > 0)
    def _():
        to_previous.wait_send()


def written(*refs):
    count = (len(refs) - 1) // 2
    sem = refs[-1]
    outs = [
        pltpu.make_async_copy(refs[i], refs[count + i], sem.at[i]) for i in range(count)
    ]
    for out in outs:
        out.start()
    for out in outs:
        out.wait()


def fused_shards(
    out_cotangent,
    stream,
    route_ids,
    route_weights,
    gate_proj,
    up_proj,
    down_proj,
    outer_gate,
    inner_gate,
    conv_input,
    conv_taps,
    out_proj,
):
    f32, bf16 = jnp.float32, jnp.bfloat16
    n = lax.axis_size("sp")
    tokens, width = stream.shape
    units = gate_proj.shape[2]
    channels = out_proj.shape[1]
    capacity = 4 * tokens // n
    slots = n * capacity
    quarter = width // lax.axis_size("tp")
    per = width // n
    labels = [0, 1, 2, 3, 4, 5, 6, 7]
    outer_steps = (
        "X Z E0 R0 a2 A2 b2 a3 B2 A3 C2 E2 R2 J Y0 V P b3 B3 C3 E3 R3 K Y2 a1 A1 a5 b1 B1 C1 E1"
        " L A5 b4 B4 C4 E4 R4 a7 M Y3 b5 B5 C5 E5 R5 Y4 A7 R1 b6 B6 C6 E6 R6 Y5 Y1"
        " b7 B7 C7 E7 R7 Y6 Y7 G H D"
    )
    inner_steps = (
        "E0 R0 w J W K X a3 a5 b2 B2 S L A3 A5 C2 E2 R2 Y0 V P T M Z b4 B4 C4 E4 R4 a7"
        " b3 B3 C3 E3 R3 Y2 A7 b5 B5 C5 E5 R5 Y4 a1 A1 b6 B6 C6 E6 R6 Y3 b1 B1 C1 E1 R1 Y5"
        " b7 B7 C7 E7 R7 Y6 Y1 Y7 G H D"
    )
    vmem = pl.BlockSpec(memory_space=pltpu.VMEM)
    hbm = pl.BlockSpec(memory_space=pltpu.HBM)
    anywhere = pl.BlockSpec(memory_space=pl.ANY)
    dma = pltpu.SemaphoreType.DMA
    shapes = [
        ((width, units), bf16),
        ((width, units), bf16),
        ((units, width), bf16),
        ((per, channels), f32),
        ((tokens, channels), f32),
        ((tokens, channels), f32),
        ((tokens, channels), f32),
    ]
    args = (
        out_cotangent,
        stream,
        route_ids.T,
        route_weights.T,
        outer_gate,
        inner_gate,
        conv_input,
        conv_taps,
        out_proj,
        gate_proj[0],
        up_proj[0],
        down_proj[0],
    )
    grads = pl.pallas_call(
        functools.partial(fused, n, labels, outer_steps, inner_steps),
        out_shape=[pltpu.VMEM(*shape) for shape in shapes],
        in_specs=[hbm] * 12,
        out_specs=[vmem] * 7,
        scratch_shapes=[
            pltpu.VMEM((tokens, width), bf16),
            pltpu.VMEM((tokens, width), bf16),
            pltpu.VMEM(route_ids.shape[::-1], jnp.int32),
            pltpu.VMEM(route_ids.shape[::-1], f32),
            pltpu.VMEM((tokens, channels), bf16),
            pltpu.VMEM((tokens, channels), bf16),
            pltpu.VMEM((tokens, channels), bf16),
            pltpu.VMEM(conv_taps.shape, f32),
            pltpu.VMEM((width, channels), bf16),
            pltpu.VMEM((2, n, tokens), f32),
            pltpu.VMEM((3, 2, n, tokens), f32),
            pltpu.VMEM((3, 2, capacity, tokens), bf16),
            pltpu.VMEM((slots, tokens), bf16),
            pltpu.VMEM((3, 2, tokens, quarter), bf16),
            pltpu.VMEM((2, slots, width), bf16),
            pltpu.VMEM((n // 2 + 1, 2, capacity, quarter), bf16),
            pltpu.VMEM((2, 2, capacity, quarter), bf16),
            pltpu.VMEM((width, 2 * units), bf16),
            pltpu.VMEM((units, width), bf16),
            pltpu.VMEM((slots, units), bf16),
            pltpu.VMEM((slots, 2 * units), bf16),
            pltpu.VMEM((2, slots, quarter), bf16),
            pltpu.VMEM((slots, quarter), f32),
            pltpu.VMEM((2, slots, quarter), bf16),
            pltpu.VMEM((2, slots, quarter), bf16),
            pltpu.VMEM((slots, quarter), bf16),
            pltpu.VMEM((slots, quarter), bf16),
            pltpu.VMEM((slots, quarter), bf16),
            pltpu.VMEM((slots, quarter), bf16),
            pltpu.VMEM((tokens, width), bf16),
            pltpu.VMEM((n, per, channels), bf16),
            pltpu.VMEM((n, per, channels), bf16),
            pltpu.VMEM((tokens + 8, channels), f32),
            pltpu.VMEM((tokens + 8, channels), f32),
            pltpu.VMEM((tokens, channels), f32),
            pltpu.VMEM((tokens, channels), bf16),
            dma((12,)),
            dma((2, 3)),
            dma((8, 2)),
            dma((2, 2)),
            dma((2, 2, n)),
            dma((2, 2, n)),
            dma((4, 2, n)),
            dma((2, 2, n)),
            dma((2, n)),
            dma((2, n)),
            dma((2, 3, quarter // per)),
            dma((2, n)),
            dma((4,)),
        ],
        compiler_params=pltpu.CompilerParams(
            collective_id=0, has_side_effects=True, vmem_limit_bytes=48 * 1024 * 1024
        ),
    )(*(pltpu.with_memory_space_constraint(arg, pltpu.HBM) for arg in args))
    outs = pl.pallas_call(
        written,
        out_shape=[jax.ShapeDtypeStruct(*shape) for shape in shapes],
        in_specs=[anywhere] * 7,
        out_specs=[hbm] * 7,
        scratch_shapes=[dma((7,))],
        compiler_params=pltpu.CompilerParams(vmem_limit_bytes=1024 * 1024),
    )(*(pltpu.with_memory_space_constraint(grad, pltpu.VMEM) for grad in grads))
    return (outs[0][None], outs[1][None], outs[2][None], *outs[3:])


def fits_kernel(mesh):
    return mesh.shape["sp"] == 8 and mesh.shape["tp"] == 4


def solution(mesh):
    placed = (
        P("sp", None),
        P("sp", None),
        P("sp", None),
        P("sp", None),
        P("sp", None, "tp"),
        P("sp", None, "tp"),
        P("sp", "tp", None),
        P("sp", "tp"),
        P("sp", "tp"),
        P("sp", "tp"),
        P(None, "tp"),
        P(None, "tp"),
    )
    return jax.shard_map(
        fused_shards if fits_kernel(mesh) else shards,
        mesh=mesh,
        in_specs=placed,
        out_specs=(
            P("sp", None, "tp"),
            P("sp", None, "tp"),
            P("sp", "tp", None),
            P("sp", "tp"),
            P("sp", "tp"),
            P("sp", "tp"),
            P("sp", "tp"),
        ),
        check_vma=False,
    )
```

```python
import functools

import jax
import jax.numpy as jnp
from jax import lax
from jax.experimental import pallas as pl
from jax.experimental.pallas import tpu as pltpu
from jax.sharding import PartitionSpec as P


def passed_along(x, axis, by):
    devices = lax.axis_size(axis)
    pairs = [(i, i + by) for i in range(devices) if 0 <= i + by < devices]
    return lax.ppermute(x, axis, pairs)


def to_owners(x, devices):
    blocks = x.reshape(devices, -1, x.shape[1])
    return lax.all_to_all(blocks, "sp", split_axis=0, concat_axis=0, tiled=True).reshape(x.shape)


def partial_rows(d_gate, d_up, w_gate, w_up):
    across = (((1,), (1,)), ((), ()))
    total = lax.dot_general(
        d_gate, w_gate, across, preferred_element_type=jnp.float32
    ) + lax.dot_general(d_up, w_up, across, preferred_element_type=jnp.float32)
    return total.astype(jnp.bfloat16)


def reduced_quarter(d_gate, d_up, w_gate, w_up):
    devices = lax.axis_size("tp")
    if devices != 4:
        return lax.psum_scatter(
            partial_rows(d_gate, d_up, w_gate, w_up), "tp", scatter_dimension=1, tiled=True
        )
    quarter = w_gate.shape[0] // devices
    me = lax.axis_index("tp")

    def rows_of(w, *flips):
        return jnp.concatenate(
            [lax.dynamic_slice_in_dim(w, (me ^ flip) * quarter, quarter, 0) for flip in flips]
        )

    def swapped(x, flip):
        return lax.ppermute(x, "tp", [(i, i ^ flip) for i in range(devices)])

    sent = partial_rows(d_gate, d_up, rows_of(w_gate, 1, 3), rows_of(w_up, 1, 3))
    got = swapped(sent, 1)
    kept = partial_rows(d_gate, d_up, rows_of(w_gate, 0, 2), rows_of(w_up, 0, 2))
    far = kept[:, quarter:].astype(jnp.float32) + got[:, quarter:].astype(jnp.float32)
    near = kept[:, :quarter].astype(jnp.float32) + got[:, :quarter].astype(jnp.float32)
    other = swapped(far.astype(jnp.bfloat16), 2)
    return (near + other.astype(jnp.float32)).astype(jnp.bfloat16)


def shards(
    out_cotangent,
    stream,
    route_ids,
    route_weights,
    gate_proj,
    up_proj,
    down_proj,
    outer_gate,
    inner_gate,
    conv_input,
    conv_taps,
    out_proj,
):
    sp_devices = lax.axis_size("sp")
    tokens_here, width = stream.shape
    experts = sp_devices * gate_proj.shape[0]
    capacity = 4 * tokens_here // experts
    quarter = width // lax.axis_size("tp")
    first_column = lax.axis_index("tp") * quarter
    own_cotangent = lax.dynamic_slice_in_dim(out_cotangent, first_column, quarter, 1)
    own_stream = lax.dynamic_slice_in_dim(stream, first_column, quarter, 1)
    over_rows = (((0,), (0,)), ((), ()))
    expert_ids = jnp.arange(experts, dtype=jnp.int32)
    chosen = route_ids[:, :, None] == expert_ids
    hit = jnp.any(chosen, axis=1)
    token_weight = jnp.sum(jnp.where(chosen, route_weights[:, :, None], 0.0), axis=1)
    token_ids = jnp.arange(tokens_here, dtype=jnp.int32)
    below = (token_ids[:, None] < token_ids[None, :]).astype(jnp.bfloat16)
    rank = lax.dot_general(
        hit.astype(jnp.bfloat16), below, over_rows, preferred_element_type=jnp.float32
    )
    rank = jnp.where(hit.T, rank, -1.0)
    in_slot = rank[:, None, :] == jnp.arange(capacity, dtype=jnp.float32)[None, :, None]
    slot_weight = jnp.sum(jnp.where(in_slot, token_weight.T[:, None, :], 0.0), axis=2)
    pick = in_slot.astype(jnp.bfloat16).reshape(experts * capacity, tokens_here)
    send_input = jnp.dot(pick, own_stream, preferred_element_type=jnp.float32).astype(jnp.bfloat16)
    send_grad = (
        slot_weight.reshape(-1, 1)
        * jnp.dot(pick, own_cotangent, preferred_element_type=jnp.float32)
    ).astype(jnp.bfloat16)
    got_input = to_owners(send_input, sp_devices)
    rows_input = lax.all_gather(got_input, "tp", axis=1, tiled=True)
    send_grad, got_input = lax.optimization_barrier((send_grad, got_input))
    got_grad = to_owners(send_grad, sp_devices)
    rows_grad = lax.all_gather(got_grad, "tp", axis=1, tiled=True)
    mixed = inner_gate.astype(jnp.float32) * conv_input.astype(jnp.float32)
    previous = passed_along(mixed[tokens_here - 2 :], "sp", 1)
    extended = jnp.concatenate([previous, mixed], axis=0)
    conv_out = (
        conv_taps[0] * extended[:tokens_here]
        + conv_taps[1] * extended[1 : tokens_here + 1]
        + conv_taps[2] * extended[2:]
    )
    mixer_out = (outer_gate.astype(jnp.float32) * conv_out).astype(jnp.bfloat16)
    conv_out, mixer_out, rows_grad = lax.optimization_barrier((conv_out, mixer_out, rows_grad))
    w_gate = gate_proj[0]
    w_up = up_proj[0]
    w_down = down_proj[0]
    gate = jnp.dot(rows_input, w_gate, preferred_element_type=jnp.float32)
    up = jnp.dot(rows_input, w_up, preferred_element_type=jnp.float32)
    sig = jax.nn.sigmoid(gate)
    silu_gate = gate * sig
    hidden = (silu_gate * up).astype(jnp.bfloat16)
    across = (((1,), (1,)), ((), ()))
    d_hidden = lax.dot_general(rows_grad, w_down, across, preferred_element_type=jnp.float32)
    d_gate = (d_hidden * up * sig * (1.0 + gate * (1.0 - sig))).astype(jnp.bfloat16)
    d_up = (d_hidden * silu_gate).astype(jnp.bfloat16)
    grad_down = lax.dot_general(
        hidden, rows_grad, over_rows, preferred_element_type=jnp.float32
    ).astype(jnp.bfloat16)
    grad_gate = lax.dot_general(
        rows_input, d_gate, over_rows, preferred_element_type=jnp.float32
    ).astype(jnp.bfloat16)
    grad_up = lax.dot_general(
        rows_input, d_up, over_rows, preferred_element_type=jnp.float32
    ).astype(jnp.bfloat16)
    chunks = 2
    piece = capacity // chunks
    shape = (sp_devices, chunks, piece, d_gate.shape[1])
    gate_pieces = d_gate.reshape(shape)
    up_pieces = d_up.reshape(shape)
    shares = []
    for c in range(chunks):
        shares.append(
            reduced_quarter(
                gate_pieces[:, c].reshape(-1, shape[3]),
                up_pieces[:, c].reshape(-1, shape[3]),
                w_gate,
                w_up,
            )
        )
    shares[0], grad_down, grad_gate, grad_up = lax.optimization_barrier(
        (shares[0], grad_down, grad_gate, grad_up)
    )
    moe_grad = own_cotangent.astype(jnp.float32)
    pick_pieces = pick.reshape(experts, chunks, piece, tokens_here)
    for c in range(chunks):
        returned = to_owners(shares[c], sp_devices)
        moe_grad = moe_grad + lax.dot_general(
            pick_pieces[:, c].reshape(-1, tokens_here), returned, over_rows,
            preferred_element_type=jnp.float32,
        )
    stream_part = moe_grad.astype(jnp.bfloat16)
    stream_grad = lax.all_gather(stream_part, "tp", axis=1, tiled=True)
    own_projection = lax.dot_general(
        stream_grad, mixer_out, over_rows, preferred_element_type=jnp.float32
    ).astype(jnp.bfloat16)
    projections = to_owners(own_projection, sp_devices)
    grad_projection = jnp.sum(
        projections.astype(jnp.float32).reshape(sp_devices, -1, projections.shape[1]), axis=0
    )
    d_mixer = jnp.dot(stream_grad, out_proj, preferred_element_type=jnp.float32)
    grad_outer = d_mixer * conv_out
    d_conv = d_mixer * outer_gate.astype(jnp.float32)
    following = passed_along(d_conv[:2], "sp", -1)
    trailing = jnp.concatenate([d_conv, following], axis=0)
    d_mixed = (
        conv_taps[2] * trailing[:tokens_here]
        + conv_taps[1] * trailing[1 : tokens_here + 1]
        + conv_taps[0] * trailing[2:]
    )
    grad_inner = d_mixed * conv_input.astype(jnp.float32)
    grad_input = d_mixed * inner_gate.astype(jnp.float32)
    return (
        grad_gate[None],
        grad_up[None],
        grad_down[None],
        grad_projection,
        grad_outer,
        grad_inner,
        grad_input,
    )


MESH = pl.DeviceIdType.MESH


def flipped(index, flips):
    place = 1
    while place <= flips:
        if (flips // place) % 2:
            index = index + place * (1 - 2 * ((index // place) % 2))
        place *= 2
    return index


def fused(
    sp_devices,
    labels,
    outer_steps,
    inner_steps,
    cot_hbm,
    stream_hbm,
    ids_hbm,
    weights_hbm,
    outer_hbm,
    inner_hbm,
    input_hbm,
    taps_hbm,
    out_proj_hbm,
    w_gate_hbm,
    w_up_hbm,
    w_down_hbm,
    grad_gate_ref,
    grad_up_ref,
    grad_down_ref,
    grad_proj_ref,
    grad_outer_ref,
    grad_inner_ref,
    grad_input_ref,
    cot_ref,
    stream_ref,
    ids_ref,
    weights_ref,
    outer_ref,
    inner_ref,
    input_ref,
    taps_ref,
    out_proj_ref,
    route,
    far_route,
    far_pick,
    pick_ref,
    raw,
    rows,
    a_send,
    close_send,
    extra_send,
    w_pair,
    w_down,
    hidden,
    d_pair,
    kept,
    near_got,
    core_send,
    core_got,
    y_send,
    y_got,
    back_send,
    back_got,
    stream_grad,
    proj_send,
    proj_got,
    before,
    after,
    conv_out,
    mixer_out,
    load_sem,
    route_sem,
    raw_sem,
    close_sem,
    extra_sem,
    a_sem,
    b_sem,
    c_sem,
    core_sem,
    y_sem,
    back_sem,
    gather_sem,
    proj_sem,
    conv_sem,
):
    f32, bf16 = jnp.float32, jnp.bfloat16
    scope = jax.named_scope
    me = lax.axis_index("sp")
    t = lax.axis_index("tp")
    t_core, t_y = flipped(t, 1), flipped(t, 2)
    half = lax.axis_size("tp") // 2
    tokens, width = stream_ref.shape
    capacity = pick_ref.shape[0] // sp_devices
    units = hidden.shape[1]
    quarter = width // lax.axis_size("tp")
    per = width // sp_devices
    over_rows = (((0,), (0,)), ((), ()))
    across = (((1,), (1,)), ((), ()))
    others = range(1, sp_devices)

    def owned(member):
        return (member % 2) * half + member // 2

    q, q_core, q_y, q_far = owned(t), owned(t_core), owned(t_y), owned(flipped(t, 3))

    def columns(index):
        return pl.ds(pl.multiple_of(index * quarter, quarter), quarter)

    def block(p):
        return pl.ds(p * capacity, capacity)

    def dynamic_block(p):
        return pl.ds(pl.multiple_of(p * capacity, capacity), capacity)

    def remote(src, dst, sems, sp, tp):
        return pltpu.make_async_remote_copy(
            src_ref=src,
            dst_ref=dst,
            send_sem=sems[0],
            recv_sem=sems[1],
            device_id=(sp, tp),
            device_id_type=MESH,
        )

    peers = [(flipped(me, k), t) for k in others] + [(me, t_core), (me, t_y)]
    barrier = pltpu.get_barrier_semaphore()
    for peer in peers:
        pl.semaphore_signal(barrier, inc=1, device_id=peer, device_id_type=MESH)

    moved = [
        (ids_hbm, ids_ref),
        (weights_hbm, weights_ref),
        (inner_hbm, inner_ref),
        (input_hbm, input_ref),
        (stream_hbm, stream_ref),
        (cot_hbm, cot_ref),
        (w_gate_hbm, w_pair.at[:, pl.ds(0, units)]),
        (w_up_hbm, w_pair.at[:, pl.ds(units, units)]),
        (w_down_hbm, w_down),
        (outer_hbm, outer_ref),
        (taps_hbm, taps_ref),
        (out_proj_hbm, out_proj_ref),
    ]
    loads = [
        pltpu.make_async_copy(src, dst, load_sem.at[i]) for i, (src, dst) in enumerate(moved)
    ]
    for load in loads:
        load.start()

    with scope("prep"):
        for load in loads[:4]:
            load.wait()
        before[pl.ds(8, tokens), :] = inner_ref[...].astype(f32) * input_ref[...].astype(f32)
        expert_ids = lax.broadcasted_iota(jnp.int32, (sp_devices, tokens), 0)
        chosen = [ids_ref[j : j + 1, :] == expert_ids for j in range(ids_ref.shape[0])]
        hit = jnp.zeros((sp_devices, tokens), f32)
        weight = jnp.zeros((sp_devices, tokens), f32)
        for j, choice in enumerate(chosen):
            hit = jnp.where(choice, 1.0, hit)
            weight = jnp.where(choice, weights_ref[j : j + 1, :], weight)
        earlier = lax.broadcasted_iota(jnp.int32, (tokens, tokens), 0)
        later = lax.broadcasted_iota(jnp.int32, (tokens, tokens), 1)
        below = jnp.where(earlier < later, 1.0, 0.0).astype(bf16)
        rank = jnp.dot(hit.astype(bf16), below, preferred_element_type=f32)
        route[0] = jnp.where(hit > 0.0, rank, -1.0)
        route[1] = weight
        slot = lax.broadcasted_iota(jnp.int32, (capacity, tokens), 0).astype(f32)

    def slots_of(ref, expert):
        return ref[0, pl.ds(expert, 1), :] == slot

    def one_hot(chosen_slot):
        return jnp.where(chosen_slot, 1.0, 0.0).astype(bf16)

    def scale_of(ref, expert, chosen_slot):
        return jnp.sum(
            jnp.where(chosen_slot, ref[1, pl.ds(expert, 1), :], 0.0), axis=1, keepdims=True
        )

    def compacted(expert, ranges):
        chosen_slot = slots_of(route, expert)
        pick = one_hot(chosen_slot)
        pick_ref[dynamic_block(expert), :] = pick
        scale = scale_of(route, expert, chosen_slot)
        return [
            (
                jnp.dot(pick, stream_ref[:, at], preferred_element_type=f32).astype(bf16),
                (scale * jnp.dot(pick, cot_ref[:, at], preferred_element_type=f32)).astype(bf16),
            )
            for at in ranges
        ]

    z, side = me // 2, me % 2
    upper = z // 2
    inside = (z + upper) % 2
    across_x, near, opposite = flipped(me, 1), flipped(me, 2), flipped(me, 6)
    lines = [z, z + 1 - 2 * (z % 2), 2 - upper, 3 - 3 * upper]
    place = {label: p for p, label in enumerate(labels)}
    a, a_extra, b, c_near, c_far, back_out, back_in, partners = {}, {}, {}, {}, {}, {}, {}, {}
    for label in range(sp_devices):
        p = place[label]
        across_side = 1 - side if label % 2 else side
        partner = partners[p] = 2 * lines[label // 2] + across_side
        a[p], a_extra[p], b[p], c_near[p], c_far[p] = [], [], [], [], []
        for i in range(2):
            mine, theirs = rows.at[i, block(p), columns(q)], rows.at[i, block(p), columns(q_y)]
            if label % 2:
                a[p].append(
                    remote(
                        a_send.at[label // 2, i],
                        mine,
                        (a_sem.at[0, i, p], a_sem.at[1, i, p]),
                        across_x,
                        t,
                    )
                )
            if label == 1:
                a_extra[p].append(
                    remote(
                        a_send.at[sp_devices // 2, i],
                        theirs,
                        (a_sem.at[0, i, 0], a_sem.at[1, i, 0]),
                        across_x,
                        t,
                    )
                )
            b[p].append(remote(mine, mine, (b_sem.at[0, i, p], b_sem.at[1, i, p]), me, t_y))
            c_near[p].append(
                remote(mine, mine, (c_sem.at[0, i, p], c_sem.at[1, i, p]), me, t_core)
            )
            c_far[p].append(
                remote(theirs, theirs, (c_sem.at[2, i, p], c_sem.at[3, i, p]), me, t_core)
            )
        back_out[p] = remote(
            back_send.at[block(p)],
            back_got.at[dynamic_block(me)],
            (back_sem.at[0, p], back_sem.at[1, me]),
            partner,
            t,
        )
        back_in[p] = remote(
            back_send.at[block(p)],
            back_got.at[dynamic_block(partner)],
            (back_sem.at[0, p], back_sem.at[1, partner]),
            partner,
            t,
        )
    close = [
        [
            remote(
                close_send.at[j, i],
                rows.at[i, block(place[2 + j]), columns(q)],
                (close_sem.at[j, i], a_sem.at[1, i, place[2 + j]]),
                flipped(me, 2 + j),
                t,
            )
            for i in range(2)
        ]
        for j in range(2)
    ]
    extra_out, extra_in = (
        [
            [
                remote(
                    extra_send.at[j, i],
                    rows.at[i, block(place[2 + j]), columns(q_y)],
                    (extra_sem.at[j, i], b_sem.at[1, i, place[2 + j]]),
                    flipped(me, 2 + j),
                    t,
                )
                for i in range(2)
            ]
            for j in range(2)
        ]
        for _ in range(2)
    )
    to_near, to_opposite, on_opposite, on_near = [], [], [], [[], []]
    for i, ref in enumerate((stream_ref, cot_ref)):
        own = ref.at[:, columns(q)]
        to_near.append(
            remote(own, raw.at[0, i], (raw_sem.at[0, i], raw_sem.at[5, i]), near, t)
        )
        to_opposite.append(
            remote(own, raw.at[1, i], (raw_sem.at[1, i], raw_sem.at[6, i]), opposite, t)
        )
        on_opposite.append(
            remote(raw.at[0, i], raw.at[2, i], (raw_sem.at[2, i], raw_sem.at[7, i]), opposite, t)
        )
        for j in range(2):
            on_near[j].append(
                remote(
                    raw.at[1 + j, i],
                    raw.at[1 + j, i],
                    (raw_sem.at[3 + j, i], raw_sem.at[6 + j, i]),
                    near,
                    t,
                )
            )
    as_far = 2 - inside
    route_out = [
        remote(route, far_route.at[0], (route_sem.at[0, 0], route_sem.at[1, 0]), near, t)
    ] + [
        remote(
            route,
            far_route.at[as_far],
            (route_sem.at[0, j], route_sem.at[1, as_far]),
            flipped(me, 2 + 2 * j),
            t,
        )
        for j in (1, 2)
    ]
    route_in = [
        remote(route, far_route.at[j], (route_sem.at[0, j], route_sem.at[1, j]), near, t)
        for j in range(3)
    ]
    to_next = remote(
        before.at[pl.ds(tokens, 8)],
        before.at[pl.ds(0, 8)],
        (conv_sem.at[0], conv_sem.at[1]),
        me + 1,
        t,
    )
    to_previous = remote(
        after.at[pl.ds(0, 8)],
        after.at[pl.ds(tokens, 8)],
        (conv_sem.at[2], conv_sem.at[3]),
        me - 1,
        t,
    )

    with scope("barrier"):
        pl.semaphore_wait(barrier, len(peers))
    for out in route_out:
        out.start()

    @pl.when(me < sp_devices - 1)
    def _():
        to_next.start()

    for i in range(2):
        loads[4 + i].wait()

        @pl.when(inside == 0)
        def _():
            to_near[i].start()

        @pl.when(inside == 1)
        def _():
            to_opposite[i].start()

    @pl.when(inside == 1)
    def _():
        for j in (1, 0):
            close_send[j, 0], close_send[j, 1] = compacted(flipped(me, 2 + j), [columns(q)])[0]
            for i in range(2):
                close[j][i].start()

    own = compacted(me, [pl.ds(0, width)])[0]
    rows[0, block(place[0]), :], rows[1, block(place[0]), :] = own
    for load in loads[6:]:
        load.wait()

    core, y_hop = {}, {}
    for p in range(len(labels)):
        core[p] = [
            remote(
                core_send.at[i, block(p)],
                core_got.at[i, block(p)],
                (core_sem.at[0, i, p], core_sem.at[1, i, p]),
                me,
                t_core,
            )
            for i in range(2)
        ]
        y_hop[p] = remote(
            y_send.at[block(p)], y_got.at[block(p)], (y_sem.at[0, p], y_sem.at[1, p]), me, t_y
        )

    def compact_far(line, i, direct):
        far = far_route.at[line - 1]
        if i == 0:
            route_in[line - 1].wait_recv()
        for j, expert in enumerate((me, across_x)):
            chosen_slot = slots_of(far, expert)
            if i == 0:
                pick = one_hot(chosen_slot)
                far_pick[line - 1, j] = pick
            else:
                pick = far_pick[line - 1, j]
            part = jnp.dot(pick, raw[line - 1, i], preferred_element_type=f32)
            if i:
                part = scale_of(far, expert, chosen_slot) * part
            p = place[2 * line + j]
            if j:
                a_send[line, i] = part.astype(bf16)
                a[p][i].start()
            else:
                rows[i, block(p), columns(q)] = part.astype(bf16)
                if 2 * line not in direct:
                    b[p][i].start()
                c_near[p][i].start()

    def first_line(i, direct):
        def go(_):
            to_near[i].wait_recv()
            on_opposite[i].start()
            to_opposite[i].wait_recv()
            on_near[0][i].start()
            compact_far(1, i, direct)

        return go

    def relay(i):
        def go(_):
            on_opposite[i].wait_recv()
            on_near[1][i].start()

        return go

    def later_line(line, i, waits):
        def go(_):
            if waits:
                on_near[line - 2][i].wait_recv()
            compact_far(line, i, ())

        return go

    def to_side(_):
        p = place[1]
        both = compacted(across_x, [columns(q), columns(q_y)])
        a_send[0, 0], a_send[0, 1] = both[0]
        a_send[sp_devices // 2, 0], a_send[sp_devices // 2, 1] = both[1]
        for i in range(2):
            a[p][i].start()

    def to_side_more(_):
        for copy in a_extra[place[1]]:
            copy.start()

    def other_picks(_):
        for k in range(2, sp_devices):
            expert = flipped(me, k)
            pick_ref[dynamic_block(expert), :] = one_hot(slots_of(route, expert))

    def to_close_more(j):
        def go(_):
            extra_send[j, 0], extra_send[j, 1] = compacted(flipped(me, 2 + j), [columns(q_y)])[0]
            for copy in extra_out[j]:
                copy.start()

        return go

    def arrive(i, direct):
        def go(p):
            (a[p] or close[0])[i].wait_recv()
            if labels[p] not in direct:
                b[p][i].start()
            c_near[p][i].start()

        return go

    def cross(i, direct):
        def go(p):
            if labels[p] == 1:
                a_extra[p][i].wait_recv()
            elif labels[p] in direct:
                extra_in[labels[p] - 2][i].wait_recv()
            else:
                b[p][i].wait_recv()
            c_far[p][i].start()

        return go

    def gather(p):
        for i in range(2):
            c_near[p][i].wait_recv()
            c_far[p][i].wait_recv()

    def expert(p):
        span = block(p)
        both = jnp.dot(rows[0, span, :], w_pair[...], preferred_element_type=f32)
        gate, up = both[:, :units], both[:, units:]
        d_hidden = lax.dot_general(
            rows[1, span, :], w_down[...], across, preferred_element_type=f32
        )
        sig = jax.nn.sigmoid(gate)
        silu_gate = gate * sig
        hidden[span, :] = (silu_gate * up).astype(bf16)
        d_gate = (d_hidden * up * sig * (1.0 + gate * (1.0 - sig))).astype(bf16)
        d_up = (d_hidden * silu_gate).astype(bf16)
        d_pair[span, pl.ds(0, units)] = d_gate
        d_pair[span, pl.ds(units, units)] = d_up

        def partial(index):
            return lax.dot_general(
                d_pair[span, :], w_pair[columns(index), :], across, preferred_element_type=f32
            ).astype(bf16)

        core_send[1, span, :] = partial(q_far)
        core_send[0, span, :] = partial(q_core)
        core[p][1].start()
        kept[1, span, :] = partial(q_y)
        core[p][0].start()
        kept[0, span, :] = partial(q)

    def reduce_core(p):
        span = block(p)
        core[p][1].wait_recv()
        y_send[span, :] = (
            kept[1, span, :].astype(f32) + core_got[1, span, :].astype(f32)
        ).astype(bf16)
        y_hop[p].start()
        core[p][0].wait_recv()
        near_got[span, :] = kept[0, span, :].astype(f32) + core_got[0, span, :].astype(f32)

    def reduce_y(p):
        span = block(p)
        y_hop[p].wait_recv()
        back_send[span, :] = (near_got[span, :] + y_got[span, :].astype(f32)).astype(bf16)
        if labels[p]:
            back_out[p].start()
        else:
            back_got[dynamic_block(me), :] = back_send[span, :]

    def convolve(p):
        @pl.when(me == 0)
        def _():
            before[pl.ds(0, 8), :] = jnp.zeros((8, before.shape[1]), f32)

        @pl.when(me > 0)
        def _():
            to_next.wait_recv()

        conv = (
            taps_ref[0:1, :] * before[pl.ds(6, tokens), :]
            + taps_ref[1:2, :] * before[pl.ds(7, tokens), :]
            + taps_ref[2:3, :] * before[pl.ds(8, tokens), :]
        )
        conv_out[...] = conv
        mixer_out[...] = (outer_ref[...].astype(f32) * conv).astype(bf16)

    step = 2 * units

    def down(j, carry):
        at = pl.ds(pl.multiple_of(j * step, step), step)
        grad_down_ref[:, at] = lax.dot_general(
            hidden[...], rows[1, :, at], over_rows, preferred_element_type=f32
        ).astype(bf16)
        return carry

    def gate_up(j, carry):
        at = pl.ds(pl.multiple_of(j * units, units), units)
        both = lax.dot_general(
            rows[0, :, at], d_pair[...], over_rows, preferred_element_type=f32
        ).astype(bf16)
        grad_gate_ref[at, :] = both[:, :units]
        grad_up_ref[at, :] = both[:, units:]
        return carry

    def first_gate_up(p):
        lax.fori_loop(0, width // units // 2, gate_up, 0)

    def second_gate_up(p):
        lax.fori_loop(width // units // 2, width // units, gate_up, 0)

    def all_down(p):
        lax.fori_loop(0, width // step, down, 0)

    def follow(steps, waits, direct):
        run = dict(
            a=arrive(0, direct),
            A=arrive(1, direct),
            b=cross(0, direct),
            B=cross(1, direct),
            C=gather,
            E=expert,
            R=reduce_core,
            Y=reduce_y,
            V=convolve,
            G=first_gate_up,
            H=second_gate_up,
            D=all_down,
            w=first_line(0, direct),
            W=first_line(1, direct),
            U=to_close_more(0),
            u=to_close_more(1),
            X=to_side,
            Z=to_side_more,
            P=other_picks,
            J=later_line(2, 0, waits),
            K=later_line(2, 1, waits),
            L=later_line(3, 0, waits),
            M=later_line(3, 1, waits),
            S=relay(0),
            T=relay(1),
        )
        for item in steps.split():
            with scope(item):
                run[item[0]](place.get(int(item[1:] or 0)))

    @pl.when(inside == 0)
    def _():
        follow(outer_steps, True, (1,))

    @pl.when(inside == 1)
    def _():
        follow(inner_steps, False, (1, 2, 3))

    for p, label in enumerate(labels):
        if label:
            with scope(f"back{label}"):
                back_in[p].wait_recv()
    share = quarter // per

    def piece_of(index, i):
        return pl.ds(pl.multiple_of(index * quarter + i * per, per), per)

    gathers = []
    for i in range(share):
        part, part_y = stream_grad.at[:, piece_of(q, i)], stream_grad.at[:, piece_of(q_y, i)]
        gathers.append(
            [
                remote(part, part, (gather_sem.at[0, 0, i], gather_sem.at[1, 0, i]), me, t_y),
                remote(part, part, (gather_sem.at[0, 1, i], gather_sem.at[1, 1, i]), me, t_core),
                remote(part_y, part_y, (gather_sem.at[0, 2, i], gather_sem.at[1, 2, i]), me, t_core),
            ]
        )
    sends = []

    def project(j, index, i):
        piece = stream_grad[:, piece_of(index, i)]
        proj_send[j * share + i] = lax.dot_general(
            piece, mixer_out[...], over_rows, preferred_element_type=f32
        ).astype(bf16)
        owner = index * share + i
        send = remote(
            proj_send.at[j * share + i],
            proj_got.at[me],
            (proj_sem.at[0, j * share + i], proj_sem.at[1, me]),
            owner,
            t,
        )

        @pl.when(owner != me)
        def _():
            send.start()

        @pl.when(owner == me)
        def _():
            proj_got[me] = proj_send[j * share + i]

        sends.append((owner, send))
        return jnp.dot(piece, out_proj_ref[piece_of(index, i), :], preferred_element_type=f32)

    for i in range(share):
        at = piece_of(q, i)
        moe_grad = lax.dot_general(
            pick_ref[...],
            back_got[:, pl.ds(i * per, per)],
            over_rows,
            preferred_element_type=f32,
        )
        stream_grad[:, at] = (cot_ref[:, at].astype(f32) + moe_grad).astype(bf16)
        gathers[i][0].start()
        gathers[i][1].start()
    d_mixer = project(0, q, 0)
    for i in range(1, share):
        d_mixer = d_mixer + project(0, q, i)
    for i in range(share):
        with scope(f"g1{i}"):
            gathers[i][1].wait_recv()
        d_mixer = d_mixer + project(1, q_core, i)
    for i in range(share):
        with scope(f"g0{i}"):
            gathers[i][0].wait_recv()
        gathers[i][2].start()
        d_mixer = d_mixer + project(2, q_y, i)
        with scope(f"g2{i}"):
            gathers[i][2].wait_recv()
        d_mixer = d_mixer + project(3, q_far, i)

    d_conv = d_mixer * outer_ref[...].astype(f32)
    after[pl.ds(0, tokens), :] = d_conv
    grad_outer_ref[...] = d_mixer * conv_out[...]

    @pl.when(me > 0)
    def _():
        to_previous.start()

    @pl.when(me == sp_devices - 1)
    def _():
        after[pl.ds(tokens, 8), :] = jnp.zeros((8, after.shape[1]), f32)

    with scope("prevw"):

        @pl.when(me < sp_devices - 1)
        def _():
            to_previous.wait_recv()

    d_mixed = (
        taps_ref[2:3, :] * after[pl.ds(0, tokens), :]
        + taps_ref[1:2, :] * after[pl.ds(1, tokens), :]
        + taps_ref[0:1, :] * after[pl.ds(2, tokens), :]
    )
    grad_inner_ref[...] = d_mixed * input_ref[...].astype(f32)
    grad_input_ref[...] = d_mixed * inner_ref[...].astype(f32)

    for k in others:
        source = flipped(me, k)
        with scope(f"pw{k}"):
            remote(
                proj_send.at[0],
                proj_got.at[source],
                (proj_sem.at[0, 0], proj_sem.at[1, source]),
                source,
                t,
            ).wait_recv()
    total = proj_got[0].astype(f32)
    for s in range(1, sp_devices):
        total = total + proj_got[s].astype(f32)
    grad_proj_ref[...] = total

    for label in others:
        p = place[label]
        for copy in (a[p] if label != 3 else []) + a_extra[p] + c_near[p] + c_far[p]:
            copy.wait_send()
        for copy in b[p] if label > 3 else []:
            copy.wait_send()
        back_out[p].wait_send()
    for copy in route_out:
        copy.wait_send()

    @pl.when(inside == 0)
    def _():
        for copy in to_near + b[place[2]] + b[place[3]] + extra_out[0] + extra_out[1]:
            copy.wait_send()
        route_in[0].wait_recv()

    @pl.when(inside == 1)
    def _():
        for copy in a[place[3]] + to_opposite + on_opposite + on_near[0] + on_near[1]:
            copy.wait_send()
        for copy in close[0] + close[1]:
            copy.wait_send()

    for p in range(len(labels)):
        core[p][0].wait_send()
        core[p][1].wait_send()
        y_hop[p].wait_send()
    for copies in gathers:
        for copy in copies:
            copy.wait_send()
    for owner, send in sends:

        @pl.when(owner != me)
        def _():
            send.wait_send()

    @pl.when(me < sp_devices - 1)
    def _():
        to_next.wait_send()

    @pl.when(me > 0)
    def _():
        to_previous.wait_send()


def written(*refs):
    count = (len(refs) - 1) // 2
    sem = refs[-1]
    outs = [
        pltpu.make_async_copy(refs[i], refs[count + i], sem.at[i]) for i in range(count)
    ]
    for out in outs:
        out.start()
    for out in outs:
        out.wait()


def fused_shards(
    out_cotangent,
    stream,
    route_ids,
    route_weights,
    gate_proj,
    up_proj,
    down_proj,
    outer_gate,
    inner_gate,
    conv_input,
    conv_taps,
    out_proj,
):
    f32, bf16 = jnp.float32, jnp.bfloat16
    n = lax.axis_size("sp")
    tokens, width = stream.shape
    units = gate_proj.shape[2]
    channels = out_proj.shape[1]
    capacity = 4 * tokens // n
    slots = n * capacity
    quarter = width // lax.axis_size("tp")
    per = width // n
    labels = [0, 1, 2, 3, 4, 5, 6, 7]
    outer_steps = (
        "X Z E0 R0 U u a3 A3 a2 b3 A2 B3 C3 E3 R3 Y0 V P a1 A1 b1 B1 J C1 E1 R1 b2 B2 K a5 C2"
        " E2 A5 b4 B4 C4 L E4 R4 Y3 a7 M b5 B5 C5 E5 R5 A7 Y4 b6 B6 C6 E6 Y5 R6 b7 B7 C7 E7 R7"
        " R2 Y1 Y6 G H Y7 Y2 D"
    )
    inner_steps = (
        "E0 R0 w J W K a5 a3 b4 B4 S L C4 E4 R4 T M X A5 A3 Z Y0 V P b2 B2 C2 E2 R2 a7 Y4 b5"
        " B5 C5 E5 R5 A7 b6 B6 C6 E6 R6 Y5 Y2 b7 B7 C7 E7 R7 Y6 b3 B3 C3 E3 R3 Y7 a1 A1 b1 B1"
        " C1 E1 Y3 R1 G Y1 H D"
    )
    vmem = pl.BlockSpec(memory_space=pltpu.VMEM)
    hbm = pl.BlockSpec(memory_space=pltpu.HBM)
    anywhere = pl.BlockSpec(memory_space=pl.ANY)
    dma = pltpu.SemaphoreType.DMA
    shapes = [
        ((width, units), bf16),
        ((width, units), bf16),
        ((units, width), bf16),
        ((per, channels), f32),
        ((tokens, channels), f32),
        ((tokens, channels), f32),
        ((tokens, channels), f32),
    ]
    args = (
        out_cotangent,
        stream,
        route_ids.T,
        route_weights.T,
        outer_gate,
        inner_gate,
        conv_input,
        conv_taps,
        out_proj,
        gate_proj[0],
        up_proj[0],
        down_proj[0],
    )
    grads = pl.pallas_call(
        functools.partial(fused, n, labels, outer_steps, inner_steps),
        out_shape=[pltpu.VMEM(*shape) for shape in shapes],
        in_specs=[hbm] * 12,
        out_specs=[vmem] * 7,
        scratch_shapes=[
            pltpu.VMEM((tokens, width), bf16),
            pltpu.VMEM((tokens, width), bf16),
            pltpu.VMEM(route_ids.shape[::-1], jnp.int32),
            pltpu.VMEM(route_ids.shape[::-1], f32),
            pltpu.VMEM((tokens, channels), bf16),
            pltpu.VMEM((tokens, channels), bf16),
            pltpu.VMEM((tokens, channels), bf16),
            pltpu.VMEM(conv_taps.shape, f32),
            pltpu.VMEM((width, channels), bf16),
            pltpu.VMEM((2, n, tokens), f32),
            pltpu.VMEM((3, 2, n, tokens), f32),
            pltpu.VMEM((3, 2, capacity, tokens), bf16),
            pltpu.VMEM((slots, tokens), bf16),
            pltpu.VMEM((3, 2, tokens, quarter), bf16),
            pltpu.VMEM((2, slots, width), bf16),
            pltpu.VMEM((n // 2 + 1, 2, capacity, quarter), bf16),
            pltpu.VMEM((2, 2, capacity, quarter), bf16),
            pltpu.VMEM((2, 2, capacity, quarter), bf16),
            pltpu.VMEM((width, 2 * units), bf16),
            pltpu.VMEM((units, width), bf16),
            pltpu.VMEM((slots, units), bf16),
            pltpu.VMEM((slots, 2 * units), bf16),
            pltpu.VMEM((2, slots, quarter), bf16),
            pltpu.VMEM((slots, quarter), f32),
            pltpu.VMEM((2, slots, quarter), bf16),
            pltpu.VMEM((2, slots, quarter), bf16),
            pltpu.VMEM((slots, quarter), bf16),
            pltpu.VMEM((slots, quarter), bf16),
            pltpu.VMEM((slots, quarter), bf16),
            pltpu.VMEM((slots, quarter), bf16),
            pltpu.VMEM((tokens, width), bf16),
            pltpu.VMEM((n, per, channels), bf16),
            pltpu.VMEM((n, per, channels), bf16),
            pltpu.VMEM((tokens + 8, channels), f32),
            pltpu.VMEM((tokens + 8, channels), f32),
            pltpu.VMEM((tokens, channels), f32),
            pltpu.VMEM((tokens, channels), bf16),
            dma((12,)),
            dma((2, 3)),
            dma((8, 2)),
            dma((2, 2)),
            dma((2, 2)),
            dma((2, 2, n)),
            dma((2, 2, n)),
            dma((4, 2, n)),
            dma((2, 2, n)),
            dma((2, n)),
            dma((2, n)),
            dma((2, 3, quarter // per)),
            dma((2, n)),
            dma((4,)),
        ],
        compiler_params=pltpu.CompilerParams(
            collective_id=0, has_side_effects=True, vmem_limit_bytes=48 * 1024 * 1024
        ),
    )(*(pltpu.with_memory_space_constraint(arg, pltpu.HBM) for arg in args))
    outs = pl.pallas_call(
        written,
        out_shape=[jax.ShapeDtypeStruct(*shape) for shape in shapes],
        in_specs=[anywhere] * 7,
        out_specs=[hbm] * 7,
        scratch_shapes=[dma((7,))],
        compiler_params=pltpu.CompilerParams(vmem_limit_bytes=1024 * 1024),
    )(*(pltpu.with_memory_space_constraint(grad, pltpu.VMEM) for grad in grads))
    return (outs[0][None], outs[1][None], outs[2][None], *outs[3:])


def fits_kernel(mesh):
    return mesh.shape["sp"] == 8 and mesh.shape["tp"] == 4


def solution(mesh):
    placed = (
        P("sp", None),
        P("sp", None),
        P("sp", None),
        P("sp", None),
        P("sp", None, "tp"),
        P("sp", None, "tp"),
        P("sp", "tp", None),
        P("sp", "tp"),
        P("sp", "tp"),
        P("sp", "tp"),
        P(None, "tp"),
        P(None, "tp"),
    )
    return jax.shard_map(
        fused_shards if fits_kernel(mesh) else shards,
        mesh=mesh,
        in_specs=placed,
        out_specs=(
            P("sp", None, "tp"),
            P("sp", None, "tp"),
            P("sp", "tp", None),
            P("sp", "tp"),
            P("sp", "tp"),
            P("sp", "tp"),
            P("sp", "tp"),
        ),
        check_vma=False,
    )
```

```python
import functools

import jax
import jax.numpy as jnp
from jax import lax
from jax.experimental import pallas as pl
from jax.experimental.pallas import tpu as pltpu
from jax.sharding import PartitionSpec as P


def passed_along(x, axis, by):
    devices = lax.axis_size(axis)
    pairs = [(i, i + by) for i in range(devices) if 0 <= i + by < devices]
    return lax.ppermute(x, axis, pairs)


def to_owners(x, devices):
    blocks = x.reshape(devices, -1, x.shape[1])
    return lax.all_to_all(blocks, "sp", split_axis=0, concat_axis=0, tiled=True).reshape(x.shape)


def partial_rows(d_gate, d_up, w_gate, w_up):
    across = (((1,), (1,)), ((), ()))
    total = lax.dot_general(
        d_gate, w_gate, across, preferred_element_type=jnp.float32
    ) + lax.dot_general(d_up, w_up, across, preferred_element_type=jnp.float32)
    return total.astype(jnp.bfloat16)


def reduced_quarter(d_gate, d_up, w_gate, w_up):
    devices = lax.axis_size("tp")
    if devices != 4:
        return lax.psum_scatter(
            partial_rows(d_gate, d_up, w_gate, w_up), "tp", scatter_dimension=1, tiled=True
        )
    quarter = w_gate.shape[0] // devices
    me = lax.axis_index("tp")

    def rows_of(w, *flips):
        return jnp.concatenate(
            [lax.dynamic_slice_in_dim(w, (me ^ flip) * quarter, quarter, 0) for flip in flips]
        )

    def swapped(x, flip):
        return lax.ppermute(x, "tp", [(i, i ^ flip) for i in range(devices)])

    sent = partial_rows(d_gate, d_up, rows_of(w_gate, 1, 3), rows_of(w_up, 1, 3))
    got = swapped(sent, 1)
    kept = partial_rows(d_gate, d_up, rows_of(w_gate, 0, 2), rows_of(w_up, 0, 2))
    far = kept[:, quarter:].astype(jnp.float32) + got[:, quarter:].astype(jnp.float32)
    near = kept[:, :quarter].astype(jnp.float32) + got[:, :quarter].astype(jnp.float32)
    other = swapped(far.astype(jnp.bfloat16), 2)
    return (near + other.astype(jnp.float32)).astype(jnp.bfloat16)


def shards(
    out_cotangent,
    stream,
    route_ids,
    route_weights,
    gate_proj,
    up_proj,
    down_proj,
    outer_gate,
    inner_gate,
    conv_input,
    conv_taps,
    out_proj,
):
    sp_devices = lax.axis_size("sp")
    tokens_here, width = stream.shape
    experts = sp_devices * gate_proj.shape[0]
    capacity = 4 * tokens_here // experts
    quarter = width // lax.axis_size("tp")
    first_column = lax.axis_index("tp") * quarter
    own_cotangent = lax.dynamic_slice_in_dim(out_cotangent, first_column, quarter, 1)
    own_stream = lax.dynamic_slice_in_dim(stream, first_column, quarter, 1)
    over_rows = (((0,), (0,)), ((), ()))
    expert_ids = jnp.arange(experts, dtype=jnp.int32)
    chosen = route_ids[:, :, None] == expert_ids
    hit = jnp.any(chosen, axis=1)
    token_weight = jnp.sum(jnp.where(chosen, route_weights[:, :, None], 0.0), axis=1)
    token_ids = jnp.arange(tokens_here, dtype=jnp.int32)
    below = (token_ids[:, None] < token_ids[None, :]).astype(jnp.bfloat16)
    rank = lax.dot_general(
        hit.astype(jnp.bfloat16), below, over_rows, preferred_element_type=jnp.float32
    )
    rank = jnp.where(hit.T, rank, -1.0)
    in_slot = rank[:, None, :] == jnp.arange(capacity, dtype=jnp.float32)[None, :, None]
    slot_weight = jnp.sum(jnp.where(in_slot, token_weight.T[:, None, :], 0.0), axis=2)
    pick = in_slot.astype(jnp.bfloat16).reshape(experts * capacity, tokens_here)
    send_input = jnp.dot(pick, own_stream, preferred_element_type=jnp.float32).astype(jnp.bfloat16)
    send_grad = (
        slot_weight.reshape(-1, 1)
        * jnp.dot(pick, own_cotangent, preferred_element_type=jnp.float32)
    ).astype(jnp.bfloat16)
    got_input = to_owners(send_input, sp_devices)
    rows_input = lax.all_gather(got_input, "tp", axis=1, tiled=True)
    send_grad, got_input = lax.optimization_barrier((send_grad, got_input))
    got_grad = to_owners(send_grad, sp_devices)
    rows_grad = lax.all_gather(got_grad, "tp", axis=1, tiled=True)
    mixed = inner_gate.astype(jnp.float32) * conv_input.astype(jnp.float32)
    previous = passed_along(mixed[tokens_here - 2 :], "sp", 1)
    extended = jnp.concatenate([previous, mixed], axis=0)
    conv_out = (
        conv_taps[0] * extended[:tokens_here]
        + conv_taps[1] * extended[1 : tokens_here + 1]
        + conv_taps[2] * extended[2:]
    )
    mixer_out = (outer_gate.astype(jnp.float32) * conv_out).astype(jnp.bfloat16)
    conv_out, mixer_out, rows_grad = lax.optimization_barrier((conv_out, mixer_out, rows_grad))
    w_gate = gate_proj[0]
    w_up = up_proj[0]
    w_down = down_proj[0]
    gate = jnp.dot(rows_input, w_gate, preferred_element_type=jnp.float32)
    up = jnp.dot(rows_input, w_up, preferred_element_type=jnp.float32)
    sig = jax.nn.sigmoid(gate)
    silu_gate = gate * sig
    hidden = (silu_gate * up).astype(jnp.bfloat16)
    across = (((1,), (1,)), ((), ()))
    d_hidden = lax.dot_general(rows_grad, w_down, across, preferred_element_type=jnp.float32)
    d_gate = (d_hidden * up * sig * (1.0 + gate * (1.0 - sig))).astype(jnp.bfloat16)
    d_up = (d_hidden * silu_gate).astype(jnp.bfloat16)
    grad_down = lax.dot_general(
        hidden, rows_grad, over_rows, preferred_element_type=jnp.float32
    ).astype(jnp.bfloat16)
    grad_gate = lax.dot_general(
        rows_input, d_gate, over_rows, preferred_element_type=jnp.float32
    ).astype(jnp.bfloat16)
    grad_up = lax.dot_general(
        rows_input, d_up, over_rows, preferred_element_type=jnp.float32
    ).astype(jnp.bfloat16)
    chunks = 2
    piece = capacity // chunks
    shape = (sp_devices, chunks, piece, d_gate.shape[1])
    gate_pieces = d_gate.reshape(shape)
    up_pieces = d_up.reshape(shape)
    shares = []
    for c in range(chunks):
        shares.append(
            reduced_quarter(
                gate_pieces[:, c].reshape(-1, shape[3]),
                up_pieces[:, c].reshape(-1, shape[3]),
                w_gate,
                w_up,
            )
        )
    shares[0], grad_down, grad_gate, grad_up = lax.optimization_barrier(
        (shares[0], grad_down, grad_gate, grad_up)
    )
    moe_grad = own_cotangent.astype(jnp.float32)
    pick_pieces = pick.reshape(experts, chunks, piece, tokens_here)
    for c in range(chunks):
        returned = to_owners(shares[c], sp_devices)
        moe_grad = moe_grad + lax.dot_general(
            pick_pieces[:, c].reshape(-1, tokens_here), returned, over_rows,
            preferred_element_type=jnp.float32,
        )
    stream_part = moe_grad.astype(jnp.bfloat16)
    stream_grad = lax.all_gather(stream_part, "tp", axis=1, tiled=True)
    own_projection = lax.dot_general(
        stream_grad, mixer_out, over_rows, preferred_element_type=jnp.float32
    ).astype(jnp.bfloat16)
    projections = to_owners(own_projection, sp_devices)
    grad_projection = jnp.sum(
        projections.astype(jnp.float32).reshape(sp_devices, -1, projections.shape[1]), axis=0
    )
    d_mixer = jnp.dot(stream_grad, out_proj, preferred_element_type=jnp.float32)
    grad_outer = d_mixer * conv_out
    d_conv = d_mixer * outer_gate.astype(jnp.float32)
    following = passed_along(d_conv[:2], "sp", -1)
    trailing = jnp.concatenate([d_conv, following], axis=0)
    d_mixed = (
        conv_taps[2] * trailing[:tokens_here]
        + conv_taps[1] * trailing[1 : tokens_here + 1]
        + conv_taps[0] * trailing[2:]
    )
    grad_inner = d_mixed * conv_input.astype(jnp.float32)
    grad_input = d_mixed * inner_gate.astype(jnp.float32)
    return (
        grad_gate[None],
        grad_up[None],
        grad_down[None],
        grad_projection,
        grad_outer,
        grad_inner,
        grad_input,
    )


MESH = pl.DeviceIdType.MESH


def flipped(index, flips):
    place = 1
    while place <= flips:
        if (flips // place) % 2:
            index = index + place * (1 - 2 * ((index // place) % 2))
        place *= 2
    return index


def fused(
    sp_devices,
    labels,
    outer_steps,
    inner_steps,
    cot_hbm,
    stream_hbm,
    ids_hbm,
    weights_hbm,
    outer_hbm,
    inner_hbm,
    input_hbm,
    taps_hbm,
    out_proj_hbm,
    w_gate_hbm,
    w_up_hbm,
    w_down_hbm,
    grad_gate_ref,
    grad_up_ref,
    grad_down_ref,
    grad_proj_ref,
    grad_outer_ref,
    grad_inner_ref,
    grad_input_ref,
    cot_ref,
    stream_ref,
    ids_ref,
    weights_ref,
    outer_ref,
    inner_ref,
    input_ref,
    taps_ref,
    out_proj_ref,
    route,
    far_route,
    far_pick,
    pick_ref,
    raw,
    rows,
    a_send,
    close_send,
    extra_send,
    w_pair,
    w_down,
    hidden,
    d_pair,
    kept,
    near_got,
    core_send,
    core_got,
    y_send,
    y_got,
    back_send,
    back_got,
    stream_grad,
    proj_send,
    proj_got,
    before,
    after,
    conv_out,
    mixer_out,
    load_sem,
    out_sem,
    route_sem,
    raw_sem,
    a_sem,
    b_sem,
    c_sem,
    core_sem,
    y_sem,
    back_sem,
    gather_sem,
    proj_sem,
    conv_sem,
):
    f32, bf16 = jnp.float32, jnp.bfloat16
    scope = jax.named_scope
    me = lax.axis_index("sp")
    t = lax.axis_index("tp")
    t_core, t_y = flipped(t, 1), flipped(t, 2)
    half = lax.axis_size("tp") // 2
    tokens, width = stream_ref.shape
    capacity = pick_ref.shape[0] // sp_devices
    units = hidden.shape[1]
    quarter = width // lax.axis_size("tp")
    per = width // sp_devices
    over_rows = (((0,), (0,)), ((), ()))
    across = (((1,), (1,)), ((), ()))
    others = range(1, sp_devices)

    def owned(member):
        return (member % 2) * half + member // 2

    q, q_core, q_y, q_far = owned(t), owned(t_core), owned(t_y), owned(flipped(t, 3))

    def columns(index):
        return pl.ds(pl.multiple_of(index * quarter, quarter), quarter)

    def block(p):
        return pl.ds(p * capacity, capacity)

    def dynamic_block(p):
        return pl.ds(pl.multiple_of(p * capacity, capacity), capacity)

    def remote(src, dst, sems, sp, tp):
        return pltpu.make_async_remote_copy(
            src_ref=src,
            dst_ref=dst,
            send_sem=sems[0],
            recv_sem=sems[1],
            device_id=(sp, tp),
            device_id_type=MESH,
        )

    peers = [(flipped(me, k), t) for k in others] + [(me, t_core), (me, t_y)]
    barrier = pltpu.get_barrier_semaphore()
    for peer in peers:
        pl.semaphore_signal(barrier, inc=1, device_id=peer, device_id_type=MESH)

    moved = [
        (ids_hbm, ids_ref),
        (weights_hbm, weights_ref),
        (inner_hbm, inner_ref),
        (input_hbm, input_ref),
        (stream_hbm, stream_ref),
        (cot_hbm, cot_ref),
        (w_gate_hbm, w_pair.at[:, pl.ds(0, units)]),
        (w_up_hbm, w_pair.at[:, pl.ds(units, units)]),
        (w_down_hbm, w_down),
        (outer_hbm, outer_ref),
        (taps_hbm, taps_ref),
        (out_proj_hbm, out_proj_ref),
    ]
    loads = [
        pltpu.make_async_copy(src, dst, load_sem.at[i]) for i, (src, dst) in enumerate(moved)
    ]
    for load in loads:
        load.start()

    with scope("prep"):
        for load in loads[:4]:
            load.wait()
        before[pl.ds(8, tokens), :] = inner_ref[...].astype(f32) * input_ref[...].astype(f32)
        expert_ids = lax.broadcasted_iota(jnp.int32, (sp_devices, tokens), 0)
        chosen = [ids_ref[j : j + 1, :] == expert_ids for j in range(ids_ref.shape[0])]
        hit = jnp.zeros((sp_devices, tokens), f32)
        weight = jnp.zeros((sp_devices, tokens), f32)
        for j, choice in enumerate(chosen):
            hit = jnp.where(choice, 1.0, hit)
            weight = jnp.where(choice, weights_ref[j : j + 1, :], weight)
        earlier = lax.broadcasted_iota(jnp.int32, (tokens, tokens), 0)
        later = lax.broadcasted_iota(jnp.int32, (tokens, tokens), 1)
        below = jnp.where(earlier < later, 1.0, 0.0).astype(bf16)
        rank = jnp.dot(hit.astype(bf16), below, preferred_element_type=f32)
        route[0] = jnp.where(hit > 0.0, rank, -1.0)
        route[1] = weight
        slot = lax.broadcasted_iota(jnp.int32, (capacity, tokens), 0).astype(f32)

    def slots_of(ref, expert):
        return ref[0, pl.ds(expert, 1), :] == slot

    def one_hot(chosen_slot):
        return jnp.where(chosen_slot, 1.0, 0.0).astype(bf16)

    def scale_of(ref, expert, chosen_slot):
        return jnp.sum(
            jnp.where(chosen_slot, ref[1, pl.ds(expert, 1), :], 0.0), axis=1, keepdims=True
        )

    def compacted(expert, ranges):
        chosen_slot = slots_of(route, expert)
        pick = one_hot(chosen_slot)
        pick_ref[dynamic_block(expert), :] = pick
        scale = scale_of(route, expert, chosen_slot)
        return [
            (
                jnp.dot(pick, stream_ref[:, at], preferred_element_type=f32).astype(bf16),
                (scale * jnp.dot(pick, cot_ref[:, at], preferred_element_type=f32)).astype(bf16),
            )
            for at in ranges
        ]

    z, side = me // 2, me % 2
    upper = z // 2
    inside = (z + upper) % 2
    across_x, near, opposite = flipped(me, 1), flipped(me, 2), flipped(me, 6)
    lines = [z, z + 1 - 2 * (z % 2), 2 - upper, 3 - 3 * upper]
    place = {label: p for p, label in enumerate(labels)}
    a, a_extra, b, c_near, c_far, back_out, back_in, partners = {}, {}, {}, {}, {}, {}, {}, {}
    for label in range(sp_devices):
        p = place[label]
        across_side = 1 - side if label % 2 else side
        partner = partners[p] = 2 * lines[label // 2] + across_side
        a[p], a_extra[p], b[p], c_near[p], c_far[p] = [], [], [], [], []
        for i in range(2):
            mine, theirs = rows.at[i, block(p), columns(q)], rows.at[i, block(p), columns(q_y)]
            if label % 2:
                a[p].append(
                    remote(
                        a_send.at[label // 2, i],
                        mine,
                        (out_sem.at[4], a_sem.at[i, p]),
                        across_x,
                        t,
                    )
                )
            if label == 1:
                a_extra[p].append(
                    remote(
                        a_send.at[sp_devices // 2, i],
                        theirs,
                        (out_sem.at[4], a_sem.at[i, 0]),
                        across_x,
                        t,
                    )
                )
            b[p].append(remote(mine, mine, (out_sem.at[5], b_sem.at[i, p]), me, t_y))
            c_near[p].append(
                remote(mine, mine, (out_sem.at[6], c_sem.at[p]), me, t_core)
            )
            c_far[p].append(
                remote(theirs, theirs, (out_sem.at[6], c_sem.at[p]), me, t_core)
            )
        back_out[p] = remote(
            back_send.at[block(p)],
            back_got.at[dynamic_block(me)],
            (out_sem.at[9], back_sem.at[me]),
            partner,
            t,
        )
        back_in[p] = remote(
            back_send.at[block(p)],
            back_got.at[dynamic_block(partner)],
            (out_sem.at[9], back_sem.at[partner]),
            partner,
            t,
        )
    close = [
        [
            remote(
                close_send.at[j, i],
                rows.at[i, block(place[2 + j]), columns(q)],
                (out_sem.at[2], a_sem.at[i, place[2 + j]]),
                flipped(me, 2 + j),
                t,
            )
            for i in range(2)
        ]
        for j in range(2)
    ]
    extra_out, extra_in = (
        [
            [
                remote(
                    extra_send.at[j, i],
                    rows.at[i, block(place[2 + j]), columns(q_y)],
                    (out_sem.at[3], b_sem.at[i, place[2 + j]]),
                    flipped(me, 2 + j),
                    t,
                )
                for i in range(2)
            ]
            for j in range(2)
        ]
        for _ in range(2)
    )
    to_near, to_opposite, on_opposite, on_near = [], [], [], [[], []]
    for i, ref in enumerate((stream_ref, cot_ref)):
        own = ref.at[:, columns(q)]
        to_near.append(
            remote(own, raw.at[0, i], (out_sem.at[1], raw_sem.at[0, i]), near, t)
        )
        to_opposite.append(
            remote(own, raw.at[1, i], (out_sem.at[1], raw_sem.at[1, i]), opposite, t)
        )
        on_opposite.append(
            remote(raw.at[0, i], raw.at[2, i], (out_sem.at[1], raw_sem.at[2, i]), opposite, t)
        )
        for j in range(2):
            on_near[j].append(
                remote(
                    raw.at[1 + j, i],
                    raw.at[1 + j, i],
                    (out_sem.at[1], raw_sem.at[1 + j, i]),
                    near,
                    t,
                )
            )
    as_far = 2 - inside
    route_out = [
        remote(route, far_route.at[0], (out_sem.at[0], route_sem.at[0]), near, t)
    ] + [
        remote(
            route,
            far_route.at[as_far],
            (out_sem.at[0], route_sem.at[as_far]),
            flipped(me, 2 + 2 * j),
            t,
        )
        for j in (1, 2)
    ]
    route_in = [
        remote(route, far_route.at[j], (out_sem.at[0], route_sem.at[j]), near, t)
        for j in range(3)
    ]
    to_next = remote(
        before.at[pl.ds(tokens, 8)],
        before.at[pl.ds(0, 8)],
        (out_sem.at[12], conv_sem.at[0]),
        me + 1,
        t,
    )
    to_previous = remote(
        after.at[pl.ds(0, 8)],
        after.at[pl.ds(tokens, 8)],
        (out_sem.at[13], conv_sem.at[1]),
        me - 1,
        t,
    )

    with scope("barrier"):
        pl.semaphore_wait(barrier, len(peers))
    for out in route_out:
        out.start()

    @pl.when(me < sp_devices - 1)
    def _():
        to_next.start()

    for i in range(2):
        loads[4 + i].wait()

        @pl.when(inside == 0)
        def _():
            to_near[i].start()

        @pl.when(inside == 1)
        def _():
            to_opposite[i].start()

    @pl.when(inside == 1)
    def _():
        for j in (1, 0):
            close_send[j, 0], close_send[j, 1] = compacted(flipped(me, 2 + j), [columns(q)])[0]
            for i in range(2):
                close[j][i].start()

    own = compacted(me, [pl.ds(0, width)])[0]
    rows[0, block(place[0]), :], rows[1, block(place[0]), :] = own
    for load in loads[6:]:
        load.wait()

    core, y_hop = {}, {}
    for p in range(len(labels)):
        core[p] = [
            remote(
                core_send.at[i, block(p)],
                core_got.at[i, block(p)],
                (out_sem.at[7], core_sem.at[i, p]),
                me,
                t_core,
            )
            for i in range(2)
        ]
        y_hop[p] = remote(
            y_send.at[block(p)], y_got.at[block(p)], (out_sem.at[8], y_sem.at[p]), me, t_y
        )

    def compact_far(line, i, direct):
        far = far_route.at[line - 1]
        if i == 0:
            route_in[line - 1].wait_recv()
        for j, expert in enumerate((me, across_x)):
            chosen_slot = slots_of(far, expert)
            if i == 0:
                pick = one_hot(chosen_slot)
                far_pick[line - 1, j] = pick
            else:
                pick = far_pick[line - 1, j]
            part = jnp.dot(pick, raw[line - 1, i], preferred_element_type=f32)
            if i:
                part = scale_of(far, expert, chosen_slot) * part
            p = place[2 * line + j]
            if j:
                a_send[line, i] = part.astype(bf16)
                a[p][i].start()
            else:
                rows[i, block(p), columns(q)] = part.astype(bf16)
                if 2 * line not in direct:
                    b[p][i].start()
                c_near[p][i].start()

    def first_line(i, direct):
        def go(_):
            to_near[i].wait_recv()
            on_opposite[i].start()
            to_opposite[i].wait_recv()
            on_near[0][i].start()
            compact_far(1, i, direct)

        return go

    def relay(i):
        def go(_):
            on_opposite[i].wait_recv()
            on_near[1][i].start()

        return go

    def later_line(line, i, waits):
        def go(_):
            if waits:
                on_near[line - 2][i].wait_recv()
            compact_far(line, i, ())

        return go

    def to_side(_):
        p = place[1]
        both = compacted(across_x, [columns(q), columns(q_y)])
        a_send[0, 0], a_send[0, 1] = both[0]
        a_send[sp_devices // 2, 0], a_send[sp_devices // 2, 1] = both[1]
        for i in range(2):
            a[p][i].start()

    def to_side_more(_):
        for copy in a_extra[place[1]]:
            copy.start()

    def other_picks(_):
        for k in range(2, sp_devices):
            expert = flipped(me, k)
            pick_ref[dynamic_block(expert), :] = one_hot(slots_of(route, expert))

    def to_close_more(j):
        def go(_):
            extra_send[j, 0], extra_send[j, 1] = compacted(flipped(me, 2 + j), [columns(q_y)])[0]
            for copy in extra_out[j]:
                copy.start()

        return go

    def arrive(i, direct):
        def go(p):
            (a[p] or close[0])[i].wait_recv()
            if labels[p] not in direct:
                b[p][i].start()
            c_near[p][i].start()

        return go

    def cross(i, direct):
        def go(p):
            if labels[p] == 1:
                a_extra[p][i].wait_recv()
            elif labels[p] in direct:
                extra_in[labels[p] - 2][i].wait_recv()
            else:
                b[p][i].wait_recv()
            c_far[p][i].start()

        return go

    def gather(p):
        four = core_got.at[:, pl.ds(0, 2 * capacity)]
        remote(four, four, (out_sem.at[6], c_sem.at[p]), me, t_core).wait_recv()

    def expert(p):
        span = block(p)
        both = jnp.dot(rows[0, span, :], w_pair[...], preferred_element_type=f32)
        gate, up = both[:, :units], both[:, units:]
        d_hidden = lax.dot_general(
            rows[1, span, :], w_down[...], across, preferred_element_type=f32
        )
        sig = jax.nn.sigmoid(gate)
        silu_gate = gate * sig
        hidden[span, :] = (silu_gate * up).astype(bf16)
        d_gate = (d_hidden * up * sig * (1.0 + gate * (1.0 - sig))).astype(bf16)
        d_up = (d_hidden * silu_gate).astype(bf16)
        d_pair[span, pl.ds(0, units)] = d_gate
        d_pair[span, pl.ds(units, units)] = d_up

        def partial(index):
            return lax.dot_general(
                d_pair[span, :], w_pair[columns(index), :], across, preferred_element_type=f32
            ).astype(bf16)

        core_send[1, span, :] = partial(q_far)
        core_send[0, span, :] = partial(q_core)
        core[p][1].start()
        kept[1, span, :] = partial(q_y)
        core[p][0].start()
        kept[0, span, :] = partial(q)

    def reduce_core(p):
        span = block(p)
        core[p][1].wait_recv()
        y_send[span, :] = (
            kept[1, span, :].astype(f32) + core_got[1, span, :].astype(f32)
        ).astype(bf16)
        y_hop[p].start()
        core[p][0].wait_recv()
        near_got[span, :] = kept[0, span, :].astype(f32) + core_got[0, span, :].astype(f32)

    def reduce_y(p):
        span = block(p)
        y_hop[p].wait_recv()
        back_send[span, :] = (near_got[span, :] + y_got[span, :].astype(f32)).astype(bf16)
        if labels[p]:
            back_out[p].start()
        else:
            back_got[dynamic_block(me), :] = back_send[span, :]

    def convolve(p):
        @pl.when(me == 0)
        def _():
            before[pl.ds(0, 8), :] = jnp.zeros((8, before.shape[1]), f32)

        @pl.when(me > 0)
        def _():
            to_next.wait_recv()

        conv = (
            taps_ref[0:1, :] * before[pl.ds(6, tokens), :]
            + taps_ref[1:2, :] * before[pl.ds(7, tokens), :]
            + taps_ref[2:3, :] * before[pl.ds(8, tokens), :]
        )
        conv_out[...] = conv
        mixer_out[...] = (outer_ref[...].astype(f32) * conv).astype(bf16)

    step = 2 * units

    def down(j, carry):
        at = pl.ds(pl.multiple_of(j * step, step), step)
        grad_down_ref[:, at] = lax.dot_general(
            hidden[...], rows[1, :, at], over_rows, preferred_element_type=f32
        ).astype(bf16)
        return carry

    def gate_up(j, carry):
        at = pl.ds(pl.multiple_of(j * units, units), units)
        both = lax.dot_general(
            rows[0, :, at], d_pair[...], over_rows, preferred_element_type=f32
        ).astype(bf16)
        grad_gate_ref[at, :] = both[:, :units]
        grad_up_ref[at, :] = both[:, units:]
        return carry

    def first_gate_up(p):
        lax.fori_loop(0, width // units // 2, gate_up, 0)

    def second_gate_up(p):
        lax.fori_loop(width // units // 2, width // units, gate_up, 0)

    def all_down(p):
        lax.fori_loop(0, width // step, down, 0)

    def follow(steps, waits, direct):
        run = dict(
            a=arrive(0, direct),
            A=arrive(1, direct),
            b=cross(0, direct),
            B=cross(1, direct),
            C=gather,
            E=expert,
            R=reduce_core,
            Y=reduce_y,
            V=convolve,
            G=first_gate_up,
            H=second_gate_up,
            D=all_down,
            w=first_line(0, direct),
            W=first_line(1, direct),
            U=to_close_more(0),
            u=to_close_more(1),
            X=to_side,
            Z=to_side_more,
            P=other_picks,
            J=later_line(2, 0, waits),
            K=later_line(2, 1, waits),
            L=later_line(3, 0, waits),
            M=later_line(3, 1, waits),
            S=relay(0),
            T=relay(1),
        )
        for item in steps.split():
            with scope(item):
                run[item[0]](place.get(int(item[1:] or 0)))

    @pl.when(inside == 0)
    def _():
        follow(outer_steps, True, (1,))

    @pl.when(inside == 1)
    def _():
        follow(inner_steps, False, (1, 2, 3))

    for p, label in enumerate(labels):
        if label:
            with scope(f"back{label}"):
                back_in[p].wait_recv()
    share = quarter // per

    def piece_of(index, i):
        return pl.ds(pl.multiple_of(index * quarter + i * per, per), per)

    gathers = []
    for i in range(share):
        part, part_y = stream_grad.at[:, piece_of(q, i)], stream_grad.at[:, piece_of(q_y, i)]
        gathers.append(
            [
                remote(part, part, (out_sem.at[10], gather_sem.at[0, i]), me, t_y),
                remote(part, part, (out_sem.at[10], gather_sem.at[1, i]), me, t_core),
                remote(part_y, part_y, (out_sem.at[10], gather_sem.at[2, i]), me, t_core),
            ]
        )

    def project(j, index, i):
        piece = stream_grad[:, piece_of(index, i)]
        proj_send[j * share + i] = lax.dot_general(
            piece, mixer_out[...], over_rows, preferred_element_type=f32
        ).astype(bf16)
        owner = index * share + i
        send = remote(
            proj_send.at[j * share + i],
            proj_got.at[me],
            (out_sem.at[11], proj_sem.at[me]),
            owner,
            t,
        )

        @pl.when(owner != me)
        def _():
            send.start()

        @pl.when(owner == me)
        def _():
            proj_got[me] = proj_send[j * share + i]

        return jnp.dot(piece, out_proj_ref[piece_of(index, i), :], preferred_element_type=f32)

    for i in range(share):
        at = piece_of(q, i)
        moe_grad = lax.dot_general(
            pick_ref[...],
            back_got[:, pl.ds(i * per, per)],
            over_rows,
            preferred_element_type=f32,
        )
        stream_grad[:, at] = (cot_ref[:, at].astype(f32) + moe_grad).astype(bf16)
        gathers[i][0].start()
        gathers[i][1].start()
    d_mixer = project(0, q, 0)
    for i in range(1, share):
        d_mixer = d_mixer + project(0, q, i)
    for i in range(share):
        with scope(f"g1{i}"):
            gathers[i][1].wait_recv()
        d_mixer = d_mixer + project(1, q_core, i)
    for i in range(share):
        with scope(f"g0{i}"):
            gathers[i][0].wait_recv()
        gathers[i][2].start()
        d_mixer = d_mixer + project(2, q_y, i)
        with scope(f"g2{i}"):
            gathers[i][2].wait_recv()
        d_mixer = d_mixer + project(3, q_far, i)

    d_conv = d_mixer * outer_ref[...].astype(f32)
    after[pl.ds(0, tokens), :] = d_conv
    grad_outer_ref[...] = d_mixer * conv_out[...]

    @pl.when(me > 0)
    def _():
        to_previous.start()

    @pl.when(me == sp_devices - 1)
    def _():
        after[pl.ds(tokens, 8), :] = jnp.zeros((8, after.shape[1]), f32)

    with scope("prevw"):

        @pl.when(me < sp_devices - 1)
        def _():
            to_previous.wait_recv()

    d_mixed = (
        taps_ref[2:3, :] * after[pl.ds(0, tokens), :]
        + taps_ref[1:2, :] * after[pl.ds(1, tokens), :]
        + taps_ref[0:1, :] * after[pl.ds(2, tokens), :]
    )
    grad_inner_ref[...] = d_mixed * input_ref[...].astype(f32)
    grad_input_ref[...] = d_mixed * inner_ref[...].astype(f32)

    for k in others:
        source = flipped(me, k)
        with scope(f"pw{k}"):
            remote(
                proj_send.at[0],
                proj_got.at[source],
                (out_sem.at[11], proj_sem.at[source]),
                source,
                t,
            ).wait_recv()
    total = proj_got[0].astype(f32)
    for s in range(1, sp_devices):
        total = total + proj_got[s].astype(f32)
    grad_proj_ref[...] = total

    def drained(kind, ref):
        remote(ref, ref, (out_sem.at[kind], conv_sem.at[0]), me, t_core).wait_send()

    pieces = sp_devices - 1
    drained(0, far_route)
    drained(6, rows.at[:, pl.ds(0, pieces * capacity), pl.ds(0, 2 * quarter)])
    drained(7, core_send)
    drained(8, y_send)
    drained(9, back_send.at[pl.ds(0, pieces * capacity)])
    drained(10, stream_grad.at[:, pl.ds(0, 3 * quarter)])
    drained(11, proj_send.at[pl.ds(0, pieces)])

    @pl.when(inside == 0)
    def _():
        drained(1, raw.at[0])
        drained(3, extra_send)
        drained(4, a_send.at[pl.ds(0, sp_devices // 2)])
        drained(5, rows.at[:, pl.ds(0, (pieces - 1) * capacity), pl.ds(0, quarter)])
        route_in[0].wait_recv()

    @pl.when(inside == 1)
    def _():
        drained(1, rows.at[:, :, pl.ds(0, quarter)])
        drained(2, close_send)
        drained(4, a_send)
        drained(5, rows.at[:, pl.ds(0, (pieces - 3) * capacity), pl.ds(0, quarter)])

    @pl.when(me < sp_devices - 1)
    def _():
        to_next.wait_send()

    @pl.when(me > 0)
    def _():
        to_previous.wait_send()


def written(*refs):
    count = (len(refs) - 1) // 2
    sem = refs[-1]
    outs = [
        pltpu.make_async_copy(refs[i], refs[count + i], sem.at[i]) for i in range(count)
    ]
    for out in outs:
        out.start()
    for out in outs:
        out.wait()


def fused_shards(
    out_cotangent,
    stream,
    route_ids,
    route_weights,
    gate_proj,
    up_proj,
    down_proj,
    outer_gate,
    inner_gate,
    conv_input,
    conv_taps,
    out_proj,
):
    f32, bf16 = jnp.float32, jnp.bfloat16
    n = lax.axis_size("sp")
    tokens, width = stream.shape
    units = gate_proj.shape[2]
    channels = out_proj.shape[1]
    capacity = 4 * tokens // n
    slots = n * capacity
    quarter = width // lax.axis_size("tp")
    per = width // n
    labels = [0, 1, 2, 3, 4, 5, 6, 7]
    outer_steps = (
        "X Z E0 R0 U u a3 A3 a2 b3 A2 B3 C3 E3 R3 Y0 V P a1 A1 b1 B1 J C1 E1 R1 b2 B2 K a5 C2"
        " E2 A5 b4 B4 C4 L E4 R4 Y3 a7 M b5 B5 C5 E5 R5 A7 Y4 b6 B6 C6 E6 Y5 R6 b7 B7 C7 E7 R7"
        " R2 Y1 Y6 G H Y7 Y2 D"
    )
    inner_steps = (
        "E0 R0 w J W K a5 a3 b4 B4 S L C4 E4 R4 T M X A5 A3 Z Y0 V P b2 B2 C2 E2 R2 a7 Y4 b5"
        " B5 C5 E5 R5 A7 b6 B6 C6 E6 R6 Y5 Y2 b7 B7 C7 E7 R7 Y6 b3 B3 C3 E3 R3 Y7 a1 A1 b1 B1"
        " C1 E1 Y3 R1 G Y1 H D"
    )
    vmem = pl.BlockSpec(memory_space=pltpu.VMEM)
    hbm = pl.BlockSpec(memory_space=pltpu.HBM)
    anywhere = pl.BlockSpec(memory_space=pl.ANY)
    dma = pltpu.SemaphoreType.DMA
    shapes = [
        ((width, units), bf16),
        ((width, units), bf16),
        ((units, width), bf16),
        ((per, channels), f32),
        ((tokens, channels), f32),
        ((tokens, channels), f32),
        ((tokens, channels), f32),
    ]
    args = (
        out_cotangent,
        stream,
        route_ids.T,
        route_weights.T,
        outer_gate,
        inner_gate,
        conv_input,
        conv_taps,
        out_proj,
        gate_proj[0],
        up_proj[0],
        down_proj[0],
    )
    grads = pl.pallas_call(
        functools.partial(fused, n, labels, outer_steps, inner_steps),
        out_shape=[pltpu.VMEM(*shape) for shape in shapes],
        in_specs=[hbm] * 12,
        out_specs=[vmem] * 7,
        scratch_shapes=[
            pltpu.VMEM((tokens, width), bf16),
            pltpu.VMEM((tokens, width), bf16),
            pltpu.VMEM(route_ids.shape[::-1], jnp.int32),
            pltpu.VMEM(route_ids.shape[::-1], f32),
            pltpu.VMEM((tokens, channels), bf16),
            pltpu.VMEM((tokens, channels), bf16),
            pltpu.VMEM((tokens, channels), bf16),
            pltpu.VMEM(conv_taps.shape, f32),
            pltpu.VMEM((width, channels), bf16),
            pltpu.VMEM((2, n, tokens), f32),
            pltpu.VMEM((3, 2, n, tokens), f32),
            pltpu.VMEM((3, 2, capacity, tokens), bf16),
            pltpu.VMEM((slots, tokens), bf16),
            pltpu.VMEM((3, 2, tokens, quarter), bf16),
            pltpu.VMEM((2, slots, width), bf16),
            pltpu.VMEM((n // 2 + 1, 2, capacity, quarter), bf16),
            pltpu.VMEM((2, 2, capacity, quarter), bf16),
            pltpu.VMEM((2, 2, capacity, quarter), bf16),
            pltpu.VMEM((width, 2 * units), bf16),
            pltpu.VMEM((units, width), bf16),
            pltpu.VMEM((slots, units), bf16),
            pltpu.VMEM((slots, 2 * units), bf16),
            pltpu.VMEM((2, slots, quarter), bf16),
            pltpu.VMEM((slots, quarter), f32),
            pltpu.VMEM((2, slots, quarter), bf16),
            pltpu.VMEM((2, slots, quarter), bf16),
            pltpu.VMEM((slots, quarter), bf16),
            pltpu.VMEM((slots, quarter), bf16),
            pltpu.VMEM((slots, quarter), bf16),
            pltpu.VMEM((slots, quarter), bf16),
            pltpu.VMEM((tokens, width), bf16),
            pltpu.VMEM((n, per, channels), bf16),
            pltpu.VMEM((n, per, channels), bf16),
            pltpu.VMEM((tokens + 8, channels), f32),
            pltpu.VMEM((tokens + 8, channels), f32),
            pltpu.VMEM((tokens, channels), f32),
            pltpu.VMEM((tokens, channels), bf16),
            dma((12,)),
            dma((14,)),
            dma((3,)),
            dma((3, 2)),
            dma((2, n)),
            dma((2, n)),
            dma((n,)),
            dma((2, n)),
            dma((n,)),
            dma((n,)),
            dma((3, quarter // per)),
            dma((n,)),
            dma((2,)),
        ],
        compiler_params=pltpu.CompilerParams(
            collective_id=0, has_side_effects=True, vmem_limit_bytes=48 * 1024 * 1024
        ),
    )(*(pltpu.with_memory_space_constraint(arg, pltpu.HBM) for arg in args))
    outs = pl.pallas_call(
        written,
        out_shape=[jax.ShapeDtypeStruct(*shape) for shape in shapes],
        in_specs=[anywhere] * 7,
        out_specs=[hbm] * 7,
        scratch_shapes=[dma((7,))],
        compiler_params=pltpu.CompilerParams(vmem_limit_bytes=1024 * 1024),
    )(*(pltpu.with_memory_space_constraint(grad, pltpu.VMEM) for grad in grads))
    return (outs[0][None], outs[1][None], outs[2][None], *outs[3:])


def fits_kernel(mesh):
    return mesh.shape["sp"] == 8 and mesh.shape["tp"] == 4


def solution(mesh):
    placed = (
        P("sp", None),
        P("sp", None),
        P("sp", None),
        P("sp", None),
        P("sp", None, "tp"),
        P("sp", None, "tp"),
        P("sp", "tp", None),
        P("sp", "tp"),
        P("sp", "tp"),
        P("sp", "tp"),
        P(None, "tp"),
        P(None, "tp"),
    )
    return jax.shard_map(
        fused_shards if fits_kernel(mesh) else shards,
        mesh=mesh,
        in_specs=placed,
        out_specs=(
            P("sp", None, "tp"),
            P("sp", None, "tp"),
            P("sp", "tp", None),
            P("sp", "tp"),
            P("sp", "tp"),
            P("sp", "tp"),
            P("sp", "tp"),
        ),
        check_vma=False,
    )
```

```python
import functools

import jax
import jax.numpy as jnp
from jax import lax
from jax.experimental import pallas as pl
from jax.experimental.pallas import tpu as pltpu
from jax.sharding import PartitionSpec as P


def passed_along(x, axis, by):
    devices = lax.axis_size(axis)
    pairs = [(i, i + by) for i in range(devices) if 0 <= i + by < devices]
    return lax.ppermute(x, axis, pairs)


def to_owners(x, devices):
    blocks = x.reshape(devices, -1, x.shape[1])
    return lax.all_to_all(blocks, "sp", split_axis=0, concat_axis=0, tiled=True).reshape(x.shape)


def partial_rows(d_gate, d_up, w_gate, w_up):
    across = (((1,), (1,)), ((), ()))
    total = lax.dot_general(
        d_gate, w_gate, across, preferred_element_type=jnp.float32
    ) + lax.dot_general(d_up, w_up, across, preferred_element_type=jnp.float32)
    return total.astype(jnp.bfloat16)


def reduced_quarter(d_gate, d_up, w_gate, w_up):
    devices = lax.axis_size("tp")
    if devices != 4:
        return lax.psum_scatter(
            partial_rows(d_gate, d_up, w_gate, w_up), "tp", scatter_dimension=1, tiled=True
        )
    quarter = w_gate.shape[0] // devices
    me = lax.axis_index("tp")

    def rows_of(w, *flips):
        return jnp.concatenate(
            [lax.dynamic_slice_in_dim(w, (me ^ flip) * quarter, quarter, 0) for flip in flips]
        )

    def swapped(x, flip):
        return lax.ppermute(x, "tp", [(i, i ^ flip) for i in range(devices)])

    sent = partial_rows(d_gate, d_up, rows_of(w_gate, 1, 3), rows_of(w_up, 1, 3))
    got = swapped(sent, 1)
    kept = partial_rows(d_gate, d_up, rows_of(w_gate, 0, 2), rows_of(w_up, 0, 2))
    far = kept[:, quarter:].astype(jnp.float32) + got[:, quarter:].astype(jnp.float32)
    near = kept[:, :quarter].astype(jnp.float32) + got[:, :quarter].astype(jnp.float32)
    other = swapped(far.astype(jnp.bfloat16), 2)
    return (near + other.astype(jnp.float32)).astype(jnp.bfloat16)


def shards(
    out_cotangent,
    stream,
    route_ids,
    route_weights,
    gate_proj,
    up_proj,
    down_proj,
    outer_gate,
    inner_gate,
    conv_input,
    conv_taps,
    out_proj,
):
    sp_devices = lax.axis_size("sp")
    tokens_here, width = stream.shape
    experts = sp_devices * gate_proj.shape[0]
    capacity = 4 * tokens_here // experts
    quarter = width // lax.axis_size("tp")
    first_column = lax.axis_index("tp") * quarter
    own_cotangent = lax.dynamic_slice_in_dim(out_cotangent, first_column, quarter, 1)
    own_stream = lax.dynamic_slice_in_dim(stream, first_column, quarter, 1)
    over_rows = (((0,), (0,)), ((), ()))
    expert_ids = jnp.arange(experts, dtype=jnp.int32)
    chosen = route_ids[:, :, None] == expert_ids
    hit = jnp.any(chosen, axis=1)
    token_weight = jnp.sum(jnp.where(chosen, route_weights[:, :, None], 0.0), axis=1)
    token_ids = jnp.arange(tokens_here, dtype=jnp.int32)
    below = (token_ids[:, None] < token_ids[None, :]).astype(jnp.bfloat16)
    rank = lax.dot_general(
        hit.astype(jnp.bfloat16), below, over_rows, preferred_element_type=jnp.float32
    )
    rank = jnp.where(hit.T, rank, -1.0)
    in_slot = rank[:, None, :] == jnp.arange(capacity, dtype=jnp.float32)[None, :, None]
    slot_weight = jnp.sum(jnp.where(in_slot, token_weight.T[:, None, :], 0.0), axis=2)
    pick = in_slot.astype(jnp.bfloat16).reshape(experts * capacity, tokens_here)
    send_input = jnp.dot(pick, own_stream, preferred_element_type=jnp.float32).astype(jnp.bfloat16)
    send_grad = (
        slot_weight.reshape(-1, 1)
        * jnp.dot(pick, own_cotangent, preferred_element_type=jnp.float32)
    ).astype(jnp.bfloat16)
    got_input = to_owners(send_input, sp_devices)
    rows_input = lax.all_gather(got_input, "tp", axis=1, tiled=True)
    send_grad, got_input = lax.optimization_barrier((send_grad, got_input))
    got_grad = to_owners(send_grad, sp_devices)
    rows_grad = lax.all_gather(got_grad, "tp", axis=1, tiled=True)
    mixed = inner_gate.astype(jnp.float32) * conv_input.astype(jnp.float32)
    previous = passed_along(mixed[tokens_here - 2 :], "sp", 1)
    extended = jnp.concatenate([previous, mixed], axis=0)
    conv_out = (
        conv_taps[0] * extended[:tokens_here]
        + conv_taps[1] * extended[1 : tokens_here + 1]
        + conv_taps[2] * extended[2:]
    )
    mixer_out = (outer_gate.astype(jnp.float32) * conv_out).astype(jnp.bfloat16)
    conv_out, mixer_out, rows_grad = lax.optimization_barrier((conv_out, mixer_out, rows_grad))
    w_gate = gate_proj[0]
    w_up = up_proj[0]
    w_down = down_proj[0]
    gate = jnp.dot(rows_input, w_gate, preferred_element_type=jnp.float32)
    up = jnp.dot(rows_input, w_up, preferred_element_type=jnp.float32)
    sig = jax.nn.sigmoid(gate)
    silu_gate = gate * sig
    hidden = (silu_gate * up).astype(jnp.bfloat16)
    across = (((1,), (1,)), ((), ()))
    d_hidden = lax.dot_general(rows_grad, w_down, across, preferred_element_type=jnp.float32)
    d_gate = (d_hidden * up * sig * (1.0 + gate * (1.0 - sig))).astype(jnp.bfloat16)
    d_up = (d_hidden * silu_gate).astype(jnp.bfloat16)
    grad_down = lax.dot_general(
        hidden, rows_grad, over_rows, preferred_element_type=jnp.float32
    ).astype(jnp.bfloat16)
    grad_gate = lax.dot_general(
        rows_input, d_gate, over_rows, preferred_element_type=jnp.float32
    ).astype(jnp.bfloat16)
    grad_up = lax.dot_general(
        rows_input, d_up, over_rows, preferred_element_type=jnp.float32
    ).astype(jnp.bfloat16)
    chunks = 2
    piece = capacity // chunks
    shape = (sp_devices, chunks, piece, d_gate.shape[1])
    gate_pieces = d_gate.reshape(shape)
    up_pieces = d_up.reshape(shape)
    shares = []
    for c in range(chunks):
        shares.append(
            reduced_quarter(
                gate_pieces[:, c].reshape(-1, shape[3]),
                up_pieces[:, c].reshape(-1, shape[3]),
                w_gate,
                w_up,
            )
        )
    shares[0], grad_down, grad_gate, grad_up = lax.optimization_barrier(
        (shares[0], grad_down, grad_gate, grad_up)
    )
    moe_grad = own_cotangent.astype(jnp.float32)
    pick_pieces = pick.reshape(experts, chunks, piece, tokens_here)
    for c in range(chunks):
        returned = to_owners(shares[c], sp_devices)
        moe_grad = moe_grad + lax.dot_general(
            pick_pieces[:, c].reshape(-1, tokens_here), returned, over_rows,
            preferred_element_type=jnp.float32,
        )
    stream_part = moe_grad.astype(jnp.bfloat16)
    stream_grad = lax.all_gather(stream_part, "tp", axis=1, tiled=True)
    own_projection = lax.dot_general(
        stream_grad, mixer_out, over_rows, preferred_element_type=jnp.float32
    ).astype(jnp.bfloat16)
    projections = to_owners(own_projection, sp_devices)
    grad_projection = jnp.sum(
        projections.astype(jnp.float32).reshape(sp_devices, -1, projections.shape[1]), axis=0
    )
    d_mixer = jnp.dot(stream_grad, out_proj, preferred_element_type=jnp.float32)
    grad_outer = d_mixer * conv_out
    d_conv = d_mixer * outer_gate.astype(jnp.float32)
    following = passed_along(d_conv[:2], "sp", -1)
    trailing = jnp.concatenate([d_conv, following], axis=0)
    d_mixed = (
        conv_taps[2] * trailing[:tokens_here]
        + conv_taps[1] * trailing[1 : tokens_here + 1]
        + conv_taps[0] * trailing[2:]
    )
    grad_inner = d_mixed * conv_input.astype(jnp.float32)
    grad_input = d_mixed * inner_gate.astype(jnp.float32)
    return (
        grad_gate[None],
        grad_up[None],
        grad_down[None],
        grad_projection,
        grad_outer,
        grad_inner,
        grad_input,
    )


MESH = pl.DeviceIdType.MESH


def flipped(index, flips):
    place = 1
    while place <= flips:
        if (flips // place) % 2:
            index = index + place * (1 - 2 * ((index // place) % 2))
        place *= 2
    return index


def fused(
    sp_devices,
    labels,
    outer_steps,
    inner_steps,
    cot_hbm,
    stream_hbm,
    ids_hbm,
    weights_hbm,
    outer_hbm,
    inner_hbm,
    input_hbm,
    taps_hbm,
    out_proj_hbm,
    w_gate_hbm,
    w_up_hbm,
    w_down_hbm,
    grad_gate_ref,
    grad_up_ref,
    grad_down_ref,
    grad_proj_ref,
    grad_outer_ref,
    grad_inner_ref,
    grad_input_ref,
    cot_ref,
    stream_ref,
    ids_ref,
    weights_ref,
    outer_ref,
    inner_ref,
    input_ref,
    taps_ref,
    out_proj_ref,
    route,
    far_route,
    far_pick,
    pick_ref,
    raw,
    rows,
    a_send,
    close_send,
    extra_send,
    w_pair,
    w_down,
    hidden,
    d_pair,
    kept,
    near_got,
    core_send,
    core_got,
    y_send,
    y_got,
    back_send,
    back_got,
    stream_grad,
    proj_send,
    proj_got,
    before,
    after,
    conv_out,
    mixer_out,
    load_sem,
    out_sem,
    route_sem,
    raw_sem,
    a_sem,
    b_sem,
    c_sem,
    core_sem,
    y_sem,
    back_sem,
    gather_sem,
    proj_sem,
    conv_sem,
):
    f32, bf16 = jnp.float32, jnp.bfloat16
    scope = jax.named_scope
    me = lax.axis_index("sp")
    t = lax.axis_index("tp")
    t_core, t_y = flipped(t, 1), flipped(t, 2)
    half = lax.axis_size("tp") // 2
    tokens, width = stream_ref.shape
    capacity = pick_ref.shape[0] // sp_devices
    units = hidden.shape[1]
    quarter = width // lax.axis_size("tp")
    per = width // sp_devices
    over_rows = (((0,), (0,)), ((), ()))
    across = (((1,), (1,)), ((), ()))
    others = range(1, sp_devices)

    def owned(member):
        return (member % 2) * half + member // 2

    q, q_core, q_y, q_far = owned(t), owned(t_core), owned(t_y), owned(flipped(t, 3))

    def columns(index):
        return pl.ds(pl.multiple_of(index * quarter, quarter), quarter)

    def block(p):
        return pl.ds(p * capacity, capacity)

    def dynamic_block(p):
        return pl.ds(pl.multiple_of(p * capacity, capacity), capacity)

    def remote(src, dst, sems, sp, tp):
        return pltpu.make_async_remote_copy(
            src_ref=src,
            dst_ref=dst,
            send_sem=sems[0],
            recv_sem=sems[1],
            device_id=(sp, tp),
            device_id_type=MESH,
        )

    peers = [(flipped(me, k), t) for k in others] + [(me, t_core), (me, t_y)]
    barrier = pltpu.get_barrier_semaphore()
    for peer in peers:
        pl.semaphore_signal(barrier, inc=1, device_id=peer, device_id_type=MESH)

    moved = [
        (ids_hbm, ids_ref),
        (weights_hbm, weights_ref),
        (inner_hbm, inner_ref),
        (input_hbm, input_ref),
        (stream_hbm, stream_ref),
        (cot_hbm, cot_ref),
        (w_gate_hbm, w_pair.at[:, pl.ds(0, units)]),
        (w_up_hbm, w_pair.at[:, pl.ds(units, units)]),
        (w_down_hbm, w_down),
        (outer_hbm, outer_ref),
        (taps_hbm, taps_ref),
        (out_proj_hbm, out_proj_ref),
    ]
    loads = [
        pltpu.make_async_copy(src, dst, load_sem.at[i]) for i, (src, dst) in enumerate(moved)
    ]
    for load in loads:
        load.start()

    with scope("prep"):
        for load in loads[:4]:
            load.wait()
        before[pl.ds(8, tokens), :] = inner_ref[...].astype(f32) * input_ref[...].astype(f32)
        expert_ids = lax.broadcasted_iota(jnp.int32, (sp_devices, tokens), 0)
        chosen = [ids_ref[j : j + 1, :] == expert_ids for j in range(ids_ref.shape[0])]
        hit = jnp.zeros((sp_devices, tokens), f32)
        weight = jnp.zeros((sp_devices, tokens), f32)
        for j, choice in enumerate(chosen):
            hit = jnp.where(choice, 1.0, hit)
            weight = jnp.where(choice, weights_ref[j : j + 1, :], weight)
        earlier = lax.broadcasted_iota(jnp.int32, (tokens, tokens), 0)
        later = lax.broadcasted_iota(jnp.int32, (tokens, tokens), 1)
        below = jnp.where(earlier < later, 1.0, 0.0).astype(bf16)
        rank = jnp.dot(hit.astype(bf16), below, preferred_element_type=f32)
        route[0] = jnp.where(hit > 0.0, rank, -1.0)
        route[1] = weight
        slot = lax.broadcasted_iota(jnp.int32, (capacity, tokens), 0).astype(f32)

    def slots_of(ref, expert):
        return ref[0, pl.ds(expert, 1), :] == slot

    def one_hot(chosen_slot):
        return jnp.where(chosen_slot, 1.0, 0.0).astype(bf16)

    def scale_of(ref, expert, chosen_slot):
        return jnp.sum(
            jnp.where(chosen_slot, ref[1, pl.ds(expert, 1), :], 0.0), axis=1, keepdims=True
        )

    def compacted(expert, ranges):
        chosen_slot = slots_of(route, expert)
        pick = one_hot(chosen_slot)
        pick_ref[dynamic_block(expert), :] = pick
        scale = scale_of(route, expert, chosen_slot)
        return [
            (
                jnp.dot(pick, stream_ref[:, at], preferred_element_type=f32).astype(bf16),
                (scale * jnp.dot(pick, cot_ref[:, at], preferred_element_type=f32)).astype(bf16),
            )
            for at in ranges
        ]

    z, side = me // 2, me % 2
    upper = z // 2
    inside = (z + upper) % 2
    across_x, near, opposite = flipped(me, 1), flipped(me, 2), flipped(me, 6)
    lines = [z, z + 1 - 2 * (z % 2), 2 - upper, 3 - 3 * upper]
    place = {label: p for p, label in enumerate(labels)}
    a, a_extra, b, c_near, c_far, back_out, back_in, partners = {}, {}, {}, {}, {}, {}, {}, {}
    for label in range(sp_devices):
        p = place[label]
        across_side = 1 - side if label % 2 else side
        partner = partners[p] = 2 * lines[label // 2] + across_side
        a[p], a_extra[p], b[p], c_near[p], c_far[p] = [], [], [], [], []
        for i in range(2):
            mine, theirs = rows.at[i, block(p), columns(q)], rows.at[i, block(p), columns(q_y)]
            if label % 2:
                a[p].append(
                    remote(
                        a_send.at[label // 2, i],
                        mine,
                        (out_sem.at[4], a_sem.at[i, p]),
                        across_x,
                        t,
                    )
                )
            if label == 1:
                a_extra[p].append(
                    remote(
                        a_send.at[sp_devices // 2, i],
                        theirs,
                        (out_sem.at[4], a_sem.at[i, 0]),
                        across_x,
                        t,
                    )
                )
            b[p].append(remote(mine, mine, (out_sem.at[5], b_sem.at[i, p]), me, t_y))
            c_near[p].append(
                remote(mine, mine, (out_sem.at[6], c_sem.at[p]), me, t_core)
            )
            c_far[p].append(
                remote(theirs, theirs, (out_sem.at[6], c_sem.at[p]), me, t_core)
            )
        back_out[p] = remote(
            back_send.at[block(p)],
            back_got.at[dynamic_block(me)],
            (out_sem.at[9], back_sem.at[me]),
            partner,
            t,
        )
        back_in[p] = remote(
            back_send.at[block(p)],
            back_got.at[dynamic_block(partner)],
            (out_sem.at[9], back_sem.at[partner]),
            partner,
            t,
        )
    close = [
        [
            remote(
                close_send.at[j, i],
                rows.at[i, block(place[2 + j]), columns(q)],
                (out_sem.at[2], a_sem.at[i, place[2 + j]]),
                flipped(me, 2 + j),
                t,
            )
            for i in range(2)
        ]
        for j in range(2)
    ]
    extra_out, extra_in = (
        [
            [
                remote(
                    extra_send.at[j, i],
                    rows.at[i, block(place[2 + j]), columns(q_y)],
                    (out_sem.at[3], b_sem.at[i, place[2 + j]]),
                    flipped(me, 2 + j),
                    t,
                )
                for i in range(2)
            ]
            for j in range(2)
        ]
        for _ in range(2)
    )
    to_near, to_opposite, on_opposite, on_near = [], [], [], [[], []]
    for i, ref in enumerate((stream_ref, cot_ref)):
        own = ref.at[:, columns(q)]
        to_near.append(
            remote(own, raw.at[0, i], (out_sem.at[1], raw_sem.at[0, i]), near, t)
        )
        to_opposite.append(
            remote(own, raw.at[1, i], (out_sem.at[1], raw_sem.at[1, i]), opposite, t)
        )
        on_opposite.append(
            remote(raw.at[0, i], raw.at[2, i], (out_sem.at[1], raw_sem.at[2, i]), opposite, t)
        )
        for j in range(2):
            on_near[j].append(
                remote(
                    raw.at[1 + j, i],
                    raw.at[1 + j, i],
                    (out_sem.at[1], raw_sem.at[1 + j, i]),
                    near,
                    t,
                )
            )
    as_far = 2 - inside
    route_out = [
        remote(route, far_route.at[0], (out_sem.at[0], route_sem.at[0]), near, t)
    ] + [
        remote(
            route,
            far_route.at[as_far],
            (out_sem.at[0], route_sem.at[as_far]),
            flipped(me, 2 + 2 * j),
            t,
        )
        for j in (1, 2)
    ]
    route_in = [
        remote(route, far_route.at[j], (out_sem.at[0], route_sem.at[j]), near, t)
        for j in range(3)
    ]
    to_next = remote(
        before.at[pl.ds(tokens, 8)],
        before.at[pl.ds(0, 8)],
        (out_sem.at[12], conv_sem.at[0]),
        me + 1,
        t,
    )
    to_previous = remote(
        after.at[pl.ds(0, 8)],
        after.at[pl.ds(tokens, 8)],
        (out_sem.at[13], conv_sem.at[1]),
        me - 1,
        t,
    )

    with scope("barrier"):
        pl.semaphore_wait(barrier, len(peers))
    for out in route_out:
        out.start()

    @pl.when(me < sp_devices - 1)
    def _():
        to_next.start()

    for i in range(2):
        loads[4 + i].wait()

        @pl.when(inside == 0)
        def _():
            to_near[i].start()

        @pl.when(inside == 1)
        def _():
            to_opposite[i].start()

    @pl.when(inside == 1)
    def _():
        for j in (1, 0):
            close_send[j, 0], close_send[j, 1] = compacted(flipped(me, 2 + j), [columns(q)])[0]
            for i in range(2):
                close[j][i].start()

    own = compacted(me, [pl.ds(0, width)])[0]
    rows[0, block(place[0]), :], rows[1, block(place[0]), :] = own
    for load in loads[6:]:
        load.wait()

    core, y_hop = {}, {}
    for p in range(len(labels)):
        core[p] = [
            remote(
                core_send.at[i, block(p)],
                core_got.at[i, block(p)],
                (out_sem.at[7], core_sem.at[i, p]),
                me,
                t_core,
            )
            for i in range(2)
        ]
        y_hop[p] = remote(
            y_send.at[block(p)], y_got.at[block(p)], (out_sem.at[8], y_sem.at[p]), me, t_y
        )

    def compact_far(line, i, direct):
        far = far_route.at[line - 1]
        if i == 0:
            route_in[line - 1].wait_recv()
        for j, expert in enumerate((me, across_x)):
            chosen_slot = slots_of(far, expert)
            if i == 0:
                pick = one_hot(chosen_slot)
                far_pick[line - 1, j] = pick
            else:
                pick = far_pick[line - 1, j]
            part = jnp.dot(pick, raw[line - 1, i], preferred_element_type=f32)
            if i:
                part = scale_of(far, expert, chosen_slot) * part
            p = place[2 * line + j]
            if j:
                a_send[line, i] = part.astype(bf16)
                a[p][i].start()
            else:
                rows[i, block(p), columns(q)] = part.astype(bf16)
                if 2 * line not in direct:
                    b[p][i].start()
                c_near[p][i].start()

    def first_line(i, direct):
        def go(_):
            to_near[i].wait_recv()
            on_opposite[i].start()
            to_opposite[i].wait_recv()
            on_near[0][i].start()
            compact_far(1, i, direct)

        return go

    def relay(i):
        def go(_):
            on_opposite[i].wait_recv()
            on_near[1][i].start()

        return go

    def later_line(line, i, waits):
        def go(_):
            if waits:
                on_near[line - 2][i].wait_recv()
            compact_far(line, i, ())

        return go

    def to_side(_):
        p = place[1]
        both = compacted(across_x, [columns(q), columns(q_y)])
        a_send[0, 0], a_send[0, 1] = both[0]
        a_send[sp_devices // 2, 0], a_send[sp_devices // 2, 1] = both[1]
        for i in range(2):
            a[p][i].start()

    def to_side_more(_):
        for copy in a_extra[place[1]]:
            copy.start()

    def other_picks(_):
        for k in range(2, sp_devices):
            expert = flipped(me, k)
            pick_ref[dynamic_block(expert), :] = one_hot(slots_of(route, expert))

    def to_close_more(j):
        def go(_):
            extra_send[j, 0], extra_send[j, 1] = compacted(flipped(me, 2 + j), [columns(q_y)])[0]
            for copy in extra_out[j]:
                copy.start()

        return go

    def arrive(i, direct):
        def go(p):
            (a[p] or close[0])[i].wait_recv()
            if labels[p] not in direct:
                b[p][i].start()
            c_near[p][i].start()

        return go

    def cross(i, direct):
        def go(p):
            if labels[p] == 1:
                a_extra[p][i].wait_recv()
            elif labels[p] in direct:
                extra_in[labels[p] - 2][i].wait_recv()
            else:
                b[p][i].wait_recv()
            c_far[p][i].start()

        return go

    def gather(p):
        four = core_got.at[:, pl.ds(0, 2 * capacity)]
        remote(four, four, (out_sem.at[6], c_sem.at[p]), me, t_core).wait_recv()

    def expert(p):
        span = block(p)
        both = jnp.dot(rows[0, span, :], w_pair[...], preferred_element_type=f32)
        gate, up = both[:, :units], both[:, units:]
        d_hidden = lax.dot_general(
            rows[1, span, :], w_down[...], across, preferred_element_type=f32
        )
        sig = jax.nn.sigmoid(gate)
        silu_gate = gate * sig
        hidden[span, :] = (silu_gate * up).astype(bf16)
        d_gate = (d_hidden * up * sig * (1.0 + gate * (1.0 - sig))).astype(bf16)
        d_up = (d_hidden * silu_gate).astype(bf16)
        d_pair[span, pl.ds(0, units)] = d_gate
        d_pair[span, pl.ds(units, units)] = d_up

        def partial(index):
            return lax.dot_general(
                d_pair[span, :], w_pair[columns(index), :], across, preferred_element_type=f32
            ).astype(bf16)

        core_send[1, span, :] = partial(q_far)
        core_send[0, span, :] = partial(q_core)
        core[p][1].start()
        kept[1, span, :] = partial(q_y)
        core[p][0].start()
        kept[0, span, :] = partial(q)

    def reduce_core(p):
        span = block(p)
        core[p][1].wait_recv()
        y_send[span, :] = (
            kept[1, span, :].astype(f32) + core_got[1, span, :].astype(f32)
        ).astype(bf16)
        y_hop[p].start()
        core[p][0].wait_recv()
        near_got[span, :] = kept[0, span, :].astype(f32) + core_got[0, span, :].astype(f32)

    def reduce_y(p):
        span = block(p)
        y_hop[p].wait_recv()
        back_send[span, :] = (near_got[span, :] + y_got[span, :].astype(f32)).astype(bf16)
        if labels[p]:
            back_out[p].start()
        else:
            back_got[dynamic_block(me), :] = back_send[span, :]

    def convolve(p):
        @pl.when(me == 0)
        def _():
            before[pl.ds(0, 8), :] = jnp.zeros((8, before.shape[1]), f32)

        @pl.when(me > 0)
        def _():
            to_next.wait_recv()

        conv = (
            taps_ref[0:1, :] * before[pl.ds(6, tokens), :]
            + taps_ref[1:2, :] * before[pl.ds(7, tokens), :]
            + taps_ref[2:3, :] * before[pl.ds(8, tokens), :]
        )
        conv_out[...] = conv
        mixer_out[...] = (outer_ref[...].astype(f32) * conv).astype(bf16)

    step = 2 * units

    def down(j, carry):
        at = pl.ds(pl.multiple_of(j * step, step), step)
        grad_down_ref[:, at] = lax.dot_general(
            hidden[...], rows[1, :, at], over_rows, preferred_element_type=f32
        ).astype(bf16)
        return carry

    def gate_up(j, carry):
        at = pl.ds(pl.multiple_of(j * units, units), units)
        both = lax.dot_general(
            rows[0, :, at], d_pair[...], over_rows, preferred_element_type=f32
        ).astype(bf16)
        grad_gate_ref[at, :] = both[:, :units]
        grad_up_ref[at, :] = both[:, units:]
        return carry

    def first_gate_up(p):
        lax.fori_loop(0, width // units // 2, gate_up, 0)

    def second_gate_up(p):
        lax.fori_loop(width // units // 2, width // units, gate_up, 0)

    def all_down(p):
        lax.fori_loop(0, width // step, down, 0)

    def follow(steps, waits, direct):
        run = dict(
            a=arrive(0, direct),
            A=arrive(1, direct),
            b=cross(0, direct),
            B=cross(1, direct),
            C=gather,
            E=expert,
            R=reduce_core,
            Y=reduce_y,
            V=convolve,
            G=first_gate_up,
            H=second_gate_up,
            D=all_down,
            w=first_line(0, direct),
            W=first_line(1, direct),
            U=to_close_more(0),
            u=to_close_more(1),
            X=to_side,
            Z=to_side_more,
            P=other_picks,
            J=later_line(2, 0, waits),
            K=later_line(2, 1, waits),
            L=later_line(3, 0, waits),
            M=later_line(3, 1, waits),
            S=relay(0),
            T=relay(1),
        )
        for item in steps.split():
            with scope(item):
                run[item[0]](place.get(int(item[1:] or 0)))

    @pl.when(inside == 0)
    def _():
        follow(outer_steps, True, (1,))

    @pl.when(inside == 1)
    def _():
        follow(inner_steps, False, (1, 2, 3))

    for p, label in enumerate(labels):
        if label:
            with scope(f"back{label}"):
                back_in[p].wait_recv()
    share = quarter // per
    cut = per // 2
    cuts = quarter // cut

    def piece_of(index, i):
        return pl.ds(pl.multiple_of(index * quarter + i * cut, cut), cut)

    gathers = []
    for i in range(cuts):
        part, part_y = stream_grad.at[:, piece_of(q, i)], stream_grad.at[:, piece_of(q_y, i)]
        gathers.append(
            [
                remote(part, part, (out_sem.at[10], gather_sem.at[0, i]), me, t_y),
                remote(part, part, (out_sem.at[10], gather_sem.at[1, i]), me, t_core),
                remote(part_y, part_y, (out_sem.at[10], gather_sem.at[2, i]), me, t_core),
            ]
        )

    def project(j, index, i):
        piece = stream_grad[:, piece_of(index, i)]
        proj_send[j * cuts + i] = lax.dot_general(
            piece, mixer_out[...], over_rows, preferred_element_type=f32
        ).astype(bf16)
        owner = index * share + i // 2
        landing = proj_got.at[me, pl.ds(i % 2 * cut, cut)]
        send = remote(
            proj_send.at[j * cuts + i], landing, (out_sem.at[11], proj_sem.at[me]), owner, t
        )

        @pl.when(owner != me)
        def _():
            send.start()

        @pl.when(owner == me)
        def _():
            landing[...] = proj_send[j * cuts + i]

        return jnp.dot(piece, out_proj_ref[piece_of(index, i), :], preferred_element_type=f32)

    for i in range(share):
        at = pl.ds(pl.multiple_of(q * quarter + i * per, per), per)
        moe_grad = lax.dot_general(
            pick_ref[...],
            back_got[:, pl.ds(i * per, per)],
            over_rows,
            preferred_element_type=f32,
        )
        stream_grad[:, at] = (cot_ref[:, at].astype(f32) + moe_grad).astype(bf16)
        for k in (2 * i, 2 * i + 1):
            gathers[k][0].start()
            gathers[k][1].start()
    d_mixer = project(0, q, 0)
    for i in range(1, cuts):
        d_mixer = d_mixer + project(0, q, i)
    for i in range(cuts):
        with scope(f"g1{i}"):
            gathers[i][1].wait_recv()
        d_mixer = d_mixer + project(1, q_core, i)
    for i in range(cuts):
        with scope(f"g0{i}"):
            gathers[i][0].wait_recv()
        gathers[i][2].start()
        d_mixer = d_mixer + project(2, q_y, i)
        with scope(f"g2{i}"):
            gathers[i][2].wait_recv()
        d_mixer = d_mixer + project(3, q_far, i)

    d_conv = d_mixer * outer_ref[...].astype(f32)
    after[pl.ds(0, tokens), :] = d_conv
    grad_outer_ref[...] = d_mixer * conv_out[...]

    @pl.when(me > 0)
    def _():
        to_previous.start()

    @pl.when(me == sp_devices - 1)
    def _():
        after[pl.ds(tokens, 8), :] = jnp.zeros((8, after.shape[1]), f32)

    with scope("prevw"):

        @pl.when(me < sp_devices - 1)
        def _():
            to_previous.wait_recv()

    d_mixed = (
        taps_ref[2:3, :] * after[pl.ds(0, tokens), :]
        + taps_ref[1:2, :] * after[pl.ds(1, tokens), :]
        + taps_ref[0:1, :] * after[pl.ds(2, tokens), :]
    )
    grad_inner_ref[...] = d_mixed * input_ref[...].astype(f32)
    grad_input_ref[...] = d_mixed * inner_ref[...].astype(f32)

    for k in others:
        source = flipped(me, k)
        with scope(f"pw{k}"):
            remote(
                proj_got.at[source],
                proj_got.at[source],
                (out_sem.at[11], proj_sem.at[source]),
                source,
                t,
            ).wait_recv()
    total = proj_got[0].astype(f32)
    for s in range(1, sp_devices):
        total = total + proj_got[s].astype(f32)
    grad_proj_ref[...] = total

    def drained(kind, ref):
        remote(ref, ref, (out_sem.at[kind], conv_sem.at[0]), me, t_core).wait_send()

    pieces = sp_devices - 1
    drained(0, far_route)
    drained(6, rows.at[:, pl.ds(0, pieces * capacity), pl.ds(0, 2 * quarter)])
    drained(7, core_send)
    drained(8, y_send)
    drained(9, back_send.at[pl.ds(0, pieces * capacity)])
    drained(10, stream_grad.at[:, pl.ds(0, 3 * quarter)])
    drained(11, proj_send.at[pl.ds(0, 2 * pieces)])

    @pl.when(inside == 0)
    def _():
        drained(1, raw.at[0])
        drained(3, extra_send)
        drained(4, a_send.at[pl.ds(0, sp_devices // 2)])
        drained(5, rows.at[:, pl.ds(0, (pieces - 1) * capacity), pl.ds(0, quarter)])
        route_in[0].wait_recv()

    @pl.when(inside == 1)
    def _():
        drained(1, rows.at[:, :, pl.ds(0, quarter)])
        drained(2, close_send)
        drained(4, a_send)
        drained(5, rows.at[:, pl.ds(0, (pieces - 3) * capacity), pl.ds(0, quarter)])

    @pl.when(me < sp_devices - 1)
    def _():
        to_next.wait_send()

    @pl.when(me > 0)
    def _():
        to_previous.wait_send()


def written(*refs):
    count = (len(refs) - 1) // 2
    sem = refs[-1]
    outs = [
        pltpu.make_async_copy(refs[i], refs[count + i], sem.at[i]) for i in range(count)
    ]
    for out in outs:
        out.start()
    for out in outs:
        out.wait()


def fused_shards(
    out_cotangent,
    stream,
    route_ids,
    route_weights,
    gate_proj,
    up_proj,
    down_proj,
    outer_gate,
    inner_gate,
    conv_input,
    conv_taps,
    out_proj,
):
    f32, bf16 = jnp.float32, jnp.bfloat16
    n = lax.axis_size("sp")
    tokens, width = stream.shape
    units = gate_proj.shape[2]
    channels = out_proj.shape[1]
    capacity = 4 * tokens // n
    slots = n * capacity
    quarter = width // lax.axis_size("tp")
    per = width // n
    labels = [0, 1, 2, 3, 4, 5, 6, 7]
    outer_steps = (
        "X Z E0 R0 U u a3 A3 a2 b3 A2 B3 C3 E3 R3 Y0 V P a1 A1 b1 B1 J C1 E1 R1 b2 B2 K a5 C2"
        " E2 A5 b4 B4 C4 L E4 R4 Y3 a7 M b5 B5 C5 E5 R5 A7 Y4 b6 B6 C6 E6 Y5 R6 b7 B7 C7 E7 R7"
        " R2 Y1 Y6 G H Y7 Y2 D"
    )
    inner_steps = (
        "E0 R0 w J W K a5 a3 b4 B4 S L C4 E4 R4 T M X A5 A3 Z Y0 V P b2 B2 C2 E2 R2 a7 Y4 b5"
        " B5 C5 E5 R5 A7 b6 B6 C6 E6 R6 Y5 Y2 b7 B7 C7 E7 R7 Y6 b3 B3 C3 E3 R3 Y7 a1 A1 b1 B1"
        " C1 E1 Y3 R1 G Y1 H D"
    )
    vmem = pl.BlockSpec(memory_space=pltpu.VMEM)
    hbm = pl.BlockSpec(memory_space=pltpu.HBM)
    anywhere = pl.BlockSpec(memory_space=pl.ANY)
    dma = pltpu.SemaphoreType.DMA
    shapes = [
        ((width, units), bf16),
        ((width, units), bf16),
        ((units, width), bf16),
        ((per, channels), f32),
        ((tokens, channels), f32),
        ((tokens, channels), f32),
        ((tokens, channels), f32),
    ]
    args = (
        out_cotangent,
        stream,
        route_ids.T,
        route_weights.T,
        outer_gate,
        inner_gate,
        conv_input,
        conv_taps,
        out_proj,
        gate_proj[0],
        up_proj[0],
        down_proj[0],
    )
    grads = pl.pallas_call(
        functools.partial(fused, n, labels, outer_steps, inner_steps),
        out_shape=[pltpu.VMEM(*shape) for shape in shapes],
        in_specs=[hbm] * 12,
        out_specs=[vmem] * 7,
        scratch_shapes=[
            pltpu.VMEM((tokens, width), bf16),
            pltpu.VMEM((tokens, width), bf16),
            pltpu.VMEM(route_ids.shape[::-1], jnp.int32),
            pltpu.VMEM(route_ids.shape[::-1], f32),
            pltpu.VMEM((tokens, channels), bf16),
            pltpu.VMEM((tokens, channels), bf16),
            pltpu.VMEM((tokens, channels), bf16),
            pltpu.VMEM(conv_taps.shape, f32),
            pltpu.VMEM((width, channels), bf16),
            pltpu.VMEM((2, n, tokens), f32),
            pltpu.VMEM((3, 2, n, tokens), f32),
            pltpu.VMEM((3, 2, capacity, tokens), bf16),
            pltpu.VMEM((slots, tokens), bf16),
            pltpu.VMEM((3, 2, tokens, quarter), bf16),
            pltpu.VMEM((2, slots, width), bf16),
            pltpu.VMEM((n // 2 + 1, 2, capacity, quarter), bf16),
            pltpu.VMEM((2, 2, capacity, quarter), bf16),
            pltpu.VMEM((2, 2, capacity, quarter), bf16),
            pltpu.VMEM((width, 2 * units), bf16),
            pltpu.VMEM((units, width), bf16),
            pltpu.VMEM((slots, units), bf16),
            pltpu.VMEM((slots, 2 * units), bf16),
            pltpu.VMEM((2, slots, quarter), bf16),
            pltpu.VMEM((slots, quarter), f32),
            pltpu.VMEM((2, slots, quarter), bf16),
            pltpu.VMEM((2, slots, quarter), bf16),
            pltpu.VMEM((slots, quarter), bf16),
            pltpu.VMEM((slots, quarter), bf16),
            pltpu.VMEM((slots, quarter), bf16),
            pltpu.VMEM((slots, quarter), bf16),
            pltpu.VMEM((tokens, width), bf16),
            pltpu.VMEM((2 * n, per // 2, channels), bf16),
            pltpu.VMEM((n, per, channels), bf16),
            pltpu.VMEM((tokens + 8, channels), f32),
            pltpu.VMEM((tokens + 8, channels), f32),
            pltpu.VMEM((tokens, channels), f32),
            pltpu.VMEM((tokens, channels), bf16),
            dma((12,)),
            dma((14,)),
            dma((3,)),
            dma((3, 2)),
            dma((2, n)),
            dma((2, n)),
            dma((n,)),
            dma((2, n)),
            dma((n,)),
            dma((n,)),
            dma((3, 2 * quarter // per)),
            dma((n,)),
            dma((2,)),
        ],
        compiler_params=pltpu.CompilerParams(
            collective_id=0, has_side_effects=True, vmem_limit_bytes=48 * 1024 * 1024
        ),
    )(*(pltpu.with_memory_space_constraint(arg, pltpu.HBM) for arg in args))
    outs = pl.pallas_call(
        written,
        out_shape=[jax.ShapeDtypeStruct(*shape) for shape in shapes],
        in_specs=[anywhere] * 7,
        out_specs=[hbm] * 7,
        scratch_shapes=[dma((7,))],
        compiler_params=pltpu.CompilerParams(vmem_limit_bytes=1024 * 1024),
    )(*(pltpu.with_memory_space_constraint(grad, pltpu.VMEM) for grad in grads))
    return (outs[0][None], outs[1][None], outs[2][None], *outs[3:])


def fits_kernel(mesh):
    return mesh.shape["sp"] == 8 and mesh.shape["tp"] == 4


def solution(mesh):
    placed = (
        P("sp", None),
        P("sp", None),
        P("sp", None),
        P("sp", None),
        P("sp", None, "tp"),
        P("sp", None, "tp"),
        P("sp", "tp", None),
        P("sp", "tp"),
        P("sp", "tp"),
        P("sp", "tp"),
        P(None, "tp"),
        P(None, "tp"),
    )
    return jax.shard_map(
        fused_shards if fits_kernel(mesh) else shards,
        mesh=mesh,
        in_specs=placed,
        out_specs=(
            P("sp", None, "tp"),
            P("sp", None, "tp"),
            P("sp", "tp", None),
            P("sp", "tp"),
            P("sp", "tp"),
            P("sp", "tp"),
            P("sp", "tp"),
        ),
        check_vma=False,
    )
```
